128 devices in a mesh: rep: 2 (over z_hi), fs: 32 (over z_lo, y, x), tp: 2 (over core).
Axes of the slice: x: 4, y: 4, z: 4 (z_hi: 2, z_lo: 2; z = z_hi * 2 + z_lo), core: 2. Of those that a mesh axis runs over, the one named last changes fastest.
Arguments:
- tokens: bfloat16 [64, 256, 1024], P(('rep', 'fs'), None, 'tp'), may hold values from -6 to 6
- pre_gain: float32 [1024], replicated, may hold values from 0.1 to 1.9
- first_gate: bfloat16 [1024, 2560], P('fs', 'tp'), may hold values from -0.1875 to 0.1875
- first_up: bfloat16 [1024, 2560], P('fs', 'tp'), may hold values from -0.1875 to 0.1875
- first_down: bfloat16 [2560, 1024], P('tp', 'fs'), may hold values from -0.125 to 0.125
- mix_gain: float32 [1024], P('tp'), may hold values from 0.1 to 1.9
- pool_weight: bfloat16 [4, 256, 256], P('tp', None, 'fs'), may hold values from -0.375 to 0.375
- pool_scale: float32 [1024], P('tp'), may hold values from 0.1 to 1.9
- post_gain: float32 [1024], replicated, may hold values from 0.1 to 1.9
- second_gate: bfloat16 [1024, 2560], P('fs', 'tp'), may hold values from -0.1875 to 0.1875
- second_up: bfloat16 [1024, 2560], P('fs', 'tp'), may hold values from -0.1875 to 0.1875
- second_down: bfloat16 [2560, 1024], P('tp', 'fs'), may hold values from -0.125 to 0.125
Outputs:
- layer_out: bfloat16 [64, 256, 1024], P(('rep', 'fs'), None, 'tp')
The draws below stay inside these ranges and needn't reach their ends.
All inputs are finite; a program needn't handle non-finite values.
Results may differ from the reference program's by a relative error of at most 0.015.
Values may be sent and summed in bfloat16 or wider, within the bound.
A program may use at most 64 MiB of HBM per device.

```python
import jax
import jax.numpy as jnp
from jax import lax

D = 1024
FF = 2560
GROUPS = 4
GROUP = 256
SEQ = 256
BATCH = 64


def levels(stream_key, extent, cuts, least, high):
    loudness = 1.0
    for axis_at, shards_of in cuts:
        steps = jax.random.uniform(jax.random.fold_in(jax.random.fold_in(stream_key, 6), axis_at), (shards_of,), jnp.float32, least / len(cuts), high / len(cuts))
        loudness = loudness * jnp.repeat(jnp.exp(steps), extent[axis_at] // shards_of).reshape((-1,) + (1,) * (len(extent) - 1 - axis_at))
    return loudness


def scatter_about(own_key, shape, deviation, reach, shards=(), held_as=jnp.bfloat16):
    values = deviation * jax.random.normal(own_key, shape, jnp.float32)
    if shards:
        values = values * levels(own_key, shape, shards, -0.22, 0.18)
    return jnp.clip(values, -reach, reach).astype(held_as)


def setup_inputs(seed: int = 0) -> dict:
    key_of = jax.random.split(jax.random.key(seed), 13)
    tokens = scatter_about(key_of[0], (BATCH, SEQ, D), 1.0, 6.0, ((0, 64), (2, 2)))
    pre_gain = jnp.clip(1.0 + 0.18 * jax.random.normal(key_of[1], (D,), jnp.float32), 0.1, 1.9)
    first_gate = scatter_about(key_of[2], (D, FF), D ** -0.5, 0.1875, ((0, 32), (1, 2)))
    first_up = scatter_about(key_of[3], (D, FF), D ** -0.5, 0.1875, ((0, 32), (1, 2)))
    first_down = scatter_about(key_of[4], (FF, D), FF ** -0.5, 0.125, ((0, 2), (1, 32)))
    mix_gain = jnp.clip(1.0 + 0.18 * jax.random.normal(key_of[5], (D,), jnp.float32), 0.1, 1.9)
    pool_weight = scatter_about(key_of[6], (GROUPS, GROUP, GROUP), GROUP ** -0.5, 0.375, ((0, 2), (2, 32)))
    pool_scale = jnp.clip(1.0 + 0.18 * jax.random.normal(key_of[7], (D,), jnp.float32), 0.1, 1.9)
    post_gain = jnp.clip(1.0 + 0.18 * jax.random.normal(key_of[8], (D,), jnp.float32), 0.1, 1.9)
    second_gate = scatter_about(key_of[9], (D, FF), D ** -0.5, 0.1875, ((0, 32), (1, 2)))
    second_up = scatter_about(key_of[10], (D, FF), D ** -0.5, 0.1875, ((0, 32), (1, 2)))
    second_down = scatter_about(key_of[11], (FF, D), FF ** -0.5, 0.125, ((0, 2), (1, 32)))
    return dict(tokens=tokens, pre_gain=pre_gain, first_gate=first_gate, first_up=first_up, first_down=first_down, mix_gain=mix_gain, pool_weight=pool_weight, pool_scale=pool_scale, post_gain=post_gain, second_gate=second_gate, second_up=second_up, second_down=second_down)


epsilon = 1e-06

def normalize(values, gain_vec):
    floats = values.astype(jnp.float32)
    scaled = floats * lax.rsqrt(lax.optimization_barrier(jnp.mean(floats * floats, axis=-1, keepdims=True)) + epsilon)
    return (scaled * gain_vec.astype(jnp.float32)).astype(jnp.bfloat16)

def half_block(flat_rows, gain_vec, gate_w, up_w, down_w):
    normed = normalize(flat_rows, gain_vec)
    gate_sum = jnp.dot(normed, gate_w, preferred_element_type=jnp.float32)
    up_sum = jnp.dot(normed, up_w, preferred_element_type=jnp.float32)
    hidden = (jax.nn.silu(gate_sum) * up_sum).astype(jnp.bfloat16)
    return jnp.dot(hidden, down_w, preferred_element_type=jnp.float32)

def trailing(grouped, windows, widest):
    seq_length = grouped.shape[1]
    running = jnp.zeros_like(grouped)
    for back_step in range(widest):
        moved = jnp.pad(grouped, ((0, 0), (back_step, 0), (0, 0), (0, 0)))[:, :seq_length]
        running = running + jnp.where(back_step < windows[None, None, :, None], moved, 0.0)
    positions = jnp.arange(seq_length, dtype=jnp.int32)
    counts = jnp.minimum(positions[:, None] + 1, windows[None, :]).astype(jnp.float32)
    return running / counts[None, :, :, None]

def reference(tokens, pre_gain, first_gate, first_up, first_down, mix_gain, pool_weight, pool_scale, post_gain, second_gate, second_up, second_down):
    flat_rows = tokens.reshape(BATCH * SEQ, D)
    first_out = half_block(flat_rows, pre_gain, first_gate, first_up, first_down)
    after_first = (flat_rows.astype(jnp.float32) + 0.5 * first_out).astype(jnp.bfloat16)
    normed = normalize(after_first, mix_gain)
    grouped = normed.astype(jnp.float32).reshape(BATCH, SEQ, GROUPS, GROUP)
    windows = 2 ** (jnp.arange(GROUPS, dtype=jnp.int32) + 1)
    pooled = trailing(grouped, windows, 2 ** GROUPS)
    diff = (pooled - grouped).astype(jnp.bfloat16)
    mixed = jnp.einsum('bsgc,gcd->bsgd', diff.astype(jnp.float32), pool_weight.astype(jnp.float32))
    mixed = mixed.reshape(BATCH * SEQ, D)
    after_mix = (after_first.astype(jnp.float32) + mixed * pool_scale.astype(jnp.float32)).astype(jnp.bfloat16)
    second_out = half_block(after_mix, post_gain, second_gate, second_up, second_down)
    layer_out = (after_mix.astype(jnp.float32) + 0.5 * second_out).astype(jnp.bfloat16)
    return layer_out.reshape(BATCH, SEQ, D)
```

```python
import functools

import jax
import jax.numpy as jnp
from jax import lax
from jax.experimental import pallas as pl
from jax.experimental.pallas import tpu as pltpu
from jax.sharding import PartitionSpec as P

F32 = jnp.float32
BF16 = jnp.bfloat16
MESH = pl.DeviceIdType.MESH
GROUPS = 4
SIDE = 4
epsilon = 1e-06
NT = (((1,), (1,)), ((), ()))


def layer_kernel(
    tok_ref, pre_ref, mixg_ref, scale_ref, post_ref, pw_ref,
    g1_ref, u1_ref, d1_ref, g2_ref, u2_ref, d2_ref, out_ref,
    WS0, WS1, WB0, WB1, TB, N, ACC, H, PX, PR, PO, S, R, SQ,
    xs, xr, ys, yr, zs, zr, ts, tr, ms, mr, hs, hr, rs, rr, qs,
):
    rep = lax.axis_index("rep")
    fs = lax.axis_index("fs")
    t = lax.axis_index("tp")
    x = lax.rem(fs, SIDE)
    y = lax.rem(fs // SIDE, SIDE)
    low = fs // (SIDE * SIDE)
    z = 2 * rep + low
    other = 1 - t
    high = 1 - low

    def dev(dx, dy, dz, tt):
        xx = lax.rem(x + dx, SIDE)
        yy = lax.rem(y + dy, SIDE)
        zz = lax.rem(z + dz, SIDE)
        return {"rep": zz // 2, "fs": lax.rem(zz, 2) * (SIDE * SIDE) + yy * SIDE + xx, "tp": tt}

    mate = dev(0, 0, 0, other)
    along_x = {d: dev(d, 0, 0, t) for d in (1, 2, 3)}
    along_y = {d: dev(0, d, 0, t) for d in (1, 2, 3)}
    along_z = {d: dev(0, 0, d, t) for d in (1, 3)}
    peers = [mate] + list(along_x.values()) + list(along_y.values()) + list(along_z.values())

    barrier = pltpu.get_barrier_semaphore()
    for peer in peers:
        pl.semaphore_signal(barrier, inc=1, device_id=peer, device_id_type=MESH)

    def remote(src, dst, ss, sr, to):
        return pltpu.make_async_remote_copy(
            src_ref=src, dst_ref=dst, send_sem=ss, recv_sem=sr, device_id=to, device_id_type=MESH
        )

    rows, half = tok_ref.shape
    depth, hid = g1_ref.shape
    part = hid // 2
    piece = rows // 2
    step = half // SIDE
    weights = ((g1_ref, u1_ref, d1_ref), (g2_ref, u2_ref, d2_ref))
    WS = (WS0, WS1)
    WB = (WB0, WB1)
    axis = (along_x, along_y)
    ring = (along_y, along_x)
    place = (x, y)
    spot = (y, x)

    def slab(b, lo, a, c):
        return WB[b].at[lo, c, a] if b == 0 else WB[b].at[lo, a, c]

    def line(b, lo, c):
        return WB[b].at[lo, c] if b == 0 else WB[b].at[lo, :, c]

    def line_half(b, lo, c, k):
        cut = slice(2 * k, 2 * k + 2)
        return WB[b].at[lo, c, cut] if b == 0 else WB[b].at[lo, cut, c]

    def pack(b):
        for k in range(2):
            for i, w in enumerate(weights[b]):
                WS[b][k, :, i * part:(i + 1) * part] = w[:, k * part:(k + 1) * part]
            if b == 0:
                flat = pw_ref[...]
                for i in range(2):
                    WS[b][k, i * 16:(i + 1) * 16, 3 * part:] = flat[:, i * 128:(i + 1) * 128]
        mine = lax.rem(place[b], 2)
        if b == 0:
            WB[b][low, y, x] = WS[b][mine]
        else:
            WB[b][low, y, x] = WS[b][mine]

    def class_send(b, i):
        d = (1, 3, 2)[i]
        kind = lax.rem(place[b] + d, 2)
        return remote(WS[b].at[kind], slab(b, low, place[b], spot[b]), xs.at[b, i], xr.at[b, i], axis[b][d])

    def ring_send(b, i):
        c = spot[b]
        if i < 2:
            ref = line(b, low, c)
            return remote(ref, ref, ys.at[b, i], yr.at[b, i], ring[b][(1, 3)[i]])
        if i == 2:
            ref = line_half(b, low, lax.rem(c + 3, SIDE), 0)
            return remote(ref, ref, ys.at[b, i], yr.at[b, i], ring[b][1])
        ref = line_half(b, low, lax.rem(c + 1, SIDE), 1)
        return remote(ref, ref, ys.at[b, i], yr.at[b, i], ring[b][3])

    def deep_send(b, j, k):
        c = lax.rem(spot[b] + (0, 3, 1, 2)[j], SIDE)
        ref = line_half(b, low, c, k)
        return remote(ref, ref, zs.at[b, j, k], zr.at[b, j, k], along_z[(1, 3)[k]])

    def tok_send(b, i):
        src = TB.at[b, t, i * piece:(i + 1) * piece]
        dst = TB.at[b, t, rows + i * piece:rows + (i + 1) * piece]
        return remote(src, dst, ts.at[b, i], tr.at[b, i], axis[b][(1, 3)[i]])

    def mate_send(b, i):
        cut = slice(0, rows) if i == 2 else slice(rows + i * piece, rows + (i + 1) * piece)
        ref = TB.at[b, t, cut]
        return remote(ref, ref, ms.at[b, i], mr.at[b, i], mate)

    chunks = (slice(rows, 2 * rows), slice(0, rows))

    def half_send(b, i):
        return remote(PX.at[b, chunks[i]], PR.at[b, chunks[i]], hs.at[b, i], hr.at[b, i], mate)

    def back_send(b, i):
        cut = slice(i * piece, (i + 1) * piece)
        return remote(S.at[b, cut], R.at[b, cut], rs.at[b, i], rr.at[b, i], axis[b][(3, 1)[i]])

    def norm_rows(b, cut, gain_ref):
        parts = [TB[b, c, cut].astype(F32) for c in range(2)]
        total = sum(jnp.sum(v * v, axis=-1, keepdims=True) for v in parts)
        inv = lax.rsqrt(total / (2 * half) + epsilon)
        for c in range(2):
            N[c, cut] = (parts[c] * inv * gain_ref[0:1, c * half:(c + 1) * half]).astype(BF16)

    def gate_up(b, lo, fresh):
        wide = WB[b][lo, :, :, :, 0:2 * part].reshape(half, 2 * part)
        for cut in chunks:
            value = jnp.dot(N[lo, cut], wide, preferred_element_type=F32)
            if fresh:
                ACC[cut] = value
            else:
                ACC[cut] += value

    def hidden(cut):
        H[cut] = (jax.nn.silu(ACC[cut, 0:part]) * ACC[cut, part:2 * part]).astype(BF16)

    def down(b, cut, lo):
        tall = WB[b][lo, :, :, :, 2 * part:3 * part].reshape(half, part)
        return lax.dot_general(H[cut], tall, NT, preferred_element_type=F32)

    def project(b):
        for i, cut in enumerate(chunks):
            hidden(cut)
            PX[b, cut] = down(b, cut, other).astype(BF16)
            half_send(b, i).start()
            PO[cut] = down(b, cut, t)
        half_send(b, 0).wait_recv()
        S[b] = (PO[chunks[0]] + PR[b, chunks[0]].astype(F32)).astype(BF16)
        for i in range(2):
            back_send(b, i).start()
        half_send(b, 1).wait_recv()
        total = PO[chunks[1]] + PR[b, chunks[1]].astype(F32)
        for i in range(2):
            back_send(b, i).wait_recv()
        return total + R[b].astype(F32)

    def spread(b):
        for i in range(3):
            class_send(b, i).wait_recv()
        for i in range(2):
            ring_send(b, i).start()

    def relay(b):
        for k in range(2):
            deep_send(b, 0, k).start()
        for i in range(2):
            ring_send(b, i).wait_recv()
            ring_send(b, 2 + i).start()
            for k in range(2):
                deep_send(b, 1 + i, k).start()
        for k in range(2):
            ring_send(b, 2 + k).wait_recv()
            deep_send(b, 3, k).start()

    def deep_wait(b):
        for j in range(4):
            for k in range(2):
                deep_send(b, j, k).wait_recv()

    TB[0, t, 0:rows] = tok_ref[...]
    pack(0)
    pack(1)
    pl.semaphore_wait(barrier, len(peers))

    for i in range(3):
        class_send(0, i).start()
    for i in range(3):
        class_send(1, i).start()
    mate_send(0, 2).start()
    for i in range(2):
        tok_send(0, i).start()
    mate_send(0, 2).wait_recv()
    norm_rows(0, chunks[1], pre_ref)
    spread(0)
    for i in range(2):
        tok_send(0, i).wait_recv()
        mate_send(0, i).start()
    spread(1)
    for i in range(2):
        mate_send(0, i).wait_recv()
    norm_rows(0, chunks[0], pre_ref)
    relay(0)
    gate_up(0, low, True)
    relay(1)
    deep_wait(0)
    gate_up(0, high, False)
    first = project(0)

    after_first = (tok_ref[...].astype(F32) + 0.5 * first).astype(BF16).astype(F32)
    square = after_first * after_first
    SQ[0] = sum(square[:, i * 128:(i + 1) * 128] for i in range(half // 128))
    swap = remote(SQ.at[0], SQ.at[1], qs.at[0], qs.at[1], mate)
    swap.start()
    swap.wait_recv()
    total = jnp.sum(SQ[0] + SQ[1], axis=-1, keepdims=True)
    h = (after_first * lax.rsqrt(total / (2 * half) + epsilon) * mixg_ref[0:1, :]).astype(BF16).astype(F32)
    groups_here = 2
    width = half // groups_here

    def shifted(v, by):
        spot_ids = lax.broadcasted_iota(jnp.int32, v.shape, 0)
        return jnp.where(spot_ids >= by, pltpu.roll(v, by, 0), 0.0)

    maps = WB0[:, :, :, :, 3 * part:].reshape(2 * SIDE * SIDE, depth, 128).astype(F32)
    maps = maps.reshape(2 * SIDE * SIDE, 4, 8, 128)
    for g in range(groups_here):
        hg = h[:, g * width:(g + 1) * width]
        run = hg + shifted(hg, 1)
        window = 2
        found = run
        number = t * groups_here + g
        reached = jnp.int32(2)
        for level in range(1, GROUPS):
            run = run + shifted(run, window)
            window = window * 2
            found = jnp.where(number >= level, run, found)
            reached = jnp.where(number >= level, window, reached)
        counts = jnp.minimum(lax.broadcasted_iota(jnp.int32, (rows, width), 0) + 1, reached).astype(F32)
        diff = (found / counts - hg).astype(BF16)
        turned = jnp.concatenate(
            [maps[:, g].reshape(width, 128), maps[:, 2 + g].reshape(width, 128)], axis=1
        ).astype(BF16)
        mixed = lax.dot_general(diff, turned, NT, preferred_element_type=F32)
        at = slice(g * width, (g + 1) * width)
        TB[1, t, 0:rows, at] = (after_first[:, at] + scale_ref[0:1, at] * mixed).astype(BF16)

    for i in range(2):
        tok_send(1, i).start()
    mate_send(1, 2).start()
    mate_send(1, 2).wait_recv()
    norm_rows(1, chunks[1], post_ref)
    for i in range(2):
        tok_send(1, i).wait_recv()
        mate_send(1, i).start()
    for i in range(2):
        mate_send(1, i).wait_recv()
    norm_rows(1, chunks[0], post_ref)
    gate_up(1, low, True)
    deep_wait(1)
    gate_up(1, high, False)
    second = project(1)
    out_ref[...] = (TB[1, t, 0:rows].astype(F32) + 0.5 * second).astype(BF16)

    for b in range(2):
        sent = [class_send(b, i) for i in range(3)] + [ring_send(b, i) for i in range(4)]
        sent += [deep_send(b, j, k) for j in range(4) for k in range(2)]
        sent += [tok_send(b, i) for i in range(2)] + [mate_send(b, i) for i in range(3)]
        sent += [half_send(b, i) for i in range(2)] + [back_send(b, i) for i in range(2)]
        for c in sent:
            c.wait_send()
    swap.wait_send()


def fused(
    tokens, pre_gain, first_gate, first_up, first_down, mix_gain, pool_weight,
    pool_scale, post_gain, second_gate, second_up, second_down,
):
    _, rows, half = tokens.shape
    depth, hid = first_gate.shape
    part = hid // 2
    groups, width, out_cols = pool_weight.shape

    vmem = pl.BlockSpec(memory_space=pltpu.VMEM)
    dma = pltpu.SemaphoreType.DMA
    out = pl.pallas_call(
        layer_kernel,
        out_shape=jax.ShapeDtypeStruct((rows, half), BF16),
        in_specs=[vmem] * 12,
        out_specs=vmem,
        scratch_shapes=[
            pltpu.VMEM((2, depth, 3 * part + 128), BF16),
            pltpu.VMEM((2, depth, 3 * part), BF16),
            pltpu.VMEM((2, SIDE, SIDE, depth, 3 * part + 128), BF16),
            pltpu.VMEM((2, SIDE, SIDE, depth, 3 * part), BF16),
            pltpu.VMEM((2, 2, 2 * rows, half), BF16),
            pltpu.VMEM((2, 2 * rows, half), BF16),
            pltpu.VMEM((2 * rows, 2 * part), F32),
            pltpu.VMEM((2 * rows, part), BF16),
            pltpu.VMEM((2, 2 * rows, half), BF16),
            pltpu.VMEM((2, 2 * rows, half), BF16),
            pltpu.VMEM((2 * rows, half), F32),
            pltpu.VMEM((2, rows, half), BF16),
            pltpu.VMEM((2, rows, half), BF16),
            pltpu.VMEM((2, rows, 128), F32),
            dma((2, 3)), dma((2, 3)), dma((2, 4)), dma((2, 4)), dma((2, 4, 2)), dma((2, 4, 2)),
            dma((2, 2)), dma((2, 2)), dma((2, 3)), dma((2, 3)), dma((2, 2)), dma((2, 2)),
            dma((2, 2)), dma((2, 2)), dma((2,)),
        ],
        compiler_params=pltpu.CompilerParams(
            collective_id=0, has_side_effects=True, vmem_limit_bytes=60 * 1024 * 1024
        ),
    )(
        tokens.reshape(rows, half), pre_gain.reshape(1, -1), mix_gain.reshape(1, -1),
        pool_scale.reshape(1, -1), post_gain.reshape(1, -1),
        jnp.swapaxes(pool_weight, 1, 2).reshape(groups * out_cols, width),
        first_gate, first_up, first_down.T, second_gate, second_up, second_down.T,
    )
    return out.reshape(tokens.shape)


def solution(mesh):
    tok = P(("rep", "fs"), None, "tp")
    wide = P("fs", "tp")
    tall = P("tp", "fs")
    placed = (
        tok, P(), wide, wide, tall, P("tp"), P("tp", None, "fs"), P("tp"), P(), wide, wide, tall,
    )

    def layer(*args):
        return jax.shard_map(fused, mesh=mesh, in_specs=placed, out_specs=tok, check_vma=False)(*args)

    return layer
```

```python
import functools

import jax
import jax.numpy as jnp
from jax import lax
from jax.experimental import pallas as pl
from jax.experimental.pallas import tpu as pltpu
from jax.sharding import PartitionSpec as P

F32 = jnp.float32
BF16 = jnp.bfloat16
MESH = pl.DeviceIdType.MESH
GROUPS = 4
SIDE = 4
epsilon = 1e-06
NT = (((1,), (1,)), ((), ()))


def layer_kernel(
    tok_ref, pre_ref, mixg_ref, scale_ref, post_ref, pw_ref,
    g1_ref, u1_ref, d1_ref, g2_ref, u2_ref, d2_ref, out_ref,
    WS0, WS1, WB0, WB1, TB, N, ACC, H, PX, PR, PO, S, R, SQ,
    xs, xr, ys, yr, fw, fr, zs, zr, ts, tr, ms, mr, hs, hr, rs, rr, qs,
):
    rep = lax.axis_index("rep")
    fs = lax.axis_index("fs")
    t = lax.axis_index("tp")
    x = lax.rem(fs, SIDE)
    y = lax.rem(fs // SIDE, SIDE)
    low = fs // (SIDE * SIDE)
    z = 2 * rep + low
    other = 1 - t
    high = 1 - low

    def dev(dx, dy, dz, tt):
        xx = lax.rem(x + dx, SIDE)
        yy = lax.rem(y + dy, SIDE)
        zz = lax.rem(z + dz, SIDE)
        return {"rep": zz // 2, "fs": lax.rem(zz, 2) * (SIDE * SIDE) + yy * SIDE + xx, "tp": tt}

    mate = dev(0, 0, 0, other)
    along_x = {d: dev(d, 0, 0, t) for d in (1, 2, 3)}
    along_y = {d: dev(0, d, 0, t) for d in (1, 2, 3)}
    along_z = {d: dev(0, 0, d, t) for d in (1, 3)}
    peers = [mate] + list(along_x.values()) + list(along_y.values()) + list(along_z.values())

    barrier = pltpu.get_barrier_semaphore()
    for peer in peers:
        pl.semaphore_signal(barrier, inc=1, device_id=peer, device_id_type=MESH)

    def remote(src, dst, ss, sr, to):
        return pltpu.make_async_remote_copy(
            src_ref=src, dst_ref=dst, send_sem=ss, recv_sem=sr, device_id=to, device_id_type=MESH
        )

    rows, half = tok_ref.shape
    depth, hid = g1_ref.shape
    part = hid // 2
    piece = rows // 2
    step = half // SIDE
    weights = ((g1_ref, u1_ref, d1_ref), (g2_ref, u2_ref, d2_ref))
    WS = (WS0, WS1)
    WB = (WB0, WB1)
    axis = (along_x, along_y)
    ring = (along_y, along_x)
    place = (x, y)
    spot = (y, x)

    def slab(b, lo, j, c):
        a = lax.rem(place[b] + j, SIDE)
        c = lax.rem(spot[b] + c, SIDE)
        return WB[b].at[lo, c, a] if b == 0 else WB[b].at[lo, a, c]

    def pack(b):
        for k in range(2):
            for i, w in enumerate(weights[b]):
                WS[b][k, :, i * part:(i + 1) * part] = w[:, k * part:(k + 1) * part]
            if b == 0:
                flat = pw_ref[...]
                for i in range(2):
                    WS[b][k, i * 16:(i + 1) * 16, 3 * part:] = flat[:, i * 128:(i + 1) * 128]
        mine = lax.rem(place[b], 2)
        WB[b][low, y, x] = WS[b][mine]

    items = [(0, 0), (0, 1), (0, 3), (1, 0), (0, 2)]
    sides = (0, 0, 1, 1, 0)
    early = (0,)
    line_of = {0: 0, 3: 1, 1: 2, 2: 3}

    def class_send(b, j):
        d = SIDE - j
        kind = lax.rem(place[b] + d, 2)
        return remote(WS[b].at[kind], slab(b, low, 0, 0), xs.at[b, j - 1], xr.at[b, j - 1], axis[b][d])

    def ring_send(b, i, side):
        comp, j = items[i]
        ref = slab(b, high if comp else low, j, 0)
        return remote(ref, ref, ys.at[b, i, side], yr.at[b, i, side], ring[b][(1, 3)[side]])

    def far_send(b, i):
        comp, j = items[i]
        side = sides[i] if b == 0 else 1 - sides[i]
        ref = slab(b, high if comp else low, j, (3, 1)[side])
        return remote(ref, ref, fw.at[b, i], fr.at[b, i], ring[b][(1, 3)[side]])

    def deep_send(b, j, c):
        up = j == 1 or (j == 2 and c in (0, 1)) or (j == 0 and b == 0)
        ref = slab(b, low, j, c)
        n = line_of[c]
        return remote(ref, ref, zs.at[b, j, n], zr.at[b, j, n], along_z[1 if up else 3])

    def begin(b):
        for j in (3, 1, 2):
            class_send(b, j).start()
        for side in range(2):
            ring_send(b, 0, side).start()
        deep_send(b, 0, 0).start()

    def on_class(b, j):
        class_send(b, j).wait_recv()
        for side in range(2):
            ring_send(b, items.index((0, j)), side).start()
        deep_send(b, j, 0).start()

    def on_cross(b):
        deep_send(b, 0, 0).wait_recv()
        for side in range(2):
            ring_send(b, items.index((1, 0)), side).start()

    def on_ring(b, i):
        comp, j = items[i]
        for side in range(2):
            ring_send(b, i, side).wait_recv()
            if side == (sides[i] if b == 0 else 1 - sides[i]):
                far_send(b, i).start()
            if not comp and j not in early:
                deep_send(b, j, (3, 1)[side]).start()

    def on_far(b, i):
        comp, j = items[i]
        far_send(b, i).wait_recv()
        if not comp and j not in early:
            deep_send(b, j, 2).start()

    def deep_wait(b):
        for c in (0, 3, 1, 2):
            for j in (1, 3, 2):
                deep_send(b, j, c).wait_recv()

    def tok_send(b, i):
        src = TB.at[b, t, i * piece:(i + 1) * piece]
        dst = TB.at[b, t, rows + i * piece:rows + (i + 1) * piece]
        return remote(src, dst, ts.at[b, i], tr.at[b, i], axis[b][(1, 3)[i]])

    def mate_send(b, i):
        cut = slice(0, rows) if i == 2 else slice(rows + i * piece, rows + (i + 1) * piece)
        ref = TB.at[b, t, cut]
        return remote(ref, ref, ms.at[b, i], mr.at[b, i], mate)

    chunks = (slice(rows, 2 * rows), slice(0, rows))

    def half_send(b, i):
        return remote(PX.at[b, chunks[i]], PR.at[b, chunks[i]], hs.at[b, i], hr.at[b, i], mate)

    def back_send(b, i):
        cut = slice(i * piece, (i + 1) * piece)
        return remote(S.at[b, cut], R.at[b, cut], rs.at[b, i], rr.at[b, i], axis[b][(3, 1)[i]])

    def norm_rows(b, cut, gain_ref):
        parts = [TB[b, c, cut].astype(F32) for c in range(2)]
        total = sum(jnp.sum(v * v, axis=-1, keepdims=True) for v in parts)
        inv = lax.rsqrt(total / (2 * half) + epsilon)
        for c in range(2):
            N[c, cut] = (parts[c] * inv * gain_ref[0:1, c * half:(c + 1) * half]).astype(BF16)

    def gate_up(b, lo, fresh, cut):
        wide = WB[b][lo, :, :, :, 0:2 * part].reshape(half, 2 * part)
        value = jnp.dot(N[lo, cut], wide, preferred_element_type=F32)
        if fresh:
            ACC[cut] = value
        else:
            ACC[cut] += value

    def hidden(cut):
        H[cut] = (jax.nn.silu(ACC[cut, 0:part]) * ACC[cut, part:2 * part]).astype(BF16)

    def down(b, cut, lo):
        tall = WB[b][lo, :, :, :, 2 * part:3 * part].reshape(half, part)
        return lax.dot_general(H[cut], tall, NT, preferred_element_type=F32)

    def project(b, meanwhile):
        for i, cut in enumerate(chunks):
            gate_up(b, high, False, cut)
            hidden(cut)
            PX[b, cut] = down(b, cut, other).astype(BF16)
            half_send(b, i).start()
            PO[cut] = down(b, cut, t)
        half_send(b, 0).wait_recv()
        S[b] = (PO[chunks[0]] + PR[b, chunks[0]].astype(F32)).astype(BF16)
        for i in range(2):
            back_send(b, i).start()
        meanwhile()
        half_send(b, 1).wait_recv()
        total = PO[chunks[1]] + PR[b, chunks[1]].astype(F32)
        for i in range(2):
            back_send(b, i).wait_recv()
        return total + R[b].astype(F32)

    TB[0, t, 0:rows] = tok_ref[...]
    pack(0)
    pack(1)
    pl.semaphore_wait(barrier, len(peers))

    begin(0)
    mate_send(0, 2).start()
    for i in range(2):
        tok_send(0, i).start()
    begin(1)
    on_class(0, 3)
    on_class(0, 1)
    on_cross(0)
    mate_send(0, 2).wait_recv()
    norm_rows(0, chunks[1], pre_ref)
    on_class(0, 2)
    for i in range(2):
        tok_send(0, i).wait_recv()
        mate_send(0, i).start()
    on_ring(0, 0)
    on_ring(0, 1)
    on_ring(0, 2)
    for i in range(2):
        mate_send(0, i).wait_recv()
    norm_rows(0, chunks[0], pre_ref)
    on_class(1, 3)
    on_class(1, 1)
    on_ring(0, 3)
    on_ring(0, 4)
    on_cross(1)
    on_class(1, 2)
    for i in range(5):
        on_far(0, i)
    for i in range(5):
        on_ring(1, i)
    for cut in chunks:
        gate_up(0, low, True, cut)
    deep_wait(0)

    def fars():
        for i in range(5):
            on_far(1, i)

    first = project(0, fars)

    after_first = (tok_ref[...].astype(F32) + 0.5 * first).astype(BF16).astype(F32)
    square = after_first * after_first
    SQ[0] = sum(square[:, i * 128:(i + 1) * 128] for i in range(half // 128))
    swap = remote(SQ.at[0], SQ.at[1], qs.at[0], qs.at[1], mate)
    swap.start()
    swap.wait_recv()
    total = jnp.sum(SQ[0] + SQ[1], axis=-1, keepdims=True)
    h = (after_first * lax.rsqrt(total / (2 * half) + epsilon) * mixg_ref[0:1, :]).astype(BF16).astype(F32)
    groups_here = 2
    width = half // groups_here

    def shifted(v, by):
        spot_ids = lax.broadcasted_iota(jnp.int32, v.shape, 0)
        return jnp.where(spot_ids >= by, pltpu.roll(v, by, 0), 0.0)

    maps = WB0[:, :, :, :, 3 * part:].reshape(2 * SIDE * SIDE, depth, 128).astype(F32)
    maps = maps.reshape(2 * SIDE * SIDE, 4, 8, 128)
    for g in range(groups_here):
        hg = h[:, g * width:(g + 1) * width]
        run = hg + shifted(hg, 1)
        window = 2
        found = run
        number = t * groups_here + g
        reached = jnp.int32(2)
        for level in range(1, GROUPS):
            run = run + shifted(run, window)
            window = window * 2
            found = jnp.where(number >= level, run, found)
            reached = jnp.where(number >= level, window, reached)
        counts = jnp.minimum(lax.broadcasted_iota(jnp.int32, (rows, width), 0) + 1, reached).astype(F32)
        diff = (found / counts - hg).astype(BF16)
        turned = jnp.concatenate(
            [maps[:, g].reshape(width, 128), maps[:, 2 + g].reshape(width, 128)], axis=1
        ).astype(BF16)
        mixed = lax.dot_general(diff, turned, NT, preferred_element_type=F32)
        at = slice(g * width, (g + 1) * width)
        TB[1, t, 0:rows, at] = (after_first[:, at] + scale_ref[0:1, at] * mixed).astype(BF16)

    for i in range(2):
        tok_send(1, i).start()
    mate_send(1, 2).start()
    mate_send(1, 2).wait_recv()
    norm_rows(1, chunks[1], post_ref)
    gate_up(1, low, True, chunks[1])
    for i in range(2):
        tok_send(1, i).wait_recv()
        mate_send(1, i).start()
    for i in range(2):
        mate_send(1, i).wait_recv()
    norm_rows(1, chunks[0], post_ref)
    gate_up(1, low, True, chunks[0])
    deep_wait(1)
    second = project(1, lambda: None)
    out_ref[...] = (TB[1, t, 0:rows].astype(F32) + 0.5 * second).astype(BF16)

    for b in range(2):
        sent = [class_send(b, j) for j in (1, 2, 3)] + [far_send(b, i) for i in range(5)]
        sent += [ring_send(b, i, k) for i in range(5) for k in range(2)]
        sent += [deep_send(b, j, c) for j in (1, 2, 3) for c in range(SIDE)] + [deep_send(b, 0, 0)]
        sent += [tok_send(b, i) for i in range(2)] + [mate_send(b, i) for i in range(3)]
        sent += [half_send(b, i) for i in range(2)] + [back_send(b, i) for i in range(2)]
        for c in sent:
            c.wait_send()
    swap.wait_send()


def fused(
    tokens, pre_gain, first_gate, first_up, first_down, mix_gain, pool_weight,
    pool_scale, post_gain, second_gate, second_up, second_down,
):
    _, rows, half = tokens.shape
    depth, hid = first_gate.shape
    part = hid // 2
    groups, width, out_cols = pool_weight.shape

    vmem = pl.BlockSpec(memory_space=pltpu.VMEM)
    dma = pltpu.SemaphoreType.DMA
    out = pl.pallas_call(
        layer_kernel,
        out_shape=jax.ShapeDtypeStruct((rows, half), BF16),
        in_specs=[vmem] * 12,
        out_specs=vmem,
        scratch_shapes=[
            pltpu.VMEM((2, depth, 3 * part + 128), BF16),
            pltpu.VMEM((2, depth, 3 * part), BF16),
            pltpu.VMEM((2, SIDE, SIDE, depth, 3 * part + 128), BF16),
            pltpu.VMEM((2, SIDE, SIDE, depth, 3 * part), BF16),
            pltpu.VMEM((2, 2, 2 * rows, half), BF16),
            pltpu.VMEM((2, 2 * rows, half), BF16),
            pltpu.VMEM((2 * rows, 2 * part), F32),
            pltpu.VMEM((2 * rows, part), BF16),
            pltpu.VMEM((2, 2 * rows, half), BF16),
            pltpu.VMEM((2, 2 * rows, half), BF16),
            pltpu.VMEM((2 * rows, half), F32),
            pltpu.VMEM((2, rows, half), BF16),
            pltpu.VMEM((2, rows, half), BF16),
            pltpu.VMEM((2, rows, 128), F32),
            dma((2, 3)), dma((2, 3)), dma((2, 5, 2)), dma((2, 5, 2)), dma((2, 5)), dma((2, 5)),
            dma((2, 4, 4)), dma((2, 4, 4)),
            dma((2, 2)), dma((2, 2)), dma((2, 3)), dma((2, 3)), dma((2, 2)), dma((2, 2)),
            dma((2, 2)), dma((2, 2)), dma((2,)),
        ],
        compiler_params=pltpu.CompilerParams(
            collective_id=0, has_side_effects=True, vmem_limit_bytes=60 * 1024 * 1024
        ),
    )(
        tokens.reshape(rows, half), pre_gain.reshape(1, -1), mix_gain.reshape(1, -1),
        pool_scale.reshape(1, -1), post_gain.reshape(1, -1),
        jnp.swapaxes(pool_weight, 1, 2).reshape(groups * out_cols, width),
        first_gate, first_up, first_down.T, second_gate, second_up, second_down.T,
    )
    return out.reshape(tokens.shape)


def solution(mesh):
    tok = P(("rep", "fs"), None, "tp")
    wide = P("fs", "tp")
    tall = P("tp", "fs")
    placed = (
        tok, P(), wide, wide, tall, P("tp"), P("tp", None, "fs"), P("tp"), P(), wide, wide, tall,
    )

    def layer(*args):
        return jax.shard_map(fused, mesh=mesh, in_specs=placed, out_specs=tok, check_vma=False)(*args)

    return layer
```

```python
import jax
import jax.numpy as jnp
from jax import lax
from jax.experimental import pallas as pl
from jax.experimental.pallas import tpu as pltpu
from jax.sharding import PartitionSpec as P

F32 = jnp.float32
BF16 = jnp.bfloat16
MESH = pl.DeviceIdType.MESH
GROUPS = 4
SIDE = 4
epsilon = 1e-06
NT = (((1,), (1,)), ((), ()))

PLAN = (
    (
        ("c", 1, 1), ("c", 0, 3), ("c", 0, 1), ("c", 1, 3), ("z", 0, 0, 0, 1), ("z", 1, 0, 0, 0), ("c", 1, 2),
        ("z", 3, 0, 0, 0), ("r", 1, 0, 0, 0), ("r", 1, 0, 0, 1), ("z", 2, 0, 0, 1), ("r", 0, 0, 0, 1),
        ("t", 1, 0), ("c", 0, 2), ("z", 1, 1, 0, 0), ("z", 1, 3, 0, 1), ("r", 0, 0, 1, 1), ("r", 1, 0, 3, 0),
        ("r", 1, 0, 1, 1), ("z", 0, 3, 0, 0), ("z", 0, 1, 0, 1), ("r", 0, 0, 1, 0), ("r", 1, 0, 1, 0),
        ("r", 1, 0, 3, 1), ("r", 0, 1, 0, 1), ("z", 1, 2, 0, 0), ("r", 0, 0, 3, 0), ("r", 1, 0, 2, 0),
        ("r", 1, 1, 0, 1), ("r", 0, 0, 3, 1), ("z", 0, 2, 0, 0), ("z", 0, 1, 1, 1), ("f", 1, 0, 1, 1),
        ("f", 1, 0, 3, 0), ("r", 0, 0, 0, 0), ("r", 0, 0, 2, 1),
    ),
    (
        ("z", 1, 1, 3, 0), ("t", 0, 0), ("f", 1, 0, 0, 1), ("z", 0, 1, 3, 1), ("f", 0, 0, 1, 0), ("t", 1, 1),
        ("z", 1, 1, 1, 0), ("r", 1, 0, 2, 1), ("z", 1, 3, 3, 1), ("r", 0, 1, 0, 0), ("z", 0, 3, 3, 0),
        ("t", 0, 1), ("f", 1, 0, 2, 0), ("z", 1, 3, 2, 1), ("f", 0, 0, 3, 1), ("r", 0, 0, 2, 0),
        ("z", 0, 3, 1, 0), ("r", 1, 1, 0, 0), ("z", 1, 2, 3, 1), ("c", 3, 1), ("c", 3, 3), ("r", 0, 1, 2, 0),
        ("r", 0, 1, 2, 1), ("z", 1, 2, 1, 0), ("z", 0, 1, 2, 1), ("c", 3, 2), ("z", 1, 1, 2, 0),
        ("f", 0, 0, 2, 1), ("f", 0, 0, 0, 0), ("z", 1, 2, 2, 1), ("r", 2, 1, 0, 0), ("r", 2, 0, 0, 1),
    ),
    (
        ("z", 0, 3, 2, 0), ("z", 1, 3, 1, 1), ("f", 0, 1, 0, 1), ("c", 2, 3), ("f", 1, 1, 0, 0),
        ("r", 2, 1, 0, 1), ("z", 3, 1, 0, 0), ("z", 3, 3, 0, 1), ("f", 0, 1, 2, 0), ("c", 2, 1),
        ("r", 2, 0, 0, 0), ("z", 3, 2, 0, 0),
    ),
    (
        ("c", 2, 2), ("r", 2, 0, 3, 0), ("r", 2, 0, 3, 1), ("z", 2, 3, 0, 0), ("r", 3, 0, 2, 0),
        ("r", 3, 0, 1, 1), ("r", 2, 0, 1, 1), ("r", 2, 0, 1, 0), ("z", 2, 1, 0, 1), ("r", 3, 0, 1, 0),
        ("r", 3, 0, 3, 1),
    ),
    (
        ("r", 3, 0, 3, 0), ("r", 3, 0, 2, 1), ("f", 2, 1, 0, 1), ("f", 2, 0, 0, 0), ("z", 2, 2, 0, 0),
        ("r", 3, 1, 0, 0), ("r", 3, 1, 0, 1), ("z", 3, 2, 3, 1), ("z", 3, 3, 1, 1), ("z", 2, 3, 1, 0),
        ("z", 3, 3, 3, 1), ("z", 3, 1, 3, 0), ("z", 2, 1, 3, 1), ("f", 2, 0, 3, 1), ("f", 2, 0, 1, 0),
        ("f", 3, 0, 1, 1), ("f", 3, 0, 3, 0), ("z", 3, 1, 1, 0), ("f", 3, 0, 2, 0), ("r", 3, 0, 0, 1),
        ("z", 2, 1, 1, 1), ("r", 2, 0, 2, 1), ("r", 2, 1, 2, 0), ("z", 3, 2, 1, 0),
    ),
    (
        ("r", 3, 0, 0, 0), ("z", 2, 3, 3, 0), ("r", 2, 1, 2, 1), ("r", 2, 0, 2, 0), ("f", 3, 1, 0, 0),
        ("z", 3, 3, 2, 1), ("z", 2, 3, 2, 0), ("f", 3, 0, 0, 1), ("z", 2, 1, 2, 1), ("f", 2, 1, 2, 0),
        ("f", 2, 0, 2, 1), ("z", 3, 1, 2, 0), ("z", 3, 2, 2, 1),
    ),
    (

    ),
)

WAVES = [op for part in PLAN for op in part]
RING_SIDE = {(op[1], op[3]): op[4] for op in WAVES if op[0] == "f" and op[2] == 0}
RISE = {op[1:4]: op[4] for op in WAVES if op[0] == "z"}
COPIES = {op: i for i, op in enumerate(op for op in WAVES if op[0] != "t")}


def sources(op):
    kind, s = op[:2]
    if kind == "c" or kind == "t":
        return []
    if kind == "r":
        _, _, comp, j, _ = op
        if comp:
            return [("z", s, j, 0, RISE[s, j, 0])]
        return [("c", s, j)] if j else []
    if kind == "f":
        return [("r",) + op[1:]]
    _, _, j, c, _ = op
    if c == 0:
        return [("c", s, j)] if j else []
    if c == 2:
        return [("f", s, 0, j, RING_SIDE[s, j])]
    return [("r", s, 0, j, 0 if c == 3 else 1)]


def layer_kernel(
    tok_ref, pre_ref, mixg_ref, scale_ref, post_ref, pw_ref,
    g1_ref, u1_ref, d1_ref, g2_ref, u2_ref, d2_ref, out_ref,
    WS0, WS1, WS2, WS3, WB0, WB1, WB2, WB3, TB, N, ACC0, ACC1, H0, H1, PX, PR, PO, S, R, SQ,
    ws, wr, ts, tr, ms, mr, hs, hr, rs, rr, qs,
):
    rep = lax.axis_index("rep")
    fs = lax.axis_index("fs")
    t = lax.axis_index("tp")
    x = lax.rem(fs, SIDE)
    y = lax.rem(fs // SIDE, SIDE)
    low = fs // (SIDE * SIDE)
    z = 2 * rep + low
    other = 1 - t
    high = 1 - low

    def dev(dx, dy, dz, tt):
        xx = lax.rem(x + dx, SIDE)
        yy = lax.rem(y + dy, SIDE)
        zz = lax.rem(z + dz, SIDE)
        return {"rep": zz // 2, "fs": lax.rem(zz, 2) * (SIDE * SIDE) + yy * SIDE + xx, "tp": tt}

    mate = dev(0, 0, 0, other)
    along_x = {d: dev(d, 0, 0, t) for d in (1, 2, 3)}
    along_y = {d: dev(0, d, 0, t) for d in (1, 2, 3)}
    along_z = {d: dev(0, 0, d, t) for d in (1, 3)}
    peers = [mate] + list(along_x.values()) + list(along_y.values()) + list(along_z.values())

    barrier = pltpu.get_barrier_semaphore()
    for peer in peers:
        pl.semaphore_signal(barrier, inc=1, device_id=peer, device_id_type=MESH)

    def remote(src, dst, ss, sr, to):
        return pltpu.make_async_remote_copy(
            src_ref=src, dst_ref=dst, send_sem=ss, recv_sem=sr, device_id=to, device_id_type=MESH
        )

    rows, half = tok_ref.shape
    depth, hid = g1_ref.shape
    piece = rows // 2
    widths = (H0.shape[1], H1.shape[1])
    weights = ((g1_ref, u1_ref, d1_ref), (g2_ref, u2_ref, d2_ref))
    WS = (WS0, WS1, WS2, WS3)
    WB = (WB0, WB1, WB2, WB3)
    ACC = (ACC0, ACC1)
    H = (H0, H1)
    axes = (along_x, along_y)
    turn = (0, 1, 1, 0)
    places = (x, y)

    def slab(s, lo, j, c):
        a = lax.rem(places[turn[s]] + j, SIDE)
        c = lax.rem(places[1 - turn[s]] + c, SIDE)
        return WB[s].at[lo, c, a] if turn[s] == 0 else WB[s].at[lo, a, c]

    def pack(s):
        b, p = divmod(s, 2)
        n = widths[p]
        start = 2 * widths[0] * p
        for k in range(2):
            for i, w in enumerate(weights[b]):
                WS[s][k, :, i * n:(i + 1) * n] = w[:, start + k * n:start + (k + 1) * n]
            if s == 1:
                flat = pw_ref[...]
                for i in range(2):
                    WS[s][k, i * 16:(i + 1) * 16, 3 * n:] = flat[:, i * 128:(i + 1) * 128]
        WB[s][low, y, x] = WS[s][lax.rem(places[turn[s]], 2)]

    def copy_of(op):
        kind = op[0]
        if kind == "t":
            return tok_send(0, op[1], op[2])
        s = op[1]
        axis, ring = axes[turn[s]], axes[1 - turn[s]]
        sems = (ws.at[COPIES[op]], wr.at[COPIES[op]])
        if kind == "c":
            d = SIDE - op[2]
            src = WS[s].at[lax.rem(places[turn[s]] + d, 2)]
            return remote(src, slab(s, low, 0, 0), *sems, axis[d])
        if kind == "r":
            _, _, comp, j, side = op
            ref = slab(s, high if comp else low, j, 0)
            return remote(ref, ref, *sems, ring[(1, 3)[side]])
        if kind == "f":
            _, _, comp, j, side = op
            ref = slab(s, high if comp else low, j, (3, 1)[side])
            return remote(ref, ref, *sems, ring[(1, 3)[side]])
        _, _, j, c, up = op
        ref = slab(s, low, j, c)
        return remote(ref, ref, *sems, along_z[1 if up else 3])

    here = set()

    def need(op):
        if op not in here:
            here.add(op)
            copy_of(op).wait_recv()

    def issue(part):
        for op in PLAN[part]:
            for source in sources(op):
                need(source)
            copy_of(op).start()

    def base(p):
        return rows * (1 + p)

    own = slice(0, rows)
    foreign = tuple(slice(base(p), base(p) + rows) for p in range(2))

    def axis_of(b, p):
        return axes[turn[2 * b + p]]

    def tok_send(b, p, i):
        src = TB.at[b, t, i * piece:(i + 1) * piece]
        dst = TB.at[b, t, base(p) + i * piece:base(p) + (i + 1) * piece]
        return remote(src, dst, ts.at[b, p, i], tr.at[b, p, i], axis_of(b, p)[(1, 3)[i]])

    def mate_send(b, n):
        cut = own if n == 4 else slice(rows + n * piece, rows + (n + 1) * piece)
        ref = TB.at[b, t, cut]
        return remote(ref, ref, ms.at[b, n], mr.at[b, n], mate)

    def half_send(b, n):
        cut = own if n == 2 else foreign[n]
        return remote(PX.at[b, cut], PR.at[b, cut], hs.at[b, n], hr.at[b, n], mate)

    def back_send(b, p, i):
        cut = slice(i * piece, (i + 1) * piece)
        return remote(
            S.at[b, p, cut], R.at[b, p, cut], rs.at[b, p, i], rr.at[b, p, i], axis_of(b, p)[(3, 1)[i]]
        )

    def norm_rows(b, cut, gain_ref):
        parts = [TB[b, c, cut].astype(F32) for c in range(2)]
        total = sum(jnp.sum(v * v, axis=-1, keepdims=True) for v in parts)
        inv = lax.rsqrt(total / (2 * half) + epsilon)
        for c in range(2):
            N[c, cut] = (parts[c] * inv * gain_ref[0:1, c * half:(c + 1) * half]).astype(BF16)

    def gate_up(b, p, lo, fresh, cut):
        n = 2 * widths[p]
        wide = WB[2 * b + p][lo, :, :, :, 0:n].reshape(half, n)
        value = jnp.dot(N[lo, cut], wide, preferred_element_type=F32)
        at = own if cut is own else slice(rows, 2 * rows)
        if fresh:
            ACC[p][at] = value
        else:
            ACC[p][at] += value

    def hidden(p, cut):
        at = own if cut is own else slice(rows, 2 * rows)
        n = widths[p]
        H[p][at] = (jax.nn.silu(ACC[p][at, 0:n]) * ACC[p][at, n:2 * n]).astype(BF16)

    def down(b, p, cut, lo):
        at = own if cut is own else slice(rows, 2 * rows)
        n = widths[p]
        tall = WB[2 * b + p][lo, :, :, :, 2 * n:3 * n].reshape(half, n)
        return lax.dot_general(H[p][at], tall, NT, preferred_element_type=F32)

    def project(b, last, meanwhile):
        for p in range(2):
            cut = foreign[p]
            gate_up(b, p, last, False, cut)
            hidden(p, cut)
            PX[b, cut] = down(b, p, cut, other).astype(BF16)
            half_send(b, p).start()
            PO[cut] = down(b, p, cut, t)
        for p in range(2):
            gate_up(b, p, last, False, own)
            hidden(p, own)
        PX[b, own] = (down(b, 0, own, other) + down(b, 1, own, other)).astype(BF16)
        half_send(b, 2).start()
        for p in range(2):
            cut = foreign[p]
            half_send(b, p).wait_recv()
            S[b, p] = (PO[cut] + PR[b, cut].astype(F32)).astype(BF16)
            for i in range(2):
                back_send(b, p, i).start()
        PO[own] = down(b, 0, own, t) + down(b, 1, own, t)
        meanwhile()
        half_send(b, 2).wait_recv()
        total = PO[own] + PR[b, own].astype(F32)
        for p in range(2):
            for i in range(2):
                back_send(b, p, i).wait_recv()
            total = total + R[b, p].astype(F32)
        return total

    def all_of(b):
        return [op for op in COPIES if op[1] // 2 == b]

    def first_half(op):
        return op[0] == "c" or (op[0] in "rf" and op[2] == 0)

    TB[0, t, own] = tok_ref[...]
    for s in range(4):
        pack(s)
    pl.semaphore_wait(barrier, len(peers))

    mate_send(0, 4).start()
    issue(0)
    mate_send(0, 4).wait_recv()
    norm_rows(0, own, pre_ref)
    issue(1)
    for p in range(2):
        for i in range(2):
            tok_send(0, p, i).wait_recv()
            mate_send(0, 2 * p + i).start()
    issue(2)
    for p in range(2):
        for i in range(2):
            mate_send(0, 2 * p + i).wait_recv()
        norm_rows(0, foreign[p], pre_ref)
    issue(3)
    for op in all_of(0):
        if first_half(op):
            need(op)
    for p in range(2):
        gate_up(0, p, low, True, foreign[p])
        gate_up(0, p, low, True, own)
    for op in all_of(0):
        need(op)
    first = project(0, high, lambda: issue(4))

    after_first = (tok_ref[...].astype(F32) + 0.5 * first).astype(BF16).astype(F32)
    square = after_first * after_first
    SQ[0] = sum(square[:, i * 128:(i + 1) * 128] for i in range(half // 128))
    swap = remote(SQ.at[0], SQ.at[1], qs.at[0], qs.at[1], mate)
    swap.start()
    swap.wait_recv()
    total = jnp.sum(SQ[0] + SQ[1], axis=-1, keepdims=True)
    h = (after_first * lax.rsqrt(total / (2 * half) + epsilon) * mixg_ref[0:1, :]).astype(BF16).astype(F32)
    groups_here = 2
    width = half // groups_here

    def shifted(v, by):
        spot_ids = lax.broadcasted_iota(jnp.int32, v.shape, 0)
        return jnp.where(spot_ids >= by, pltpu.roll(v, by, 0), 0.0)

    maps = WB1[:, :, :, :, 3 * widths[1]:].reshape(2 * SIDE * SIDE, depth, 128).astype(F32)
    maps = maps.reshape(2 * SIDE * SIDE, 4, 8, 128)
    for g in range(groups_here):
        hg = h[:, g * width:(g + 1) * width]
        run = hg + shifted(hg, 1)
        window = 2
        found = run
        number = t * groups_here + g
        reached = jnp.int32(2)
        for level in range(1, GROUPS):
            run = run + shifted(run, window)
            window = window * 2
            found = jnp.where(number >= level, run, found)
            reached = jnp.where(number >= level, window, reached)
        counts = jnp.minimum(lax.broadcasted_iota(jnp.int32, (rows, width), 0) + 1, reached).astype(F32)
        diff = (found / counts - hg).astype(BF16)
        turned = jnp.concatenate(
            [maps[:, g].reshape(width, 128), maps[:, 2 + g].reshape(width, 128)], axis=1
        ).astype(BF16)
        mixed = lax.dot_general(diff, turned, NT, preferred_element_type=F32)
        at = slice(g * width, (g + 1) * width)
        TB[1, t, own, at] = (after_first[:, at] + scale_ref[0:1, at] * mixed).astype(BF16)

    for p in range(2):
        for i in range(2):
            tok_send(1, p, i).start()
    mate_send(1, 4).start()
    mate_send(1, 4).wait_recv()
    norm_rows(1, own, post_ref)
    issue(5)
    for p in range(2):
        for i in range(2):
            tok_send(1, p, i).wait_recv()
            mate_send(1, 2 * p + i).start()
    issue(6)
    for op in all_of(1):
        if first_half(op):
            need(op)
    for p in range(2):
        gate_up(1, p, low, True, own)
    for p in range(2):
        for i in range(2):
            mate_send(1, 2 * p + i).wait_recv()
        norm_rows(1, foreign[p], post_ref)
        gate_up(1, p, low, True, foreign[p])
    for op in all_of(1):
        need(op)
    second = project(1, high, lambda: None)
    out_ref[...] = (TB[1, t, own].astype(F32) + 0.5 * second).astype(BF16)

    for op in COPIES:
        copy_of(op).wait_send()
    for b in range(2):
        sent = [tok_send(b, p, i) for p in range(2) for i in range(2)]
        sent += [back_send(b, p, i) for p in range(2) for i in range(2)]
        sent += [mate_send(b, n) for n in range(5)] + [half_send(b, n) for n in range(3)]
        for c in sent:
            c.wait_send()
    swap.wait_send()


def fused(
    tokens, pre_gain, first_gate, first_up, first_down, mix_gain, pool_weight,
    pool_scale, post_gain, second_gate, second_up, second_down,
):
    _, rows, half = tokens.shape
    depth, hid = first_gate.shape
    wide = 3 * hid // 10
    slim = hid // 2 - wide
    groups, width, out_cols = pool_weight.shape
    lanes = (3 * wide, 3 * slim + 128, 3 * wide, 3 * slim)

    vmem = pl.BlockSpec(memory_space=pltpu.VMEM)
    dma = pltpu.SemaphoreType.DMA
    out = pl.pallas_call(
        layer_kernel,
        out_shape=jax.ShapeDtypeStruct((rows, half), BF16),
        in_specs=[vmem] * 12,
        out_specs=vmem,
        scratch_shapes=[pltpu.VMEM((2, depth, n), BF16) for n in lanes]
        + [pltpu.VMEM((2, SIDE, SIDE, depth, n), BF16) for n in lanes]
        + [
            pltpu.VMEM((2, 2, 3 * rows, half), BF16),
            pltpu.VMEM((2, 3 * rows, half), BF16),
            pltpu.VMEM((2 * rows, 2 * wide), F32),
            pltpu.VMEM((2 * rows, 2 * slim), F32),
            pltpu.VMEM((2 * rows, wide), BF16),
            pltpu.VMEM((2 * rows, slim), BF16),
            pltpu.VMEM((2, 3 * rows, half), BF16),
            pltpu.VMEM((2, 3 * rows, half), BF16),
            pltpu.VMEM((3 * rows, half), F32),
            pltpu.VMEM((2, 2, rows, half), BF16),
            pltpu.VMEM((2, 2, rows, half), BF16),
            pltpu.VMEM((2, rows, 128), F32),
            dma((len(COPIES),)), dma((len(COPIES),)),
            dma((2, 2, 2)), dma((2, 2, 2)), dma((2, 5)), dma((2, 5)), dma((2, 3)), dma((2, 3)),
            dma((2, 2, 2)), dma((2, 2, 2)), dma((2,)),
        ],
        compiler_params=pltpu.CompilerParams(
            collective_id=0, has_side_effects=True, vmem_limit_bytes=60 * 1024 * 1024
        ),
    )(
        tokens.reshape(rows, half), pre_gain.reshape(1, -1), mix_gain.reshape(1, -1),
        pool_scale.reshape(1, -1), post_gain.reshape(1, -1),
        jnp.swapaxes(pool_weight, 1, 2).reshape(groups * out_cols, width),
        first_gate, first_up, first_down.T, second_gate, second_up, second_down.T,
    )
    return out.reshape(tokens.shape)


def solution(mesh):
    tok = P(("rep", "fs"), None, "tp")
    wide = P("fs", "tp")
    tall = P("tp", "fs")
    placed = (
        tok, P(), wide, wide, tall, P("tp"), P("tp", None, "fs"), P("tp"), P(), wide, wide, tall,
    )

    def layer(*args):
        return jax.shard_map(fused, mesh=mesh, in_specs=placed, out_specs=tok, check_vma=False)(*args)

    return layer
```

```python
import jax
import jax.numpy as jnp
from jax import lax
from jax.experimental import pallas as pl
from jax.experimental.pallas import tpu as pltpu
from jax.sharding import PartitionSpec as P

F32 = jnp.float32
BF16 = jnp.bfloat16
MESH = pl.DeviceIdType.MESH
GROUPS = 4
SIDE = 4
epsilon = 1e-06
NT = (((1,), (1,)), ((), ()))

PLAN = (
    (
        ("c", 1, 3), ("c", 0, 1), ("c", 1, 1), ("z", 0, 0, 0, 1), ("c", 0, 3), ("z", 1, 0, 0, 0), ("c", 1, 2),
        ("z", 3, 0, 0, 0), ("r", 1, 0, 0, 0), ("r", 1, 0, 0, 1), ("z", 2, 0, 0, 1), ("r", 0, 0, 0, 1),
        ("t", 1, 0), ("c", 0, 2),
    ),
    (
        ("z", 1, 3, 0, 1), ("z", 1, 1, 0, 0), ("r", 1, 0, 3, 1), ("r", 1, 0, 3, 0), ("r", 1, 0, 1, 1),
        ("t", 0, 0), ("r", 0, 0, 1, 1), ("z", 0, 1, 0, 1), ("z", 0, 3, 0, 0), ("r", 0, 1, 0, 0),
        ("r", 0, 0, 3, 1), ("r", 0, 0, 1, 0), ("r", 0, 1, 0, 1), ("r", 0, 0, 3, 0), ("t", 1, 1),
        ("z", 1, 2, 0, 0), ("r", 1, 0, 2, 1), ("f", 1, 0, 0, 1), ("z", 0, 2, 0, 0), ("r", 0, 0, 2, 0),
        ("z", 1, 3, 1, 1), ("f", 1, 0, 3, 0), ("z", 1, 3, 3, 1), ("r", 1, 1, 0, 0), ("z", 0, 1, 1, 1),
        ("r", 1, 0, 1, 0), ("r", 1, 0, 2, 0), ("z", 1, 1, 1, 0), ("f", 1, 0, 1, 1), ("r", 1, 1, 0, 1),
        ("t", 0, 1), ("z", 0, 3, 1, 0), ("f", 0, 0, 3, 1), ("r", 0, 0, 2, 1), ("z", 1, 2, 1, 0),
        ("f", 0, 0, 1, 0), ("r", 0, 0, 0, 0), ("c", 2, 3),
    ),
    (
        ("r", 0, 1, 2, 1), ("f", 0, 1, 0, 1), ("r", 0, 1, 2, 0), ("z", 1, 3, 2, 1), ("z", 0, 1, 3, 1),
        ("z", 0, 3, 3, 0), ("f", 1, 1, 0, 0), ("c", 3, 2), ("c", 3, 1), ("r", 2, 1, 0, 0), ("r", 2, 1, 0, 1),
        ("r", 2, 0, 0, 1), ("z", 1, 1, 3, 0), ("z", 0, 1, 2, 1), ("z", 0, 3, 2, 0), ("z", 1, 1, 2, 0),
        ("z", 1, 2, 3, 1), ("f", 1, 0, 2, 0), ("c", 3, 3),
    ),
    (
        ("f", 0, 0, 2, 1), ("f", 0, 0, 0, 0), ("c", 2, 2), ("c", 2, 1), ("z", 3, 2, 0, 1), ("z", 2, 3, 0, 0),
        ("r", 2, 0, 3, 0), ("r", 2, 0, 3, 1), ("r", 2, 0, 0, 0), ("z", 3, 1, 0, 0), ("r", 3, 0, 1, 1),
    ),
    (
        ("f", 0, 1, 2, 0), ("f", 2, 1, 0, 1), ("z", 1, 2, 2, 1), ("z", 3, 3, 0, 1), ("r", 3, 0, 3, 0),
        ("r", 3, 0, 1, 0), ("r", 3, 0, 3, 1), ("r", 3, 0, 0, 0), ("r", 3, 0, 2, 1), ("r", 3, 1, 0, 0),
        ("r", 3, 1, 0, 1),
    ),
    (
        ("z", 2, 3, 3, 0), ("f", 2, 0, 3, 1), ("z", 2, 3, 1, 0), ("r", 2, 0, 2, 0), ("z", 2, 2, 0, 1),
        ("r", 2, 0, 1, 1), ("r", 2, 0, 1, 0), ("z", 2, 1, 0, 1), ("r", 2, 0, 2, 1),
    ),
    (
        ("z", 3, 1, 1, 0), ("f", 3, 0, 3, 0), ("f", 3, 0, 1, 1), ("z", 3, 3, 3, 1),
    ),
    (
        ("z", 3, 1, 3, 0), ("z", 3, 3, 1, 1), ("r", 3, 0, 0, 1), ("r", 3, 1, 2, 1), ("z", 2, 2, 3, 0),
        ("f", 2, 0, 2, 0), ("f", 3, 1, 0, 0), ("r", 3, 0, 2, 0), ("r", 3, 1, 2, 0), ("z", 2, 1, 1, 1),
        ("f", 2, 0, 1, 0), ("f", 2, 0, 0, 0),
    ),
    (
        ("z", 3, 1, 2, 0), ("z", 3, 3, 2, 1), ("z", 2, 3, 2, 0), ("z", 2, 1, 3, 1), ("z", 2, 2, 1, 1),
    ),
    (
        ("z", 2, 2, 2, 0), ("f", 3, 0, 0, 1), ("f", 3, 1, 2, 1), ("f", 3, 0, 2, 0), ("z", 2, 1, 2, 1),
    ),
)

WAVES = [op for part in PLAN for op in part]
RING_SIDE = {(op[1], op[3]): op[4] for op in WAVES if op[0] == "f" and op[2] == 0}
RISE = {op[1:4]: op[4] for op in WAVES if op[0] == "z"}
COPIES = {op: i for i, op in enumerate(op for op in WAVES if op[0] != "t")}


def sources(op):
    kind, s = op[:2]
    if kind == "c" or kind == "t":
        return []
    if kind == "r":
        _, _, comp, j, _ = op
        if comp:
            return [("z", s, j, 0, RISE[s, j, 0])]
        return [("c", s, j)] if j else []
    if kind == "f":
        return [("r",) + op[1:]]
    _, _, j, c, _ = op
    if c == 0:
        return [("c", s, j)] if j else []
    if c == 2:
        return [("f", s, 0, j, RING_SIDE[s, j])]
    return [("r", s, 0, j, 0 if c == 3 else 1)]


def layer_kernel(
    tok_ref, pre_ref, mixg_ref, scale_ref, post_ref, pw_ref,
    g1_ref, u1_ref, d1_ref, g2_ref, u2_ref, d2_ref, out_ref,
    WS0, WS1, WS2, WS3, WB0, WB1, WB2, WB3, TB, N, ACC0, ACC1, H0, H1, PX, PR, PO, S, R, SQ,
    ws, wr, ts, tr, ms, mr, hs, hr, rs, rr, qs,
):
    rep = lax.axis_index("rep")
    fs = lax.axis_index("fs")
    t = lax.axis_index("tp")
    x = lax.rem(fs, SIDE)
    y = lax.rem(fs // SIDE, SIDE)
    low = fs // (SIDE * SIDE)
    z = 2 * rep + low
    other = 1 - t
    high = 1 - low

    def dev(dx, dy, dz, tt):
        xx = lax.rem(x + dx, SIDE)
        yy = lax.rem(y + dy, SIDE)
        zz = lax.rem(z + dz, SIDE)
        return {"rep": zz // 2, "fs": lax.rem(zz, 2) * (SIDE * SIDE) + yy * SIDE + xx, "tp": tt}

    mate = dev(0, 0, 0, other)
    along_x = {d: dev(d, 0, 0, t) for d in (1, 2, 3)}
    along_y = {d: dev(0, d, 0, t) for d in (1, 2, 3)}
    along_z = {d: dev(0, 0, d, t) for d in (1, 3)}
    peers = [mate] + list(along_x.values()) + list(along_y.values()) + list(along_z.values())

    barrier = pltpu.get_barrier_semaphore()
    for peer in peers:
        pl.semaphore_signal(barrier, inc=1, device_id=peer, device_id_type=MESH)

    def remote(src, dst, ss, sr, to):
        return pltpu.make_async_remote_copy(
            src_ref=src, dst_ref=dst, send_sem=ss, recv_sem=sr, device_id=to, device_id_type=MESH
        )

    rows, half = tok_ref.shape
    depth, hid = g1_ref.shape
    piece = rows // 2
    widths = (H0.shape[1], H1.shape[1])
    weights = ((g1_ref, u1_ref, d1_ref), (g2_ref, u2_ref, d2_ref))
    WS = (WS0, WS1, WS2, WS3)
    WB = (WB0, WB1, WB2, WB3)
    ACC = (ACC0, ACC1)
    H = (H0, H1)
    axes = (along_x, along_y)
    turn = (0, 1, 1, 0)
    places = (x, y)

    def slab(s, lo, j, c):
        a = lax.rem(places[turn[s]] + j, SIDE)
        c = lax.rem(places[1 - turn[s]] + c, SIDE)
        return WB[s].at[lo, c, a] if turn[s] == 0 else WB[s].at[lo, a, c]

    def pack(s):
        b, p = divmod(s, 2)
        n = widths[p]
        start = 2 * widths[0] * p
        for k in range(2):
            for i, w in enumerate(weights[b]):
                WS[s][k, :, i * n:(i + 1) * n] = w[:, start + k * n:start + (k + 1) * n]
            if s == 1:
                flat = pw_ref[...]
                for i in range(2):
                    WS[s][k, i * 16:(i + 1) * 16, 3 * n:] = flat[:, i * 128:(i + 1) * 128]
        WB[s][low, y, x] = WS[s][lax.rem(places[turn[s]], 2)]

    def copy_of(op):
        kind = op[0]
        if kind == "t":
            return tok_send(0, op[1], op[2])
        s = op[1]
        axis, ring = axes[turn[s]], axes[1 - turn[s]]
        sems = (ws.at[COPIES[op]], wr.at[COPIES[op]])
        if kind == "c":
            d = SIDE - op[2]
            src = WS[s].at[lax.rem(places[turn[s]] + d, 2)]
            return remote(src, slab(s, low, 0, 0), *sems, axis[d])
        if kind == "r":
            _, _, comp, j, side = op
            ref = slab(s, high if comp else low, j, 0)
            return remote(ref, ref, *sems, ring[(1, 3)[side]])
        if kind == "f":
            _, _, comp, j, side = op
            ref = slab(s, high if comp else low, j, (3, 1)[side])
            return remote(ref, ref, *sems, ring[(1, 3)[side]])
        _, _, j, c, up = op
        ref = slab(s, low, j, c)
        return remote(ref, ref, *sems, along_z[1 if up else 3])

    here = set()

    def need(op):
        if op not in here:
            here.add(op)
            copy_of(op).wait_recv()

    def issue(part):
        for op in PLAN[part]:
            for source in sources(op):
                need(source)
            copy_of(op).start()

    def base(p):
        return rows * (1 + p)

    own = slice(0, rows)
    foreign = tuple(slice(base(p), base(p) + rows) for p in range(2))

    def axis_of(b, p):
        return axes[turn[2 * b + p]]

    def tok_send(b, p, i):
        src = TB.at[b, t, i * piece:(i + 1) * piece]
        dst = TB.at[b, t, base(p) + i * piece:base(p) + (i + 1) * piece]
        return remote(src, dst, ts.at[b, p, i], tr.at[b, p, i], axis_of(b, p)[(1, 3)[i]])

    def mate_send(b, n):
        cut = own if n == 4 else slice(rows + n * piece, rows + (n + 1) * piece)
        ref = TB.at[b, t, cut]
        return remote(ref, ref, ms.at[b, n], mr.at[b, n], mate)

    def half_send(b, n):
        cut = own if n == 2 else foreign[n]
        return remote(PX.at[b, cut], PR.at[b, cut], hs.at[b, n], hr.at[b, n], mate)

    def back_send(b, p, i):
        cut = slice(i * piece, (i + 1) * piece)
        return remote(
            S.at[b, p, cut], R.at[b, p, cut], rs.at[b, p, i], rr.at[b, p, i], axis_of(b, p)[(3, 1)[i]]
        )

    def norm_rows(b, cut, gain_ref):
        parts = [TB[b, c, cut].astype(F32) for c in range(2)]
        total = sum(jnp.sum(v * v, axis=-1, keepdims=True) for v in parts)
        inv = lax.rsqrt(total / (2 * half) + epsilon)
        for c in range(2):
            N[c, cut] = (parts[c] * inv * gain_ref[0:1, c * half:(c + 1) * half]).astype(BF16)

    def gate_up(b, p, lo, fresh, cut):
        n = 2 * widths[p]
        wide = WB[2 * b + p][lo, :, :, :, 0:n].reshape(half, n)
        value = jnp.dot(N[lo, cut], wide, preferred_element_type=F32)
        at = own if cut is own else slice(rows, 2 * rows)
        if fresh:
            ACC[p][at] = value
        else:
            ACC[p][at] += value

    def hidden(p, cut):
        at = own if cut is own else slice(rows, 2 * rows)
        n = widths[p]
        H[p][at] = (jax.nn.silu(ACC[p][at, 0:n]) * ACC[p][at, n:2 * n]).astype(BF16)

    def down(b, p, cut, lo):
        at = own if cut is own else slice(rows, 2 * rows)
        n = widths[p]
        tall = WB[2 * b + p][lo, :, :, :, 2 * n:3 * n].reshape(half, n)
        return lax.dot_general(H[p][at], tall, NT, preferred_element_type=F32)

    def project(b, last, gaps):
        for p in range(2):
            cut = foreign[p]
            gate_up(b, p, last, False, cut)
            hidden(p, cut)
            PX[b, cut] = down(b, p, cut, other).astype(BF16)
            half_send(b, p).start()
            PO[cut] = down(b, p, cut, t)
        gaps[0]()
        for p in range(2):
            cut = foreign[p]
            half_send(b, p).wait_recv()
            S[b, p] = (PO[cut] + PR[b, cut].astype(F32)).astype(BF16)
            for i in range(2):
                back_send(b, p, i).start()
        for p in range(2):
            gate_up(b, p, last, False, own)
            hidden(p, own)
        PX[b, own] = (down(b, 0, own, other) + down(b, 1, own, other)).astype(BF16)
        half_send(b, 2).start()
        gaps[1]()
        PO[own] = down(b, 0, own, t) + down(b, 1, own, t)
        gaps[2]()
        half_send(b, 2).wait_recv()
        total = PO[own] + PR[b, own].astype(F32)
        for p in range(2):
            for i in range(2):
                back_send(b, p, i).wait_recv()
            total = total + R[b, p].astype(F32)
        return total

    def all_of(b):
        return [op for op in COPIES if op[1] // 2 == b]

    def first_half(op):
        return op[0] == "c" or (op[0] in "rf" and op[2] == 0)

    TB[0, t, own] = tok_ref[...]
    for s in range(4):
        pack(s)
    pl.semaphore_wait(barrier, len(peers))

    issue(0)
    mate_send(0, 4).start()
    mate_send(0, 4).wait_recv()
    norm_rows(0, own, pre_ref)
    issue(1)
    issue(2)
    for p in range(2):
        for i in range(2):
            tok_send(0, p, i).wait_recv()
            mate_send(0, 2 * p + i).start()
    issue(3)
    for p in range(2):
        for i in range(2):
            mate_send(0, 2 * p + i).wait_recv()
        norm_rows(0, foreign[p], pre_ref)
    issue(4)
    for op in all_of(0):
        if first_half(op):
            need(op)
    for p in range(2):
        gate_up(0, p, low, True, foreign[p])
        gate_up(0, p, low, True, own)
    issue(5)
    for op in all_of(0):
        need(op)
    first = project(0, high, [lambda: issue(6), lambda: issue(7), lambda: issue(8)])

    after_first = (tok_ref[...].astype(F32) + 0.5 * first).astype(BF16).astype(F32)
    square = after_first * after_first
    SQ[0] = sum(square[:, i * 128:(i + 1) * 128] for i in range(half // 128))
    swap = remote(SQ.at[0], SQ.at[1], qs.at[0], qs.at[1], mate)
    swap.start()
    swap.wait_recv()
    total = jnp.sum(SQ[0] + SQ[1], axis=-1, keepdims=True)
    h = (after_first * lax.rsqrt(total / (2 * half) + epsilon) * mixg_ref[0:1, :]).astype(BF16).astype(F32)
    groups_here = 2
    width = half // groups_here

    def shifted(v, by):
        spot_ids = lax.broadcasted_iota(jnp.int32, v.shape, 0)
        return jnp.where(spot_ids >= by, pltpu.roll(v, by, 0), 0.0)

    maps = WB1[:, :, :, :, 3 * widths[1]:].reshape(2 * SIDE * SIDE, depth, 128).astype(F32)
    maps = maps.reshape(2 * SIDE * SIDE, 4, 8, 128)
    for g in range(groups_here):
        hg = h[:, g * width:(g + 1) * width]
        run = hg + shifted(hg, 1)
        window = 2
        found = run
        number = t * groups_here + g
        reached = jnp.int32(2)
        for level in range(1, GROUPS):
            run = run + shifted(run, window)
            window = window * 2
            found = jnp.where(number >= level, run, found)
            reached = jnp.where(number >= level, window, reached)
        counts = jnp.minimum(lax.broadcasted_iota(jnp.int32, (rows, width), 0) + 1, reached).astype(F32)
        diff = (found / counts - hg).astype(BF16)
        turned = jnp.concatenate(
            [maps[:, g].reshape(width, 128), maps[:, 2 + g].reshape(width, 128)], axis=1
        ).astype(BF16)
        mixed = lax.dot_general(diff, turned, NT, preferred_element_type=F32)
        at = slice(g * width, (g + 1) * width)
        TB[1, t, own, at] = (after_first[:, at] + scale_ref[0:1, at] * mixed).astype(BF16)

    for p in range(2):
        for i in range(2):
            tok_send(1, p, i).start()
    mate_send(1, 4).start()
    mate_send(1, 4).wait_recv()
    norm_rows(1, own, post_ref)
    issue(9)
    for p in range(2):
        for i in range(2):
            tok_send(1, p, i).wait_recv()
            mate_send(1, 2 * p + i).start()
    for op in all_of(1):
        if first_half(op):
            need(op)
    for p in range(2):
        gate_up(1, p, low, True, own)
    for p in range(2):
        for i in range(2):
            mate_send(1, 2 * p + i).wait_recv()
        norm_rows(1, foreign[p], post_ref)
        gate_up(1, p, low, True, foreign[p])
    for op in all_of(1):
        need(op)
    second = project(1, high, [lambda: None] * 3)
    out_ref[...] = (TB[1, t, own].astype(F32) + 0.5 * second).astype(BF16)

    for op in COPIES:
        copy_of(op).wait_send()
    for b in range(2):
        sent = [tok_send(b, p, i) for p in range(2) for i in range(2)]
        sent += [back_send(b, p, i) for p in range(2) for i in range(2)]
        sent += [mate_send(b, n) for n in range(5)] + [half_send(b, n) for n in range(3)]
        for c in sent:
            c.wait_send()
    swap.wait_send()


def fused(
    tokens, pre_gain, first_gate, first_up, first_down, mix_gain, pool_weight,
    pool_scale, post_gain, second_gate, second_up, second_down,
):
    _, rows, half = tokens.shape
    depth, hid = first_gate.shape
    wide = 3 * hid // 10
    slim = hid // 2 - wide
    groups, width, out_cols = pool_weight.shape
    lanes = (3 * wide, 3 * slim + 128, 3 * wide, 3 * slim)

    vmem = pl.BlockSpec(memory_space=pltpu.VMEM)
    dma = pltpu.SemaphoreType.DMA
    out = pl.pallas_call(
        layer_kernel,
        out_shape=jax.ShapeDtypeStruct((rows, half), BF16),
        in_specs=[vmem] * 12,
        out_specs=vmem,
        scratch_shapes=[pltpu.VMEM((2, depth, n), BF16) for n in lanes]
        + [pltpu.VMEM((2, SIDE, SIDE, depth, n), BF16) for n in lanes]
        + [
            pltpu.VMEM((2, 2, 3 * rows, half), BF16),
            pltpu.VMEM((2, 3 * rows, half), BF16),
            pltpu.VMEM((2 * rows, 2 * wide), F32),
            pltpu.VMEM((2 * rows, 2 * slim), F32),
            pltpu.VMEM((2 * rows, wide), BF16),
            pltpu.VMEM((2 * rows, slim), BF16),
            pltpu.VMEM((2, 3 * rows, half), BF16),
            pltpu.VMEM((2, 3 * rows, half), BF16),
            pltpu.VMEM((3 * rows, half), F32),
            pltpu.VMEM((2, 2, rows, half), BF16),
            pltpu.VMEM((2, 2, rows, half), BF16),
            pltpu.VMEM((2, rows, 128), F32),
            dma((len(COPIES),)), dma((len(COPIES),)),
            dma((2, 2, 2)), dma((2, 2, 2)), dma((2, 5)), dma((2, 5)), dma((2, 3)), dma((2, 3)),
            dma((2, 2, 2)), dma((2, 2, 2)), dma((2,)),
        ],
        compiler_params=pltpu.CompilerParams(
            collective_id=0, has_side_effects=True, vmem_limit_bytes=60 * 1024 * 1024
        ),
    )(
        tokens.reshape(rows, half), pre_gain.reshape(1, -1), mix_gain.reshape(1, -1),
        pool_scale.reshape(1, -1), post_gain.reshape(1, -1),
        jnp.swapaxes(pool_weight, 1, 2).reshape(groups * out_cols, width),
        first_gate, first_up, first_down.T, second_gate, second_up, second_down.T,
    )
    return out.reshape(tokens.shape)


def solution(mesh):
    tok = P(("rep", "fs"), None, "tp")
    wide = P("fs", "tp")
    tall = P("tp", "fs")
    placed = (
        tok, P(), wide, wide, tall, P("tp"), P("tp", None, "fs"), P("tp"), P(), wide, wide, tall,
    )

    def layer(*args):
        return jax.shard_map(fused, mesh=mesh, in_specs=placed, out_specs=tok, check_vma=False)(*args)

    return layer
```

```python
import jax
import jax.numpy as jnp
from jax import lax
from jax.experimental import pallas as pl
from jax.experimental.pallas import tpu as pltpu
from jax.sharding import PartitionSpec as P

F32 = jnp.float32
BF16 = jnp.bfloat16
MESH = pl.DeviceIdType.MESH
GROUPS = 4
SIDE = 4
epsilon = 1e-06
NT = (((1,), (1,)), ((), ()))

PLAN = (
    (
        ("c", 1, 3), ("c", 0, 1), ("c", 1, 1), ("z", 0, 0, 0, 1), ("c", 0, 3), ("z", 1, 0, 0, 0), ("c", 1, 2),
        ("z", 3, 0, 0, 0), ("r", 1, 0, 0, 0), ("r", 1, 0, 0, 1), ("z", 2, 0, 0, 1), ("r", 0, 0, 0, 1),
        ("t", 1, 0), ("c", 0, 2),
    ),
    (
        ("z", 1, 3, 0, 1), ("z", 1, 1, 0, 0), ("r", 1, 0, 3, 1), ("r", 1, 0, 3, 0), ("r", 1, 0, 1, 1),
        ("t", 0, 0), ("r", 0, 0, 1, 1), ("z", 0, 1, 0, 1), ("z", 0, 3, 0, 0), ("r", 0, 1, 0, 0),
        ("r", 0, 0, 3, 1), ("r", 0, 0, 1, 0), ("r", 0, 1, 0, 1), ("r", 0, 0, 3, 0), ("t", 1, 1),
        ("z", 1, 2, 0, 0), ("r", 1, 0, 2, 1), ("f", 1, 0, 0, 1), ("z", 0, 2, 0, 0), ("r", 0, 0, 2, 0),
        ("z", 1, 3, 1, 1), ("f", 1, 0, 3, 0), ("z", 1, 3, 3, 1), ("r", 1, 1, 0, 0), ("z", 0, 1, 1, 1),
        ("r", 1, 0, 1, 0), ("r", 1, 0, 2, 0), ("z", 1, 1, 1, 0), ("f", 1, 0, 1, 1), ("r", 1, 1, 0, 1),
        ("t", 0, 1), ("z", 0, 3, 1, 0), ("f", 0, 0, 3, 1), ("r", 0, 0, 2, 1), ("z", 1, 2, 1, 0),
        ("f", 0, 0, 1, 0), ("r", 0, 0, 0, 0), ("c", 2, 3),
    ),
    (
        ("r", 0, 1, 2, 1), ("f", 0, 1, 0, 1), ("r", 0, 1, 2, 0), ("z", 1, 3, 2, 1), ("z", 0, 1, 3, 1),
        ("z", 0, 3, 3, 0), ("f", 1, 1, 0, 0), ("c", 3, 2), ("c", 3, 1), ("r", 2, 1, 0, 0), ("r", 2, 1, 0, 1),
        ("r", 2, 0, 0, 1), ("z", 1, 1, 3, 0), ("z", 0, 1, 2, 1), ("z", 0, 3, 2, 0), ("z", 1, 1, 2, 0),
        ("z", 1, 2, 3, 1), ("f", 1, 0, 2, 0), ("c", 3, 3),
    ),
    (
        ("f", 0, 0, 2, 1), ("f", 0, 0, 0, 0), ("c", 2, 2), ("c", 2, 1), ("z", 3, 2, 0, 1), ("z", 2, 3, 0, 0),
        ("r", 2, 0, 3, 0), ("r", 2, 0, 3, 1), ("r", 2, 0, 0, 0), ("z", 3, 1, 0, 0), ("r", 3, 0, 1, 1),
    ),
    (
        ("f", 0, 1, 2, 0), ("f", 2, 1, 0, 1), ("z", 1, 2, 2, 1), ("z", 3, 3, 0, 1), ("r", 3, 0, 3, 0),
        ("r", 3, 0, 1, 0), ("r", 3, 0, 3, 1), ("r", 3, 0, 0, 0), ("r", 3, 0, 2, 1), ("r", 3, 1, 0, 0),
        ("r", 3, 1, 0, 1),
    ),
    (
        ("z", 2, 3, 3, 0), ("f", 2, 0, 3, 1), ("z", 2, 3, 1, 0), ("r", 2, 0, 2, 0), ("z", 2, 2, 0, 1),
        ("r", 2, 0, 1, 1), ("r", 2, 0, 1, 0), ("z", 2, 1, 0, 1), ("r", 2, 0, 2, 1),
    ),
    (
        ("z", 3, 1, 1, 0), ("f", 3, 0, 3, 0), ("f", 3, 0, 1, 1), ("z", 3, 3, 3, 1),
    ),
    (
        ("z", 3, 1, 3, 0), ("z", 3, 3, 1, 1), ("r", 3, 0, 0, 1), ("r", 3, 1, 2, 1), ("z", 2, 2, 3, 0),
        ("f", 2, 0, 2, 0), ("f", 3, 1, 0, 0), ("r", 3, 0, 2, 0), ("r", 3, 1, 2, 0), ("z", 2, 1, 1, 1),
        ("f", 2, 0, 1, 0), ("f", 2, 0, 0, 0),
    ),
    (
        ("z", 3, 1, 2, 0), ("z", 3, 3, 2, 1), ("z", 2, 3, 2, 0), ("z", 2, 1, 3, 1), ("z", 2, 2, 1, 1),
    ),
    (
        ("z", 2, 2, 2, 0), ("f", 3, 0, 0, 1), ("f", 3, 1, 2, 1), ("f", 3, 0, 2, 0), ("z", 2, 1, 2, 1),
    ),
)

WAVES = [op for part in PLAN for op in part]
RING_SIDE = {(op[1], op[3]): op[4] for op in WAVES if op[0] == "f" and op[2] == 0}
RISE = {op[1:4]: op[4] for op in WAVES if op[0] == "z"}
def sources(op):
    kind, s = op[:2]
    if kind == "c" or kind == "t":
        return []
    if kind == "r":
        _, _, comp, j, _ = op
        if comp:
            return [("z", s, j, 0, RISE[s, j, 0])]
        return [("c", s, j)] if j else []
    if kind == "f":
        return [("r",) + op[1:]]
    _, _, j, c, _ = op
    if c == 0:
        return [("c", s, j)] if j else []
    if c == 2:
        return [("f", s, 0, j, RING_SIDE[s, j])]
    return [("r", s, 0, j, 0 if c == 3 else 1)]


def own_rows(op):
    return op[0] == "c" or (op[0] in "rf" and op[2] == 0)


COPIES = [op for op in WAVES if op[0] != "t"]
WANTED = {source for op in COPIES for source in sources(op)}


def arrival(op):
    return op if op in WANTED else ("low" if own_rows(op) else "high", op[1])


ARRIVALS = {key: i for i, key in enumerate(dict.fromkeys(arrival(op) for op in COPIES))}


def layer_kernel(
    tok_hbm, pre_hbm, mixg_hbm, scale_hbm, post_hbm, pw_hbm,
    g1_hbm, u1_hbm, d1_hbm, g2_hbm, u2_hbm, d2_hbm, out_ref,
    wide_gain, slim_gain, pw_ref, own_w,
    WS0, WS1, WS2, WS3, WB0, WB1, WB2, WB3, TB, N, ACC0, ACC1, H0, H1, PX, PR, PO, S, R, SQ, TM, RC,
    ls, ws, wr, ts, tr, ms, mr, hs, hr, rs, rr, qs,
):
    rep = lax.axis_index("rep")
    fs = lax.axis_index("fs")
    t = lax.axis_index("tp")
    x = lax.rem(fs, SIDE)
    y = lax.rem(fs // SIDE, SIDE)
    low = fs // (SIDE * SIDE)
    z = 2 * rep + low
    other = 1 - t
    high = 1 - low

    def dev(dx, dy, dz, tt):
        xx = lax.rem(x + dx, SIDE)
        yy = lax.rem(y + dy, SIDE)
        zz = lax.rem(z + dz, SIDE)
        return {"rep": zz // 2, "fs": lax.rem(zz, 2) * (SIDE * SIDE) + yy * SIDE + xx, "tp": tt}

    mate = dev(0, 0, 0, other)
    along_x = {d: dev(d, 0, 0, t) for d in (1, 2, 3)}
    along_y = {d: dev(0, d, 0, t) for d in (1, 2, 3)}
    along_z = {d: dev(0, 0, d, t) for d in (1, 3)}
    peers = [mate] + list(along_x.values()) + list(along_y.values()) + list(along_z.values())

    barrier = pltpu.get_barrier_semaphore()
    for peer in peers:
        pl.semaphore_signal(barrier, inc=1, device_id=peer, device_id_type=MESH)

    rows, half = out_ref.shape
    def remote(src, dst, ss, sr, to):
        return pltpu.make_async_remote_copy(
            src_ref=src, dst_ref=dst, send_sem=ss, recv_sem=sr, device_id=to, device_id_type=MESH
        )

    depth, hid = g1_hbm.shape
    loads = [
        pltpu.make_async_copy(src, dst, ls.at[i])
        for i, src, dst in (
            (0, g1_hbm, own_w.at[0, 0]), (0, u1_hbm, own_w.at[0, 1]), (0, d1_hbm, own_w.at[0, 2]),
            (1, pw_hbm, pw_ref), (2, tok_hbm, TB.at[0, t, 0:rows]),
            (3, g2_hbm, own_w.at[1, 0]), (3, u2_hbm, own_w.at[1, 1]), (3, d2_hbm, own_w.at[1, 2]),
            (4, pre_hbm, wide_gain.at[0:1]), (4, post_hbm, wide_gain.at[1:2]),
            (5, mixg_hbm, slim_gain.at[0:1]), (5, scale_hbm, slim_gain.at[1:2]),
        )
    ]
    for load in loads:
        load.start()

    def loaded(i, ref):
        pltpu.make_async_copy(ref, ref, ls.at[i]).wait()

    piece = rows // 2
    widths = (H0.shape[1], H1.shape[1])
    WS = (WS0, WS1, WS2, WS3)
    WB = (WB0, WB1, WB2, WB3)
    ACC = (ACC0, ACC1)
    H = (H0, H1)
    axes = (along_x, along_y)
    turn = (0, 1, 1, 0)
    places = (x, y)

    def slab(s, lo, j, c):
        a = lax.rem(places[turn[s]] + j, SIDE)
        c = lax.rem(places[1 - turn[s]] + c, SIDE)
        yy, xx = (c, a) if turn[s] == 0 else (a, c)
        start = ((lo * SIDE + yy) * SIDE + xx) * depth
        return WB[s].at[pl.ds(pl.multiple_of(start, depth), depth)]

    def side_of(s, lo, lanes):
        return WB[s][pl.ds(pl.multiple_of(lo * half, half), half), lanes]

    def pack(s):
        b, p = divmod(s, 2)
        n = widths[p]
        start = 2 * widths[0] * p
        for k in range(2):
            for i in range(3):
                WS[s][k, :, i * n:(i + 1) * n] = own_w[b, i, :, start + k * n:start + (k + 1) * n]
            if s == 1:
                flat = pw_ref[...]
                for i in range(2):
                    WS[s][k, i * 16:(i + 1) * 16, 3 * n:] = flat[:, i * 128:(i + 1) * 128]
        start = ((low * SIDE + y) * SIDE + x) * depth
        WB[s][pl.ds(pl.multiple_of(start, depth), depth)] = WS[s][lax.rem(places[turn[s]], 2)]

    def copy_of(op):
        kind = op[0]
        if kind == "t":
            return tok_send(0, op[1], op[2])
        s = op[1]
        axis, ring = axes[turn[s]], axes[1 - turn[s]]
        sems = (ws.at[s], wr.at[ARRIVALS[arrival(op)]])
        if kind == "c":
            d = SIDE - op[2]
            src = WS[s].at[lax.rem(places[turn[s]] + d, 2)]
            return remote(src, slab(s, low, 0, 0), *sems, axis[d])
        if kind == "r":
            _, _, comp, j, side = op
            ref = slab(s, high if comp else low, j, 0)
            return remote(ref, ref, *sems, ring[(1, 3)[side]])
        if kind == "f":
            _, _, comp, j, side = op
            ref = slab(s, high if comp else low, j, (3, 1)[side])
            return remote(ref, ref, *sems, ring[(1, 3)[side]])
        _, _, j, c, up = op
        ref = slab(s, low, j, c)
        return remote(ref, ref, *sems, along_z[1 if up else 3])

    here = set()

    def need(op):
        if op not in here:
            here.add(op)
            copy_of(op).wait_recv()

    def issue(part):
        for op in PLAN[part]:
            for source in sources(op):
                need(source)
            copy_of(op).start()

    def base(p):
        return rows * (1 + p)

    own = slice(0, rows)
    foreign = tuple(slice(base(p), base(p) + rows) for p in range(2))

    def axis_of(b, p):
        return axes[turn[2 * b + p]]

    def tok_send(b, p, i):
        src = TB.at[b, t, i * piece:(i + 1) * piece]
        dst = TB.at[b, t, base(p) + i * piece:base(p) + (i + 1) * piece]
        return remote(src, dst, ts.at[b], tr.at[b, p], axis_of(b, p)[(1, 3)[i]])

    def tok_here(b, p):
        ref = TB.at[b, t, foreign[p]]
        remote(ref, ref, ts.at[b], tr.at[b, p], mate).wait_recv()

    def mate_send(b, n):
        ref = TB.at[b, t, own if n == 2 else foreign[n]]
        return remote(ref, ref, ms.at[b], mr.at[b, n], mate)

    def half_send(b, n):
        cut = own if n == 2 else foreign[n]
        return remote(PX.at[b, cut], PR.at[b, cut], hs.at[b], hr.at[b, n], mate)

    def back_send(b, p, i):
        cut = slice(i * piece, (i + 1) * piece)
        return remote(S.at[b, p, cut], R.at[b, p, cut], rs.at[b], rr.at[b, p], axis_of(b, p)[(3, 1)[i]])

    def back_here(b, p):
        remote(S.at[b, p], R.at[b, p], rs.at[b], rr.at[b, p], mate).wait_recv()

    def norm_rows(b, cut):
        parts = [TB[b, c, cut].astype(F32) for c in range(2)]
        total = sum(jnp.sum(v * v, axis=-1, keepdims=True) for v in parts)
        inv = lax.rsqrt(total / (2 * half) + epsilon)
        for c in range(2):
            N[c, cut] = (parts[c] * inv * wide_gain[b:b + 1, c * half:(c + 1) * half]).astype(BF16)

    def gate_up(b, p, lo, fresh, cut):
        n = 2 * widths[p]
        wide = side_of(2 * b + p, lo, slice(0, n))
        value = jnp.dot(N[lo, cut], wide, preferred_element_type=F32)
        at = own if cut is own else slice(rows, 2 * rows)
        if fresh:
            ACC[p][at] = value
        else:
            ACC[p][at] += value

    def hidden(p, cut):
        at = own if cut is own else slice(rows, 2 * rows)
        n = widths[p]
        H[p][at] = (jax.nn.silu(ACC[p][at, 0:n]) * ACC[p][at, n:2 * n]).astype(BF16)

    def down(b, p, cut, lo):
        at = own if cut is own else slice(rows, 2 * rows)
        n = widths[p]
        tall = side_of(2 * b + p, lo, slice(2 * n, 3 * n))
        return lax.dot_general(H[p][at], tall, NT, preferred_element_type=F32)

    def project(b, last, gaps):
        for p in range(2):
            cut = foreign[p]
            gate_up(b, p, last, False, cut)
            hidden(p, cut)
            PX[b, cut] = down(b, p, cut, other).astype(BF16)
            half_send(b, p).start()
        for p in range(2):
            PO[foreign[p]] = down(b, p, foreign[p], t)
        gaps[0]()
        for p in range(2):
            cut = foreign[p]
            half_send(b, p).wait_recv()
            S[b, p] = (PO[cut] + PR[b, cut].astype(F32)).astype(BF16)
            for i in range(2):
                back_send(b, p, i).start()
        for p in range(2):
            gate_up(b, p, last, False, own)
            hidden(p, own)
        PX[b, own] = (down(b, 0, own, other) + down(b, 1, own, other)).astype(BF16)
        half_send(b, 2).start()
        gaps[1]()
        PO[own] = down(b, 0, own, t) + down(b, 1, own, t)
        gaps[2]()
        half_send(b, 2).wait_recv()
        total = PO[own] + PR[b, own].astype(F32)
        for p in range(2):
            back_here(b, p)
            total = total + R[b, p].astype(F32)
        return total

    groups_here = 2
    width = half // groups_here

    def ready_pool():
        issue(8)
        maps = WB1[:, 3 * widths[1]:].reshape(2 * SIDE * SIDE, depth, 128).astype(F32)
        maps = maps.reshape(2 * SIDE * SIDE, 4, 8, 128)
        for g in range(groups_here):
            TM[g] = jnp.concatenate(
                [maps[:, g].reshape(width, 128), maps[:, 2 + g].reshape(width, 128)], axis=1
            ).astype(BF16)
            reached = 2 * 2 ** g * jnp.where(t == 0, 1, 2 ** groups_here)
            ages = lax.broadcasted_iota(jnp.int32, (rows, 128), 0) + 1
            RC[g] = 1.0 / jnp.minimum(ages, reached).astype(F32)

    def slabs(s, n):
        ref = WB[s].at[0:n * depth]
        return lambda key: remote(ref, ref, ws.at[s], wr.at[ARRIVALS[key]], mate)

    def need_all(b, mine):
        for op in COPIES:
            if op[1] // 2 == b and own_rows(op) == mine and op in WANTED:
                need(op)
        for s in (2 * b, 2 * b + 1):
            key = ("low" if mine else "high", s)
            n = sum(arrival(op) == key for op in COPIES)
            if n:
                slabs(s, n)(key).wait_recv()

    loaded(0, own_w.at[0])
    loaded(1, pw_ref)
    pack(0)
    pack(1)
    loaded(3, own_w.at[1])
    pack(2)
    pack(3)
    loaded(2, TB.at[0, t, own])
    loaded(4, wide_gain)
    loaded(5, slim_gain)
    pl.semaphore_wait(barrier, len(peers))

    issue(0)
    mate_send(0, 2).start()
    mate_send(0, 2).wait_recv()
    norm_rows(0, own)
    issue(1)
    issue(2)
    for p in range(2):
        tok_here(0, p)
        mate_send(0, p).start()
    issue(3)
    for p in range(2):
        mate_send(0, p).wait_recv()
        norm_rows(0, foreign[p])
    issue(4)
    need_all(0, True)
    for p in range(2):
        gate_up(0, p, low, True, foreign[p])
        gate_up(0, p, low, True, own)
    issue(5)
    need_all(0, False)
    first = project(0, high, [lambda: issue(6), lambda: issue(7), ready_pool])

    after_first = (TB[0, t, own].astype(F32) + 0.5 * first).astype(BF16).astype(F32)
    square = after_first * after_first
    SQ[0] = sum(square[:, i * 128:(i + 1) * 128] for i in range(half // 128))
    swap = remote(SQ.at[0], SQ.at[1], qs.at[0], qs.at[1], mate)
    swap.start()
    swap.wait_recv()
    total = jnp.sum(SQ[0] + SQ[1], axis=-1, keepdims=True)
    h = (after_first * lax.rsqrt(total / (2 * half) + epsilon) * slim_gain[0:1, :]).astype(BF16).astype(F32)

    def shifted(v, by):
        spot_ids = lax.broadcasted_iota(jnp.int32, v.shape, 0)
        return jnp.where(spot_ids >= by, pltpu.roll(v, by, 0), 0.0)

    for g in range(groups_here):
        hg = h[:, g * width:(g + 1) * width]
        run = hg + shifted(hg, 1)
        window = 2
        found = run
        number = t * groups_here + g
        for level in range(1, GROUPS):
            run = run + shifted(run, window)
            window = window * 2
            found = jnp.where(number >= level, run, found)
        share = jnp.concatenate([RC[g]] * (width // 128), axis=1)
        diff = (found * share - hg).astype(BF16)
        mixed = lax.dot_general(diff, TM[g], NT, preferred_element_type=F32)
        at = slice(g * width, (g + 1) * width)
        TB[1, t, own, at] = (after_first[:, at] + slim_gain[1:2, at] * mixed).astype(BF16)

    for p in range(2):
        for i in range(2):
            tok_send(1, p, i).start()
    mate_send(1, 2).start()
    mate_send(1, 2).wait_recv()
    norm_rows(1, own)
    issue(9)
    for p in range(2):
        tok_here(1, p)
        mate_send(1, p).start()
    need_all(1, True)
    for p in range(2):
        gate_up(1, p, low, True, own)
    for p in range(2):
        mate_send(1, p).wait_recv()
        norm_rows(1, foreign[p])
        gate_up(1, p, low, True, foreign[p])
    need_all(1, False)
    second = project(1, high, [lambda: None] * 3)
    out_ref[...] = (TB[1, t, own].astype(F32) + 0.5 * second).astype(BF16)

    for s in range(4):
        n = sum(op[1] == s for op in COPIES)
        ref = WB[s].at[0:n * depth]
        remote(ref, ref, ws.at[s], wr.at[0], mate).wait_send()
    for b in range(2):
        remote(S.at[b], R.at[b], ts.at[b], tr.at[b, 0], mate).wait_send()
        remote(S.at[b], R.at[b], rs.at[b], rr.at[b, 0], mate).wait_send()
        remote(PX.at[b], PR.at[b], ms.at[b], mr.at[b, 0], mate).wait_send()
        remote(PX.at[b], PR.at[b], hs.at[b], hr.at[b, 0], mate).wait_send()
    swap.wait_send()


def fused(
    tokens, pre_gain, first_gate, first_up, first_down, mix_gain, pool_weight,
    pool_scale, post_gain, second_gate, second_up, second_down,
):
    _, rows, half = tokens.shape
    depth, hid = first_gate.shape
    wide = 3 * hid // 10
    slim = hid // 2 - wide
    groups, width, out_cols = pool_weight.shape
    lanes = (3 * wide, 3 * slim + 128, 3 * wide, 3 * slim)

    vmem = pl.BlockSpec(memory_space=pltpu.VMEM)
    anyw = pl.BlockSpec(memory_space=pl.ANY)
    dma = pltpu.SemaphoreType.DMA
    out = pl.pallas_call(
        layer_kernel,
        out_shape=jax.ShapeDtypeStruct((rows, half), BF16),
        in_specs=[anyw] * 12,
        out_specs=vmem,
        scratch_shapes=[
            pltpu.VMEM((2, 2 * half), F32),
            pltpu.VMEM((2, half), F32),
            pltpu.VMEM((groups * out_cols, width), BF16),
            pltpu.VMEM((2, 3, depth, hid), BF16),
        ]
        + [pltpu.VMEM((2, depth, n), BF16) for n in lanes]
        + [pltpu.VMEM((2 * half, n), BF16) for n in lanes]
        + [
            pltpu.VMEM((2, 2, 3 * rows, half), BF16),
            pltpu.VMEM((2, 3 * rows, half), BF16),
            pltpu.VMEM((2 * rows, 2 * wide), F32),
            pltpu.VMEM((2 * rows, 2 * slim), F32),
            pltpu.VMEM((2 * rows, wide), BF16),
            pltpu.VMEM((2 * rows, slim), BF16),
            pltpu.VMEM((2, 3 * rows, half), BF16),
            pltpu.VMEM((2, 3 * rows, half), BF16),
            pltpu.VMEM((3 * rows, half), F32),
            pltpu.VMEM((2, 2, rows, half), BF16),
            pltpu.VMEM((2, 2, rows, half), BF16),
            pltpu.VMEM((2, rows, 128), F32),
            pltpu.VMEM((groups, width, width), BF16),
            pltpu.VMEM((groups, rows, 128), F32),
            dma((6,)), dma((4,)), dma((len(ARRIVALS),)),
            dma((2,)), dma((2, 2)), dma((2,)), dma((2, 3)), dma((2,)), dma((2, 3)),
            dma((2,)), dma((2, 2)), dma((2,)),
        ],
        compiler_params=pltpu.CompilerParams(
            collective_id=0, has_side_effects=True, vmem_limit_bytes=60 * 1024 * 1024
        ),
    )(
        tokens.reshape(rows, half), pre_gain.reshape(1, -1), mix_gain.reshape(1, -1),
        pool_scale.reshape(1, -1), post_gain.reshape(1, -1),
        jnp.swapaxes(pool_weight, 1, 2).reshape(groups * out_cols, width),
        first_gate, first_up, first_down.T, second_gate, second_up, second_down.T,
    )
    return out.reshape(tokens.shape)


def solution(mesh):
    tok = P(("rep", "fs"), None, "tp")
    wide = P("fs", "tp")
    tall = P("tp", "fs")
    placed = (
        tok, P(), wide, wide, tall, P("tp"), P("tp", None, "fs"), P("tp"), P(), wide, wide, tall,
    )

    def layer(*args):
        return jax.shard_map(fused, mesh=mesh, in_specs=placed, out_specs=tok, check_vma=False)(*args)

    return layer
```

```python
import jax
import jax.numpy as jnp
from jax import lax
from jax.experimental import pallas as pl
from jax.experimental.pallas import tpu as pltpu
from jax.sharding import PartitionSpec as P

F32 = jnp.float32
BF16 = jnp.bfloat16
MESH = pl.DeviceIdType.MESH
GROUPS = 4
SIDE = 4
epsilon = 1e-06
NT = (((1,), (1,)), ((), ()))

PLAN = (
    (
        ("c", 0, 1), ("c", 1, 3), ("c", 1, 1), ("c", 0, 3), ("z", 0, 0, 0, 1), ("z", 1, 0, 0, 0), ("c", 1, 2),
        ("z", 3, 0, 0, 0), ("c", 0, 2), ("z", 2, 0, 0, 1), ("r", 0, 0, 0, 1), ("t", 1, 0), ("r", 1, 0, 0, 0),
        ("r", 1, 0, 0, 1),
    ),
    (
        ("z", 1, 3, 0, 1), ("z", 1, 1, 0, 0), ("r", 1, 0, 3, 0), ("r", 1, 0, 3, 1), ("r", 1, 0, 1, 0),
        ("r", 0, 0, 3, 1), ("z", 0, 3, 0, 0), ("z", 0, 1, 0, 1), ("r", 0, 0, 1, 0), ("r", 0, 0, 1, 1),
        ("r", 1, 0, 2, 1), ("z", 1, 2, 0, 0), ("r", 1, 0, 1, 1), ("r", 1, 0, 2, 0), ("r", 1, 1, 0, 0),
        ("r", 1, 1, 0, 1), ("z", 0, 2, 0, 1), ("r", 0, 0, 2, 0), ("r", 0, 0, 2, 1), ("r", 0, 0, 3, 0),
        ("r", 0, 1, 0, 0), ("f", 1, 0, 0, 1), ("z", 0, 3, 1, 0), ("z", 1, 3, 3, 1), ("f", 0, 0, 3, 1),
        ("z", 1, 3, 1, 1), ("f", 1, 0, 3, 0), ("r", 0, 1, 0, 1), ("t", 1, 1), ("z", 1, 1, 3, 0),
        ("z", 1, 2, 3, 1), ("f", 1, 0, 2, 0), ("f", 1, 0, 1, 1), ("z", 1, 1, 1, 0), ("z", 0, 1, 1, 1),
        ("t", 0, 1), ("c", 3, 1), ("r", 2, 0, 0, 1), ("r", 2, 1, 0, 1), ("f", 0, 0, 2, 0), ("z", 0, 2, 3, 0),
        ("f", 0, 0, 1, 0), ("r", 0, 0, 0, 0), ("c", 2, 3),
    ),
    (
        ("f", 1, 1, 0, 0), ("t", 0, 0), ("c", 3, 3), ("r", 2, 0, 0, 0), ("r", 2, 1, 0, 0), ("c", 3, 2),
        ("z", 0, 3, 3, 0), ("z", 1, 3, 2, 1), ("z", 0, 2, 1, 1), ("z", 1, 1, 2, 0), ("z", 1, 2, 2, 1),
        ("z", 0, 3, 2, 0), ("z", 1, 2, 1, 0), ("f", 0, 1, 0, 1), ("c", 2, 1), ("c", 2, 2), ("z", 0, 2, 2, 0),
        ("z", 0, 1, 2, 1), ("z", 0, 1, 3, 1), ("z", 3, 1, 0, 0),
    ),
    (
        ("f", 0, 0, 0, 0), ("r", 3, 0, 3, 1), ("r", 3, 0, 1, 1), ("r", 3, 0, 3, 0), ("r", 3, 1, 0, 1),
        ("r", 3, 0, 1, 0), ("r", 3, 0, 0, 1), ("r", 3, 0, 0, 0), ("r", 3, 1, 0, 0), ("z", 2, 1, 0, 1),
        ("r", 2, 0, 1, 0), ("r", 2, 0, 1, 1), ("z", 2, 3, 0, 0), ("z", 3, 3, 0, 1),
    ),
    (
        ("r", 2, 0, 2, 0), ("r", 2, 0, 2, 1), ("z", 2, 2, 0, 1), ("r", 2, 0, 3, 1), ("r", 2, 0, 3, 0),
    ),
    (

    ),
    (
        ("f", 3, 0, 1, 1), ("z", 3, 1, 1, 0), ("z", 3, 2, 0, 1), ("r", 3, 0, 2, 1), ("f", 3, 0, 3, 0),
        ("z", 2, 1, 3, 1), ("z", 3, 3, 3, 1), ("z", 3, 3, 1, 1),
    ),
    (
        ("z", 3, 1, 3, 0), ("f", 2, 0, 1, 0), ("r", 3, 0, 2, 0), ("z", 2, 2, 3, 0), ("z", 2, 2, 1, 1),
        ("f", 2, 0, 2, 0), ("z", 2, 1, 1, 1), ("f", 2, 0, 0, 0), ("r", 3, 1, 2, 1), ("f", 3, 0, 0, 1),
        ("r", 3, 1, 2, 0), ("f", 3, 1, 0, 0), ("z", 2, 3, 3, 0), ("f", 2, 0, 3, 1), ("z", 3, 1, 2, 0),
        ("f", 2, 1, 0, 1), ("z", 2, 3, 1, 0),
    ),
    (

    ),
    (
        ("f", 3, 1, 2, 1), ("f", 3, 0, 2, 0), ("z", 2, 3, 2, 0), ("z", 2, 1, 2, 1), ("z", 3, 3, 2, 1),
        ("z", 2, 2, 2, 0),
    ),
)

TURNS = ((1, 0), (1, 0))
WAVES = [op for part in PLAN for op in part]
RING_SIDE = {(op[1], op[3]): op[4] for op in WAVES if op[0] == "f" and op[2] == 0}
RISE = {op[1:4]: op[4] for op in WAVES if op[0] == "z"}
def sources(op):
    kind, s = op[:2]
    if kind == "c" or kind == "t":
        return []
    if kind == "r":
        _, _, comp, j, _ = op
        if comp:
            return [("z", s, j, 0, RISE[s, j, 0])]
        return [("c", s, j)] if j else []
    if kind == "f":
        return [("r",) + op[1:]]
    _, _, j, c, _ = op
    if c == 0:
        return [("c", s, j)] if j else []
    if c == 2:
        return [("f", s, 0, j, RING_SIDE[s, j])]
    return [("r", s, 0, j, 0 if c == 3 else 1)]


def own_rows(op):
    return op[0] == "c" or (op[0] in "rf" and op[2] == 0)


COPIES = [op for op in WAVES if op[0] != "t"]
WANTED = {source for op in COPIES for source in sources(op)}


def arrival(op):
    return op if op in WANTED else ("low" if own_rows(op) else "high", op[1])


ARRIVALS = {key: i for i, key in enumerate(dict.fromkeys(arrival(op) for op in COPIES))}


def layer_kernel(
    tok_hbm, pre_hbm, mixg_hbm, scale_hbm, post_hbm, pw_hbm,
    g1_hbm, u1_hbm, d1_hbm, g2_hbm, u2_hbm, d2_hbm, out_ref,
    wide_gain, slim_gain, pw_ref, own_w,
    WS0, WS1, WS2, WS3, WB0, WB1, WB2, WB3, TB, N, ACC0, ACC1, H0, H1, PX, PR, PO, S, R, SQ, TM, RC,
    ls, ws, wr, ts, tr, ms, mr, hs, hr, rs, rr, qs,
):
    rep = lax.axis_index("rep")
    fs = lax.axis_index("fs")
    t = lax.axis_index("tp")
    x = lax.rem(fs, SIDE)
    y = lax.rem(fs // SIDE, SIDE)
    low = fs // (SIDE * SIDE)
    z = 2 * rep + low
    other = 1 - t
    high = 1 - low

    def dev(dx, dy, dz, tt):
        xx = lax.rem(x + dx, SIDE)
        yy = lax.rem(y + dy, SIDE)
        zz = lax.rem(z + dz, SIDE)
        return {"rep": zz // 2, "fs": lax.rem(zz, 2) * (SIDE * SIDE) + yy * SIDE + xx, "tp": tt}

    mate = dev(0, 0, 0, other)
    along_x = {d: dev(d, 0, 0, t) for d in (1, 2, 3)}
    along_y = {d: dev(0, d, 0, t) for d in (1, 2, 3)}
    along_z = {d: dev(0, 0, d, t) for d in (1, 3)}
    peers = [mate] + list(along_x.values()) + list(along_y.values()) + list(along_z.values())

    barrier = pltpu.get_barrier_semaphore()
    for peer in peers:
        pl.semaphore_signal(barrier, inc=1, device_id=peer, device_id_type=MESH)

    rows, half = out_ref.shape
    def remote(src, dst, ss, sr, to):
        return pltpu.make_async_remote_copy(
            src_ref=src, dst_ref=dst, send_sem=ss, recv_sem=sr, device_id=to, device_id_type=MESH
        )

    depth, hid = g1_hbm.shape
    loads = [
        pltpu.make_async_copy(src, dst, ls.at[i])
        for i, src, dst in (
            (0, g1_hbm, own_w.at[0, 0]), (0, u1_hbm, own_w.at[0, 1]), (0, d1_hbm, own_w.at[0, 2]),
            (1, pw_hbm, pw_ref), (2, tok_hbm, TB.at[0, t, 0:rows]),
            (3, g2_hbm, own_w.at[1, 0]), (3, u2_hbm, own_w.at[1, 1]), (3, d2_hbm, own_w.at[1, 2]),
            (4, pre_hbm, wide_gain.at[0:1]), (4, post_hbm, wide_gain.at[1:2]),
            (5, mixg_hbm, slim_gain.at[0:1]), (5, scale_hbm, slim_gain.at[1:2]),
        )
    ]
    for load in loads:
        load.start()

    def loaded(i, ref):
        pltpu.make_async_copy(ref, ref, ls.at[i]).wait()

    piece = rows // 2
    widths = (H0.shape[1], H1.shape[1])
    WS = (WS0, WS1, WS2, WS3)
    WB = (WB0, WB1, WB2, WB3)
    ACC = (ACC0, ACC1)
    H = (H0, H1)
    axes = (along_x, along_y)
    turn = (0, 1, 1, 0)
    places = (x, y)

    def slab(s, lo, j, c):
        a = lax.rem(places[turn[s]] + j, SIDE)
        c = lax.rem(places[1 - turn[s]] + c, SIDE)
        yy, xx = (c, a) if turn[s] == 0 else (a, c)
        start = ((lo * SIDE + yy) * SIDE + xx) * depth
        return WB[s].at[pl.ds(pl.multiple_of(start, depth), depth)]

    def side_of(s, lo, lanes):
        return WB[s][pl.ds(pl.multiple_of(lo * half, half), half), lanes]

    def pack(s):
        b, p = divmod(s, 2)
        n = widths[p]
        start = 2 * widths[0] * p
        for k in range(2):
            for i in range(3):
                WS[s][k, :, i * n:(i + 1) * n] = own_w[b, i, :, start + k * n:start + (k + 1) * n]
            if s == 1:
                flat = pw_ref[...]
                for i in range(2):
                    WS[s][k, i * 16:(i + 1) * 16, 3 * n:] = flat[:, i * 128:(i + 1) * 128]
        start = ((low * SIDE + y) * SIDE + x) * depth
        WB[s][pl.ds(pl.multiple_of(start, depth), depth)] = WS[s][lax.rem(places[turn[s]], 2)]

    def copy_of(op):
        kind = op[0]
        if kind == "t":
            return tok_send(0, op[1], op[2])
        s = op[1]
        axis, ring = axes[turn[s]], axes[1 - turn[s]]
        sems = (ws.at[s], wr.at[ARRIVALS[arrival(op)]])
        if kind == "c":
            d = SIDE - op[2]
            src = WS[s].at[lax.rem(places[turn[s]] + d, 2)]
            return remote(src, slab(s, low, 0, 0), *sems, axis[d])
        if kind == "r":
            _, _, comp, j, side = op
            ref = slab(s, high if comp else low, j, 0)
            return remote(ref, ref, *sems, ring[(1, 3)[side]])
        if kind == "f":
            _, _, comp, j, side = op
            ref = slab(s, high if comp else low, j, (3, 1)[side])
            return remote(ref, ref, *sems, ring[(1, 3)[side]])
        _, _, j, c, up = op
        ref = slab(s, low, j, c)
        return remote(ref, ref, *sems, along_z[1 if up else 3])

    here = set()

    def need(op):
        if op not in here:
            here.add(op)
            copy_of(op).wait_recv()

    def issue(part):
        for op in PLAN[part]:
            for source in sources(op):
                need(source)
            copy_of(op).start()

    def base(p):
        return rows * (1 + p)

    own = slice(0, rows)
    foreign = tuple(slice(base(p), base(p) + rows) for p in range(2))

    def axis_of(b, p):
        return axes[turn[2 * b + p]]

    def tok_send(b, p, i):
        src = TB.at[b, t, i * piece:(i + 1) * piece]
        dst = TB.at[b, t, base(p) + i * piece:base(p) + (i + 1) * piece]
        return remote(src, dst, ts.at[b], tr.at[b, p], axis_of(b, p)[(1, 3)[i]])

    def tok_here(b, p):
        ref = TB.at[b, t, foreign[p]]
        remote(ref, ref, ts.at[b], tr.at[b, p], mate).wait_recv()

    def mate_send(b, n):
        ref = TB.at[b, t, own if n == 2 else foreign[n]]
        return remote(ref, ref, ms.at[b], mr.at[b, n], mate)

    def half_send(b, n):
        cut = own if n == 2 else foreign[n]
        return remote(PX.at[b, cut], PR.at[b, cut], hs.at[b], hr.at[b, n], mate)

    def back_send(b, p, i):
        cut = slice(i * piece, (i + 1) * piece)
        return remote(S.at[b, p, cut], R.at[b, p, cut], rs.at[b], rr.at[b, p], axis_of(b, p)[(3, 1)[i]])

    def back_here(b, p):
        remote(S.at[b, p], R.at[b, p], rs.at[b], rr.at[b, p], mate).wait_recv()

    def norm_rows(b, cut):
        parts = [TB[b, c, cut].astype(F32) for c in range(2)]
        total = sum(jnp.sum(v * v, axis=-1, keepdims=True) for v in parts)
        inv = lax.rsqrt(total / (2 * half) + epsilon)
        for c in range(2):
            N[c, cut] = (parts[c] * inv * wide_gain[b:b + 1, c * half:(c + 1) * half]).astype(BF16)

    def gate_up(b, p, lo, fresh, cut):
        n = 2 * widths[p]
        wide = side_of(2 * b + p, lo, slice(0, n))
        value = jnp.dot(N[lo, cut], wide, preferred_element_type=F32)
        at = own if cut is own else slice(rows, 2 * rows)
        if fresh:
            ACC[p][at] = value
        else:
            ACC[p][at] += value

    def hidden(p, cut):
        at = own if cut is own else slice(rows, 2 * rows)
        n = widths[p]
        H[p][at] = (jax.nn.silu(ACC[p][at, 0:n]) * ACC[p][at, n:2 * n]).astype(BF16)

    def down(b, p, cut, lo):
        at = own if cut is own else slice(rows, 2 * rows)
        n = widths[p]
        tall = side_of(2 * b + p, lo, slice(2 * n, 3 * n))
        return lax.dot_general(H[p][at], tall, NT, preferred_element_type=F32)

    def project(b, last, gaps):
        for p in TURNS[b]:
            cut = foreign[p]
            need_all(2 * b + p, False)
            gate_up(b, p, last, False, cut)
            hidden(p, cut)
            PX[b, cut] = down(b, p, cut, other).astype(BF16)
            half_send(b, p).start()
        for p in range(2):
            PO[foreign[p]] = down(b, p, foreign[p], t)
        gaps[0]()
        for p in TURNS[b]:
            cut = foreign[p]
            half_send(b, p).wait_recv()
            S[b, p] = (PO[cut] + PR[b, cut].astype(F32)).astype(BF16)
            for i in range(2):
                back_send(b, p, i).start()
        for p in range(2):
            gate_up(b, p, last, False, own)
            hidden(p, own)
        PX[b, own] = (down(b, 0, own, other) + down(b, 1, own, other)).astype(BF16)
        half_send(b, 2).start()
        gaps[1]()
        PO[own] = down(b, 0, own, t) + down(b, 1, own, t)
        gaps[2]()
        half_send(b, 2).wait_recv()
        total = PO[own] + PR[b, own].astype(F32)
        for p in range(2):
            back_here(b, p)
            total = total + R[b, p].astype(F32)
        return total

    groups_here = 2
    width = half // groups_here

    def ready_pool():
        issue(8)
        maps = WB1[:, 3 * widths[1]:].reshape(2 * SIDE * SIDE, depth, 128).astype(F32)
        maps = maps.reshape(2 * SIDE * SIDE, 4, 8, 128)
        for g in range(groups_here):
            TM[g] = jnp.concatenate(
                [maps[:, g].reshape(width, 128), maps[:, 2 + g].reshape(width, 128)], axis=1
            ).astype(BF16)
            reached = 2 * 2 ** g * jnp.where(t == 0, 1, 2 ** groups_here)
            ages = lax.broadcasted_iota(jnp.int32, (rows, 128), 0) + 1
            RC[g] = 1.0 / jnp.minimum(ages, reached).astype(F32)

    def slabs(s, n):
        ref = WB[s].at[0:n * depth]
        return lambda key: remote(ref, ref, ws.at[s], wr.at[ARRIVALS[key]], mate)

    def need_all(s, mine):
        for op in COPIES:
            if op[1] == s and own_rows(op) == mine and op in WANTED:
                need(op)
        key = ("low" if mine else "high", s)
        n = sum(arrival(op) == key for op in COPIES)
        if n:
            slabs(s, n)(key).wait_recv()

    loaded(0, own_w.at[0])
    loaded(1, pw_ref)
    pack(0)
    pack(1)
    loaded(3, own_w.at[1])
    pack(2)
    pack(3)
    loaded(2, TB.at[0, t, own])
    loaded(4, wide_gain)
    loaded(5, slim_gain)
    pl.semaphore_wait(barrier, len(peers))

    issue(0)
    mate_send(0, 2).start()
    mate_send(0, 2).wait_recv()
    norm_rows(0, own)
    issue(1)
    issue(2)
    for p in range(2):
        tok_here(0, p)
        mate_send(0, p).start()
    issue(3)
    for p in range(2):
        mate_send(0, p).wait_recv()
        norm_rows(0, foreign[p])
    issue(4)
    for p in TURNS[0]:
        need_all(p, True)
        gate_up(0, p, low, True, foreign[p])
        gate_up(0, p, low, True, own)
    issue(5)
    first = project(0, high, [lambda: issue(6), lambda: issue(7), ready_pool])

    after_first = (TB[0, t, own].astype(F32) + 0.5 * first).astype(BF16).astype(F32)
    square = after_first * after_first
    SQ[0] = sum(square[:, i * 128:(i + 1) * 128] for i in range(half // 128))
    swap = remote(SQ.at[0], SQ.at[1], qs.at[0], qs.at[1], mate)
    swap.start()
    swap.wait_recv()
    total = jnp.sum(SQ[0] + SQ[1], axis=-1, keepdims=True)
    h = (after_first * lax.rsqrt(total / (2 * half) + epsilon) * slim_gain[0:1, :]).astype(BF16).astype(F32)

    def shifted(v, by):
        spot_ids = lax.broadcasted_iota(jnp.int32, v.shape, 0)
        return jnp.where(spot_ids >= by, pltpu.roll(v, by, 0), 0.0)

    for g in range(groups_here):
        hg = h[:, g * width:(g + 1) * width]
        run = hg + shifted(hg, 1)
        window = 2
        found = run
        number = t * groups_here + g
        for level in range(1, GROUPS):
            run = run + shifted(run, window)
            window = window * 2
            found = jnp.where(number >= level, run, found)
        share = jnp.concatenate([RC[g]] * (width // 128), axis=1)
        diff = (found * share - hg).astype(BF16)
        mixed = lax.dot_general(diff, TM[g], NT, preferred_element_type=F32)
        at = slice(g * width, (g + 1) * width)
        TB[1, t, own, at] = (after_first[:, at] + slim_gain[1:2, at] * mixed).astype(BF16)

    for p in range(2):
        for i in range(2):
            tok_send(1, p, i).start()
    mate_send(1, 2).start()
    mate_send(1, 2).wait_recv()
    norm_rows(1, own)
    issue(9)
    for p in range(2):
        tok_here(1, p)
        mate_send(1, p).start()
    for p in TURNS[1]:
        need_all(2 + p, True)
        gate_up(1, p, low, True, own)
    for p in TURNS[1]:
        mate_send(1, p).wait_recv()
        norm_rows(1, foreign[p])
        gate_up(1, p, low, True, foreign[p])
    second = project(1, high, [lambda: None] * 3)
    out_ref[...] = (TB[1, t, own].astype(F32) + 0.5 * second).astype(BF16)

    for s in range(4):
        n = sum(op[1] == s for op in COPIES)
        ref = WB[s].at[0:n * depth]
        remote(ref, ref, ws.at[s], wr.at[0], mate).wait_send()
    for b in range(2):
        remote(S.at[b], R.at[b], ts.at[b], tr.at[b, 0], mate).wait_send()
        remote(S.at[b], R.at[b], rs.at[b], rr.at[b, 0], mate).wait_send()
        remote(PX.at[b], PR.at[b], ms.at[b], mr.at[b, 0], mate).wait_send()
        remote(PX.at[b], PR.at[b], hs.at[b], hr.at[b, 0], mate).wait_send()
    swap.wait_send()


def fused(
    tokens, pre_gain, first_gate, first_up, first_down, mix_gain, pool_weight,
    pool_scale, post_gain, second_gate, second_up, second_down,
):
    _, rows, half = tokens.shape
    depth, hid = first_gate.shape
    wide = 3 * hid // 10
    slim = hid // 2 - wide
    groups, width, out_cols = pool_weight.shape
    lanes = (3 * wide, 3 * slim + 128, 3 * wide, 3 * slim)

    vmem = pl.BlockSpec(memory_space=pltpu.VMEM)
    anyw = pl.BlockSpec(memory_space=pl.ANY)
    dma = pltpu.SemaphoreType.DMA
    out = pl.pallas_call(
        layer_kernel,
        out_shape=pltpu.VMEM((rows, half), BF16),
        in_specs=[anyw] * 12,
        out_specs=vmem,
        scratch_shapes=[
            pltpu.VMEM((2, 2 * half), F32),
            pltpu.VMEM((2, half), F32),
            pltpu.VMEM((groups * out_cols, width), BF16),
            pltpu.VMEM((2, 3, depth, hid), BF16),
        ]
        + [pltpu.VMEM((2, depth, n), BF16) for n in lanes]
        + [pltpu.VMEM((2 * half, n), BF16) for n in lanes]
        + [
            pltpu.VMEM((2, 2, 3 * rows, half), BF16),
            pltpu.VMEM((2, 3 * rows, half), BF16),
            pltpu.VMEM((2 * rows, 2 * wide), F32),
            pltpu.VMEM((2 * rows, 2 * slim), F32),
            pltpu.VMEM((2 * rows, wide), BF16),
            pltpu.VMEM((2 * rows, slim), BF16),
            pltpu.VMEM((2, 3 * rows, half), BF16),
            pltpu.VMEM((2, 3 * rows, half), BF16),
            pltpu.VMEM((3 * rows, half), F32),
            pltpu.VMEM((2, 2, rows, half), BF16),
            pltpu.VMEM((2, 2, rows, half), BF16),
            pltpu.VMEM((2, rows, 128), F32),
            pltpu.VMEM((groups, width, width), BF16),
            pltpu.VMEM((groups, rows, 128), F32),
            dma((6,)), dma((4,)), dma((len(ARRIVALS),)),
            dma((2,)), dma((2, 2)), dma((2,)), dma((2, 3)), dma((2,)), dma((2, 3)),
            dma((2,)), dma((2, 2)), dma((2,)),
        ],
        compiler_params=pltpu.CompilerParams(
            collective_id=0, has_side_effects=True, vmem_limit_bytes=60 * 1024 * 1024
        ),
    )(
        tokens.reshape(rows, half), pre_gain.reshape(1, -1), mix_gain.reshape(1, -1),
        pool_scale.reshape(1, -1), post_gain.reshape(1, -1),
        jnp.swapaxes(pool_weight, 1, 2).reshape(groups * out_cols, width),
        first_gate, first_up, first_down.T, second_gate, second_up, second_down.T,
    )
    return out.reshape(tokens.shape)


def solution(mesh):
    tok = P(("rep", "fs"), None, "tp")
    wide = P("fs", "tp")
    tall = P("tp", "fs")
    placed = (
        tok, P(), wide, wide, tall, P("tp"), P("tp", None, "fs"), P("tp"), P(), wide, wide, tall,
    )

    def layer(*args):
        return jax.shard_map(fused, mesh=mesh, in_specs=placed, out_specs=tok, check_vma=False)(*args)

    return layer
```

```python
import jax
import jax.numpy as jnp
from jax import lax
from jax.experimental import pallas as pl
from jax.experimental.pallas import tpu as pltpu
from jax.sharding import PartitionSpec as P

F32 = jnp.float32
BF16 = jnp.bfloat16
MESH = pl.DeviceIdType.MESH
GROUPS = 4
SIDE = 4
epsilon = 1e-06
NT = (((1,), (1,)), ((), ()))

PLAN = (
    (
        ("c", 0, 1), ("c", 1, 3), ("c", 1, 1), ("c", 0, 3), ("z", 0, 0, 0, 1), ("z", 1, 0, 0, 0), ("c", 1, 2),
        ("z", 3, 0, 0, 0), ("c", 0, 2), ("z", 2, 0, 0, 1), ("r", 0, 0, 0, 1), ("t", 1, 0), ("r", 1, 0, 0, 0),
        ("r", 1, 0, 0, 1),
    ),
    (
        ("z", 1, 3, 0, 1), ("z", 1, 1, 0, 0), ("r", 1, 0, 3, 0), ("r", 1, 0, 3, 1), ("r", 1, 0, 1, 0),
        ("r", 0, 0, 3, 1), ("z", 0, 3, 0, 0), ("z", 0, 1, 0, 1), ("r", 0, 0, 1, 0), ("r", 0, 0, 1, 1),
        ("r", 1, 0, 2, 1), ("z", 1, 2, 0, 0), ("r", 1, 0, 1, 1), ("r", 1, 0, 2, 0), ("r", 1, 1, 0, 0),
        ("r", 1, 1, 0, 1), ("z", 0, 2, 0, 1), ("r", 0, 0, 2, 0), ("r", 0, 0, 2, 1), ("r", 0, 0, 3, 0),
        ("r", 0, 1, 0, 0), ("f", 1, 0, 0, 1), ("z", 0, 3, 1, 0), ("z", 1, 3, 3, 1), ("f", 0, 0, 3, 1),
        ("z", 1, 3, 1, 1), ("f", 1, 0, 3, 0), ("r", 0, 1, 0, 1), ("t", 1, 1), ("z", 1, 1, 3, 0),
        ("z", 1, 2, 3, 1), ("f", 1, 0, 2, 0), ("f", 1, 0, 1, 1), ("z", 1, 1, 1, 0), ("z", 0, 1, 1, 1),
        ("t", 0, 1), ("c", 3, 1), ("r", 2, 0, 0, 1), ("r", 2, 1, 0, 1), ("f", 0, 0, 2, 0), ("z", 0, 2, 3, 0),
        ("f", 0, 0, 1, 0), ("r", 0, 0, 0, 0), ("c", 2, 3),
    ),
    (
        ("f", 1, 1, 0, 0), ("t", 0, 0), ("c", 3, 3), ("r", 2, 0, 0, 0), ("r", 2, 1, 0, 0), ("c", 3, 2),
        ("z", 0, 3, 3, 0), ("z", 1, 3, 2, 1), ("z", 0, 2, 1, 1), ("z", 1, 1, 2, 0), ("z", 1, 2, 2, 1),
        ("z", 0, 3, 2, 0), ("z", 1, 2, 1, 0), ("f", 0, 1, 0, 1), ("c", 2, 1), ("c", 2, 2), ("z", 0, 2, 2, 0),
        ("z", 0, 1, 2, 1), ("z", 0, 1, 3, 1), ("z", 3, 1, 0, 0),
    ),
    (
        ("f", 0, 0, 0, 0), ("r", 3, 0, 3, 1), ("r", 3, 0, 1, 1), ("r", 3, 0, 3, 0), ("r", 3, 1, 0, 1),
        ("r", 3, 0, 1, 0), ("r", 3, 0, 0, 1), ("r", 3, 0, 0, 0), ("r", 3, 1, 0, 0), ("z", 2, 1, 0, 1),
        ("r", 2, 0, 1, 0), ("r", 2, 0, 1, 1), ("z", 2, 3, 0, 0), ("z", 3, 3, 0, 1),
    ),
    (
        ("r", 2, 0, 2, 0), ("r", 2, 0, 2, 1), ("z", 2, 2, 0, 1), ("r", 2, 0, 3, 1), ("r", 2, 0, 3, 0),
    ),
    (

    ),
    (
        ("f", 3, 0, 1, 1), ("z", 3, 1, 1, 0), ("z", 3, 2, 0, 1), ("r", 3, 0, 2, 1), ("f", 3, 0, 3, 0),
        ("z", 2, 1, 3, 1), ("z", 3, 3, 3, 1), ("z", 3, 3, 1, 1),
    ),
    (
        ("z", 3, 1, 3, 0), ("f", 2, 0, 1, 0), ("r", 3, 0, 2, 0), ("z", 2, 2, 3, 0), ("z", 2, 2, 1, 1),
        ("f", 2, 0, 2, 0), ("z", 2, 1, 1, 1), ("f", 2, 0, 0, 0), ("r", 3, 1, 2, 1), ("f", 3, 0, 0, 1),
        ("r", 3, 1, 2, 0), ("f", 3, 1, 0, 0), ("z", 2, 3, 3, 0), ("f", 2, 0, 3, 1), ("z", 3, 1, 2, 0),
        ("f", 2, 1, 0, 1), ("z", 2, 3, 1, 0),
    ),
    (

    ),
    (
        ("f", 3, 1, 2, 1), ("f", 3, 0, 2, 0), ("z", 2, 3, 2, 0), ("z", 2, 1, 2, 1), ("z", 3, 3, 2, 1),
        ("z", 2, 2, 2, 0),
    ),
)

TURNS = ((1, 0), (0, 1))
WAVES = [op for part in PLAN for op in part]
RING_SIDE = {(op[1], op[3]): op[4] for op in WAVES if op[0] == "f" and op[2] == 0}
RISE = {op[1:4]: op[4] for op in WAVES if op[0] == "z"}
def sources(op):
    kind, s = op[:2]
    if kind == "c" or kind == "t":
        return []
    if kind == "r":
        _, _, comp, j, _ = op
        if comp:
            return [("z", s, j, 0, RISE[s, j, 0])]
        return [("c", s, j)] if j else []
    if kind == "f":
        return [("r",) + op[1:]]
    _, _, j, c, _ = op
    if c == 0:
        return [("c", s, j)] if j else []
    if c == 2:
        return [("f", s, 0, j, RING_SIDE[s, j])]
    return [("r", s, 0, j, 0 if c == 3 else 1)]


def own_rows(op):
    return op[0] == "c" or (op[0] in "rf" and op[2] == 0)


COPIES = [op for op in WAVES if op[0] != "t"]
WANTED = {source for op in COPIES for source in sources(op)}


def arrival(op):
    return op if op in WANTED else ("low" if own_rows(op) else "high", op[1])


ARRIVALS = {key: i for i, key in enumerate(dict.fromkeys(arrival(op) for op in COPIES))}


def layer_kernel(
    tok_hbm, pre_hbm, mixg_hbm, scale_hbm, post_hbm, pw_hbm,
    g1_hbm, u1_hbm, d1_hbm, g2_hbm, u2_hbm, d2_hbm, out_ref,
    wide_gain, slim_gain, pw_ref, own_w,
    WS0, WS1, WS2, WS3, WB0, WB1, WB2, WB3, TB, N, ACC0, ACC1, H0, H1, PX, PR, PO, S, R, SQ, TM, RC, HB,
    ls, ws, wr, ts, tr, ms, mr, hs, hr, rs, rr, qs,
):
    rep = lax.axis_index("rep")
    fs = lax.axis_index("fs")
    t = lax.axis_index("tp")
    x = lax.rem(fs, SIDE)
    y = lax.rem(fs // SIDE, SIDE)
    low = fs // (SIDE * SIDE)
    z = 2 * rep + low
    other = 1 - t
    high = 1 - low

    def dev(dx, dy, dz, tt):
        xx = lax.rem(x + dx, SIDE)
        yy = lax.rem(y + dy, SIDE)
        zz = lax.rem(z + dz, SIDE)
        return {"rep": zz // 2, "fs": lax.rem(zz, 2) * (SIDE * SIDE) + yy * SIDE + xx, "tp": tt}

    mate = dev(0, 0, 0, other)
    along_x = {d: dev(d, 0, 0, t) for d in (1, 2, 3)}
    along_y = {d: dev(0, d, 0, t) for d in (1, 2, 3)}
    along_z = {d: dev(0, 0, d, t) for d in (1, 3)}
    peers = [mate] + list(along_x.values()) + list(along_y.values()) + list(along_z.values())

    barrier = pltpu.get_barrier_semaphore()
    for peer in peers:
        pl.semaphore_signal(barrier, inc=1, device_id=peer, device_id_type=MESH)

    rows, half = out_ref.shape
    def remote(src, dst, ss, sr, to):
        return pltpu.make_async_remote_copy(
            src_ref=src, dst_ref=dst, send_sem=ss, recv_sem=sr, device_id=to, device_id_type=MESH
        )

    depth, hid = g1_hbm.shape
    loads = [
        pltpu.make_async_copy(src, dst, ls.at[i])
        for i, src, dst in (
            (0, g1_hbm, own_w.at[0, 0]), (0, u1_hbm, own_w.at[0, 1]), (0, d1_hbm, own_w.at[0, 2]),
            (1, pw_hbm, pw_ref), (2, tok_hbm, TB.at[0, t, 0:rows]),
            (3, g2_hbm, own_w.at[1, 0]), (3, u2_hbm, own_w.at[1, 1]), (3, d2_hbm, own_w.at[1, 2]),
            (4, pre_hbm, wide_gain.at[0:1]), (4, post_hbm, wide_gain.at[1:2]),
            (5, mixg_hbm, slim_gain.at[0:1]), (5, scale_hbm, slim_gain.at[1:2]),
        )
    ]
    for load in loads:
        load.start()

    def loaded(i, ref):
        pltpu.make_async_copy(ref, ref, ls.at[i]).wait()

    piece = rows // 2
    widths = (H0.shape[1], H1.shape[1])
    WS = (WS0, WS1, WS2, WS3)
    WB = (WB0, WB1, WB2, WB3)
    ACC = (ACC0, ACC1)
    H = (H0, H1)
    axes = (along_x, along_y)
    turn = (0, 1, 1, 0)
    places = (x, y)

    def slab(s, lo, j, c):
        a = lax.rem(places[turn[s]] + j, SIDE)
        c = lax.rem(places[1 - turn[s]] + c, SIDE)
        yy, xx = (c, a) if turn[s] == 0 else (a, c)
        start = ((lo * SIDE + yy) * SIDE + xx) * depth
        return WB[s].at[pl.ds(pl.multiple_of(start, depth), depth)]

    def side_of(s, lo, lanes):
        return WB[s][pl.ds(pl.multiple_of(lo * half, half), half), lanes]

    def pack(s):
        b, p = divmod(s, 2)
        n = widths[p]
        start = 2 * widths[0] * p
        for k in range(2):
            for i in range(3):
                WS[s][k, :, i * n:(i + 1) * n] = own_w[b, i, :, start + k * n:start + (k + 1) * n]
            if s == 1:
                flat = pw_ref[...]
                for i in range(2):
                    WS[s][k, i * 16:(i + 1) * 16, 3 * n:] = flat[:, i * 128:(i + 1) * 128]
        start = ((low * SIDE + y) * SIDE + x) * depth
        WB[s][pl.ds(pl.multiple_of(start, depth), depth)] = WS[s][lax.rem(places[turn[s]], 2)]

    def copy_of(op):
        kind = op[0]
        s = op[1]
        axis, ring = axes[turn[s]], axes[1 - turn[s]]
        sems = (ws.at[s], wr.at[ARRIVALS[arrival(op)]])
        if kind == "c":
            d = SIDE - op[2]
            src = WS[s].at[lax.rem(places[turn[s]] + d, 2)]
            return remote(src, slab(s, low, 0, 0), *sems, axis[d])
        if kind == "r":
            _, _, comp, j, side = op
            ref = slab(s, high if comp else low, j, 0)
            return remote(ref, ref, *sems, ring[(1, 3)[side]])
        if kind == "f":
            _, _, comp, j, side = op
            ref = slab(s, high if comp else low, j, (3, 1)[side])
            return remote(ref, ref, *sems, ring[(1, 3)[side]])
        _, _, j, c, up = op
        ref = slab(s, low, j, c)
        return remote(ref, ref, *sems, along_z[1 if up else 3])

    here = set()

    def need(op):
        if op not in here:
            here.add(op)
            copy_of(op).wait_recv()

    def issue(part):
        for op in PLAN[part]:
            for source in sources(op):
                need(source)
            if op[0] == "t":
                for k in range(2):
                    tok_send(0, op[1], op[2], k).start()
            else:
                copy_of(op).start()

    def base(p):
        return rows * (1 + p)

    own = slice(0, rows)
    foreign = tuple(slice(base(p), base(p) + rows) for p in range(2))

    def axis_of(b, p):
        return axes[turn[2 * b + p]]

    def part_of(k):
        return slice(k * piece, (k + 1) * piece)

    def far_part(p, k):
        return slice(base(p) + k * piece, base(p) + (k + 1) * piece)

    def strip(i, k):
        return slice(k * piece + i * piece // 2, k * piece + (i + 1) * piece // 2)

    def tok_send(b, p, i, k):
        cut = strip(i, k)
        src = TB.at[b, t, cut]
        dst = TB.at[b, t, base(p) + cut.start:base(p) + cut.stop]
        return remote(src, dst, ts.at[b], tr.at[b, p, k * b], axis_of(b, p)[(1, 3)[i]])

    def tok_here(b, p, k, cut):
        ref = TB.at[b, t, cut]
        remote(ref, ref, ts.at[b], tr.at[b, p, k], mate).wait_recv()

    def mate_send(b, n, cut):
        ref = TB.at[b, t, cut]
        return remote(ref, ref, ms.at[b], mr.at[b, n], mate)

    def half_send(b, n):
        cut = own if n == 2 else foreign[n]
        return remote(PX.at[b, cut], PR.at[b, cut], hs.at[b], hr.at[b, n], mate)

    def back_send(b, p, i, k):
        cut = strip(i, k)
        return remote(S.at[b, p, cut], R.at[b, p, cut], rs.at[b], rr.at[b, p, k], axis_of(b, p)[(3, 1)[i]])

    def back_here(b, p, k):
        cut = part_of(k)
        remote(S.at[b, p, cut], R.at[b, p, cut], rs.at[b], rr.at[b, p, k], mate).wait_recv()

    def norm_rows(b, cut):
        parts = [TB[b, c, cut].astype(F32) for c in range(2)]
        total = sum(jnp.sum(v * v, axis=-1, keepdims=True) for v in parts)
        inv = lax.rsqrt(total / (2 * half) + epsilon)
        for c in range(2):
            N[c, cut] = (parts[c] * inv * wide_gain[b:b + 1, c * half:(c + 1) * half]).astype(BF16)

    def gate_up(b, p, lo, cut):
        wide = side_of(2 * b + p, lo, slice(0, 2 * widths[p]))
        return jnp.dot(N[lo, cut], wide, preferred_element_type=F32)

    def hidden(p, cut, value):
        at = own if cut is own else slice(rows, 2 * rows)
        n = widths[p]
        H[p][at] = (jax.nn.silu(value[:, 0:n]) * value[:, n:2 * n]).astype(BF16)

    def down(b, p, cut, lo):
        at = own if cut is own else slice(rows, 2 * rows)
        n = widths[p]
        tall = side_of(2 * b + p, lo, slice(2 * n, 3 * n))
        return lax.dot_general(H[p][at], tall, NT, preferred_element_type=F32)

    def project(b, gaps):
        for p in TURNS[b]:
            cut = foreign[p]
            need_all(2 * b + p, False)
            begun = ACC[p][...] if b == 0 else gate_up(b, p, low, cut)
            hidden(p, cut, begun + gate_up(b, p, high, cut))
            PX[b, cut] = down(b, p, cut, other).astype(BF16)
            half_send(b, p).start()
        for p in range(2):
            PO[foreign[p]] = down(b, p, foreign[p], t)
        gaps[0]()
        for p in TURNS[b]:
            cut = foreign[p]
            half_send(b, p).wait_recv()
            S[b, p] = (PO[cut] + PR[b, cut].astype(F32)).astype(BF16)
            for k in range(2):
                for i in range(2):
                    back_send(b, p, i, k).start()
        for p in range(2):
            hidden(p, own, gate_up(b, p, low, own) + gate_up(b, p, high, own))
        PX[b, own] = (down(b, 0, own, other) + down(b, 1, own, other)).astype(BF16)
        half_send(b, 2).start()
        gaps[1]()
        PO[own] = down(b, 0, own, t) + down(b, 1, own, t)
        gaps[2]()
        half_send(b, 2).wait_recv()

    def collect(b, k):
        cut = part_of(k)
        total = PO[cut] + PR[b, cut].astype(F32)
        for p in range(2):
            back_here(b, p, k)
            total = total + R[b, p, cut].astype(F32)
        return total

    groups_here = 2
    width = half // groups_here

    def ready_pool():
        issue(8)
        maps = WB1[:, 3 * widths[1]:].reshape(2 * SIDE * SIDE, depth, 128).astype(F32)
        maps = maps.reshape(2 * SIDE * SIDE, 4, 8, 128)
        for g in range(groups_here):
            TM[g] = jnp.concatenate(
                [maps[:, g].reshape(width, 128), maps[:, 2 + g].reshape(width, 128)], axis=1
            ).astype(BF16)
            reached = 2 * 2 ** g * jnp.where(t == 0, 1, 2 ** groups_here)
            ages = lax.broadcasted_iota(jnp.int32, (rows, 128), 0) + 1
            RC[g] = 1.0 / jnp.minimum(ages, reached).astype(F32)

    def slabs(s, n):
        ref = WB[s].at[0:n * depth]
        return lambda key: remote(ref, ref, ws.at[s], wr.at[ARRIVALS[key]], mate)

    def need_all(s, mine):
        for op in COPIES:
            if op[1] == s and own_rows(op) == mine and op in WANTED:
                need(op)
        key = ("low" if mine else "high", s)
        n = sum(arrival(op) == key for op in COPIES)
        if n:
            slabs(s, n)(key).wait_recv()

    loaded(0, own_w.at[0])
    loaded(1, pw_ref)
    pack(0)
    pack(1)
    loaded(3, own_w.at[1])
    pack(2)
    pack(3)
    loaded(2, TB.at[0, t, own])
    loaded(4, wide_gain)
    loaded(5, slim_gain)
    pl.semaphore_wait(barrier, len(peers))

    issue(0)
    mate_send(0, 2, own).start()
    mate_send(0, 2, own).wait_recv()
    norm_rows(0, own)
    issue(1)
    issue(2)
    for p in range(2):
        tok_here(0, p, 0, foreign[p])
        mate_send(0, p, foreign[p]).start()
    issue(3)
    for p in range(2):
        mate_send(0, p, foreign[p]).wait_recv()
        norm_rows(0, foreign[p])
    issue(4)
    for p in TURNS[0]:
        need_all(p, True)
        ACC[p][...] = gate_up(0, p, low, foreign[p])
    issue(5)
    project(0, [lambda: issue(6), lambda: issue(7), ready_pool])

    def shifted(v, by):
        spot_ids = lax.broadcasted_iota(jnp.int32, v.shape, 0)
        return jnp.where(spot_ids >= by, pltpu.roll(v, by, 0), 0.0)

    def swap(k):
        cut = part_of(k)
        return remote(SQ.at[0, cut], SQ.at[1, cut], qs.at[0], qs.at[1 + k], mate)

    reach = 2 ** GROUPS
    for k in range(2):
        cut = part_of(k)
        after_first = (TB[0, t, cut].astype(F32) + 0.5 * collect(0, k)).astype(BF16).astype(F32)
        square = after_first * after_first
        SQ[0, cut] = sum(square[:, i * 128:(i + 1) * 128] for i in range(half // 128))
        swap(k).start()
        swap(k).wait_recv()
        total = jnp.sum(SQ[0, cut] + SQ[1, cut], axis=-1, keepdims=True)
        inv = lax.rsqrt(total / (2 * half) + epsilon)
        HB[cut] = (after_first * inv * slim_gain[0:1, :]).astype(BF16).astype(F32)
        lead = reach if k else 0
        for g in range(groups_here):
            at = slice(g * width, (g + 1) * width)
            hg = HB[cut.start - lead:cut.stop, at]
            run = hg + shifted(hg, 1)
            window = 2
            found = run
            number = t * groups_here + g
            for level in range(1, GROUPS):
                run = run + shifted(run, window)
                window = window * 2
                found = jnp.where(number >= level, run, found)
            share = jnp.concatenate([RC[g, cut]] * (width // 128), axis=1)
            diff = (found[lead:] * share - hg[lead:]).astype(BF16)
            mixed = lax.dot_general(diff, TM[g], NT, preferred_element_type=F32)
            TB[1, t, cut, at] = (after_first[:, at] + slim_gain[1:2, at] * mixed).astype(BF16)
        for p in range(2):
            for i in range(2):
                tok_send(1, p, i, k).start()
        mate_send(1, 2 + 3 * k, cut).start()

    issue(9)
    for k in range(2):
        for p in TURNS[1]:
            tok_here(1, p, k, far_part(p, k))
            mate_send(1, p + 3 * k, far_part(p, k)).start()
        if k == 0:
            for i in range(2):
                mate_send(1, 2 + 3 * i, part_of(i)).wait_recv()
            norm_rows(1, own)
        for p in TURNS[1]:
            mate_send(1, p + 3 * k, far_part(p, k)).wait_recv()
            norm_rows(1, far_part(p, k))
    for p in TURNS[1]:
        need_all(2 + p, True)
    project(1, [lambda: None] * 3)
    for k in range(2):
        cut = part_of(k)
        out_ref[cut] = (TB[1, t, cut].astype(F32) + 0.5 * collect(1, k)).astype(BF16)

    for s in range(4):
        n = sum(op[1] == s for op in COPIES)
        ref = WB[s].at[0:n * depth]
        remote(ref, ref, ws.at[s], wr.at[0], mate).wait_send()
    for b in range(2):
        remote(S.at[b], R.at[b], ts.at[b], tr.at[b, 0, 0], mate).wait_send()
        remote(S.at[b], R.at[b], rs.at[b], rr.at[b, 0, 0], mate).wait_send()
        remote(PX.at[b], PR.at[b], ms.at[b], mr.at[b, 0], mate).wait_send()
        remote(PX.at[b], PR.at[b], hs.at[b], hr.at[b, 0], mate).wait_send()
    remote(SQ.at[0], SQ.at[1], qs.at[0], qs.at[1], mate).wait_send()


def fused(
    tokens, pre_gain, first_gate, first_up, first_down, mix_gain, pool_weight,
    pool_scale, post_gain, second_gate, second_up, second_down,
):
    _, rows, half = tokens.shape
    depth, hid = first_gate.shape
    wide = 3 * hid // 10
    slim = hid // 2 - wide
    groups, width, out_cols = pool_weight.shape
    lanes = (3 * wide, 3 * slim + 128, 3 * wide, 3 * slim)

    vmem = pl.BlockSpec(memory_space=pltpu.VMEM)
    anyw = pl.BlockSpec(memory_space=pl.ANY)
    dma = pltpu.SemaphoreType.DMA
    out = pl.pallas_call(
        layer_kernel,
        out_shape=pltpu.VMEM((rows, half), BF16),
        in_specs=[anyw] * 12,
        out_specs=vmem,
        scratch_shapes=[
            pltpu.VMEM((2, 2 * half), F32),
            pltpu.VMEM((2, half), F32),
            pltpu.VMEM((groups * out_cols, width), BF16),
            pltpu.VMEM((2, 3, depth, hid), BF16),
        ]
        + [pltpu.VMEM((2, depth, n), BF16) for n in lanes]
        + [pltpu.VMEM((2 * half, n), BF16) for n in lanes]
        + [
            pltpu.VMEM((2, 2, 3 * rows, half), BF16),
            pltpu.VMEM((2, 3 * rows, half), BF16),
            pltpu.VMEM((rows, 2 * wide), F32),
            pltpu.VMEM((rows, 2 * slim), F32),
            pltpu.VMEM((2 * rows, wide), BF16),
            pltpu.VMEM((2 * rows, slim), BF16),
            pltpu.VMEM((2, 3 * rows, half), BF16),
            pltpu.VMEM((2, 3 * rows, half), BF16),
            pltpu.VMEM((3 * rows, half), F32),
            pltpu.VMEM((2, 2, rows, half), BF16),
            pltpu.VMEM((2, 2, rows, half), BF16),
            pltpu.VMEM((2, rows, 128), F32),
            pltpu.VMEM((groups, width, width), BF16),
            pltpu.VMEM((groups, rows, 128), F32),
            pltpu.VMEM((rows, half), F32),
            dma((6,)), dma((4,)), dma((len(ARRIVALS),)),
            dma((2,)), dma((2, 2, 2)), dma((2,)), dma((2, 6)), dma((2,)), dma((2, 3)),
            dma((2,)), dma((2, 2, 2)), dma((3,)),
        ],
        compiler_params=pltpu.CompilerParams(
            collective_id=0, has_side_effects=True, vmem_limit_bytes=60 * 1024 * 1024
        ),
    )(
        tokens.reshape(rows, half), pre_gain.reshape(1, -1), mix_gain.reshape(1, -1),
        pool_scale.reshape(1, -1), post_gain.reshape(1, -1),
        jnp.swapaxes(pool_weight, 1, 2).reshape(groups * out_cols, width),
        first_gate, first_up, first_down.T, second_gate, second_up, second_down.T,
    )
    return out.reshape(tokens.shape)


def solution(mesh):
    tok = P(("rep", "fs"), None, "tp")
    wide = P("fs", "tp")
    tall = P("tp", "fs")
    placed = (
        tok, P(), wide, wide, tall, P("tp"), P("tp", None, "fs"), P("tp"), P(), wide, wide, tall,
    )

    def layer(*args):
        return jax.shard_map(fused, mesh=mesh, in_specs=placed, out_specs=tok, check_vma=False)(*args)

    return layer
```

```python
import jax
import jax.numpy as jnp
from jax import lax
from jax.experimental import pallas as pl
from jax.experimental.pallas import tpu as pltpu
from jax.sharding import PartitionSpec as P

F32 = jnp.float32
BF16 = jnp.bfloat16
MESH = pl.DeviceIdType.MESH
GROUPS = 4
SIDE = 4
epsilon = 1e-06
NT = (((1,), (1,)), ((), ()))

PLAN = (
    (
        ("c", 0, 1), ("c", 1, 3), ("c", 1, 1), ("c", 0, 3), ("z", 0, 0, 0, 1), ("z", 1, 0, 0, 0), ("c", 1, 2),
        ("z", 3, 0, 0, 0), ("c", 0, 2), ("z", 2, 0, 0, 1), ("r", 0, 0, 0, 1), ("t", 1, 0), ("r", 1, 0, 0, 1),
        ("t", 0, 0),
    ),
    (
        ("z", 1, 3, 0, 1), ("z", 1, 1, 0, 0), ("r", 1, 0, 3, 1), ("r", 1, 0, 3, 0), ("r", 1, 0, 1, 0),
        ("r", 0, 0, 3, 1), ("z", 0, 3, 0, 0), ("z", 0, 1, 0, 1), ("r", 0, 0, 1, 0), ("r", 0, 0, 1, 1),
        ("r", 1, 0, 2, 1), ("z", 1, 2, 0, 0), ("r", 1, 0, 1, 1), ("r", 1, 1, 0, 1), ("r", 1, 0, 2, 0),
        ("r", 1, 1, 0, 0), ("z", 0, 2, 0, 1), ("r", 0, 0, 2, 0), ("r", 0, 0, 2, 1), ("r", 0, 0, 3, 0),
        ("f", 1, 0, 0, 1), ("z", 0, 3, 1, 0), ("z", 1, 3, 1, 1), ("f", 0, 0, 3, 1), ("r", 0, 1, 0, 1),
        ("t", 1, 1), ("z", 0, 1, 3, 1), ("f", 0, 0, 1, 0), ("z", 1, 2, 1, 0), ("f", 1, 0, 3, 0),
        ("z", 0, 1, 1, 1), ("f", 1, 0, 1, 1), ("z", 1, 1, 1, 0), ("t", 0, 1), ("c", 3, 1), ("r", 2, 0, 0, 1),
        ("r", 2, 1, 0, 1), ("f", 0, 0, 2, 0), ("z", 1, 1, 3, 0), ("r", 0, 0, 0, 0), ("r", 0, 1, 0, 0),
    ),
    (
        ("f", 1, 0, 2, 0), ("z", 1, 2, 3, 1), ("r", 1, 0, 0, 0), ("z", 0, 2, 1, 1), ("z", 0, 3, 3, 0),
        ("f", 1, 1, 0, 0), ("c", 3, 3), ("r", 2, 0, 0, 0), ("r", 2, 1, 0, 0), ("c", 3, 2), ("z", 0, 1, 2, 1),
        ("z", 1, 1, 2, 0), ("z", 0, 3, 2, 0), ("z", 0, 2, 3, 0), ("f", 0, 1, 0, 1), ("c", 2, 2), ("c", 2, 1),
        ("z", 1, 3, 2, 1), ("z", 1, 3, 3, 1), ("z", 0, 2, 2, 0), ("z", 1, 2, 2, 1), ("f", 0, 0, 0, 0),
        ("c", 2, 3),
    ),
    (
        ("z", 3, 1, 0, 0), ("r", 3, 0, 3, 1), ("z", 3, 3, 0, 1), ("r", 3, 0, 1, 1), ("r", 3, 0, 3, 0),
        ("r", 3, 1, 0, 1), ("r", 3, 0, 1, 0), ("r", 3, 0, 0, 1), ("r", 3, 0, 0, 0), ("r", 3, 1, 0, 0),
    ),
    (
        ("r", 2, 0, 2, 0), ("r", 2, 0, 2, 1), ("z", 2, 2, 0, 1), ("r", 2, 0, 1, 0), ("r", 2, 0, 1, 1),
    ),
    (
        ("z", 3, 3, 1, 1), ("z", 2, 3, 0, 0), ("r", 2, 0, 3, 1), ("r", 2, 0, 3, 0),
    ),
    (
        ("f", 3, 0, 1, 1), ("z", 3, 1, 1, 0), ("z", 3, 2, 0, 1), ("r", 3, 0, 2, 1), ("z", 3, 3, 3, 1),
        ("f", 3, 0, 3, 0), ("z", 2, 1, 0, 1), ("z", 2, 2, 3, 0),
    ),
    (
        ("z", 2, 1, 1, 1), ("z", 2, 1, 3, 1), ("z", 2, 2, 1, 1), ("f", 2, 0, 1, 0), ("f", 2, 0, 2, 0),
        ("f", 2, 0, 0, 0), ("z", 3, 1, 2, 0), ("r", 3, 1, 2, 1), ("f", 3, 0, 0, 1), ("r", 3, 0, 2, 0),
        ("r", 3, 1, 2, 0), ("f", 3, 1, 0, 0), ("f", 2, 0, 3, 1), ("z", 2, 3, 3, 0), ("f", 2, 1, 0, 1),
        ("z", 2, 3, 1, 0), ("z", 3, 1, 3, 0),
    ),
    (

    ),
    (
        ("f", 3, 1, 2, 1), ("z", 2, 1, 2, 1), ("z", 2, 3, 2, 0), ("z", 3, 3, 2, 1), ("f", 3, 0, 2, 0),
        ("z", 2, 2, 2, 0),
    ),
)

TURNS = ((1, 0), (0, 1))
WAVES = [op for part in PLAN for op in part]
RING_SIDE = {(op[1], op[3]): op[4] for op in WAVES if op[0] == "f" and op[2] == 0}
RISE = {op[1:4]: op[4] for op in WAVES if op[0] == "z"}
def sources(op):
    kind, s = op[:2]
    if kind == "c" or kind == "t":
        return []
    if kind == "r":
        _, _, comp, j, _ = op
        if comp:
            return [("z", s, j, 0, RISE[s, j, 0])]
        return [("c", s, j)] if j else []
    if kind == "f":
        return [("r",) + op[1:]]
    _, _, j, c, _ = op
    if c == 0:
        return [("c", s, j)] if j else []
    if c == 2:
        return [("f", s, 0, j, RING_SIDE[s, j])]
    return [("r", s, 0, j, 0 if c == 3 else 1)]


def own_rows(op):
    return op[0] == "c" or (op[0] in "rf" and op[2] == 0)


COPIES = [op for op in WAVES if op[0] != "t"]
WANTED = {source for op in COPIES for source in sources(op)}


def arrival(op):
    return op if op in WANTED else ("low" if own_rows(op) else "high", op[1])


ARRIVALS = {key: i for i, key in enumerate(dict.fromkeys(arrival(op) for op in COPIES))}


def layer_kernel(
    tok_hbm, pre_hbm, mixg_hbm, scale_hbm, post_hbm, pw_hbm,
    g1_hbm, u1_hbm, d1_hbm, g2_hbm, u2_hbm, d2_hbm, out_ref,
    wide_gain, slim_gain, pw_ref, own_w,
    WS0, WS1, WS2, WS3, WB0, WB1, WB2, WB3, TB, N, ACC0, ACC1, H0, H1, PX, PR, PO, S, R, SQ, TM, RC, HB,
    ls, ws, wr, ts, tr, ms, mr, hs, hr, rs, rr, qs,
):
    rep = lax.axis_index("rep")
    fs = lax.axis_index("fs")
    t = lax.axis_index("tp")
    x = lax.rem(fs, SIDE)
    y = lax.rem(fs // SIDE, SIDE)
    low = fs // (SIDE * SIDE)
    z = 2 * rep + low
    other = 1 - t
    high = 1 - low

    def dev(dx, dy, dz, tt):
        xx = lax.rem(x + dx, SIDE)
        yy = lax.rem(y + dy, SIDE)
        zz = lax.rem(z + dz, SIDE)
        return {"rep": zz // 2, "fs": lax.rem(zz, 2) * (SIDE * SIDE) + yy * SIDE + xx, "tp": tt}

    mate = dev(0, 0, 0, other)
    along_x = {d: dev(d, 0, 0, t) for d in (1, 2, 3)}
    along_y = {d: dev(0, d, 0, t) for d in (1, 2, 3)}
    along_z = {d: dev(0, 0, d, t) for d in (1, 3)}
    peers = [mate] + list(along_x.values()) + list(along_y.values()) + list(along_z.values())

    barrier = pltpu.get_barrier_semaphore()
    for peer in peers:
        pl.semaphore_signal(barrier, inc=1, device_id=peer, device_id_type=MESH)

    rows, half = out_ref.shape
    def remote(src, dst, ss, sr, to):
        return pltpu.make_async_remote_copy(
            src_ref=src, dst_ref=dst, send_sem=ss, recv_sem=sr, device_id=to, device_id_type=MESH
        )

    depth, hid = g1_hbm.shape
    loads = [
        pltpu.make_async_copy(src, dst, ls.at[i])
        for i, src, dst in (
            (0, g1_hbm, own_w.at[0, 0]), (0, u1_hbm, own_w.at[0, 1]), (0, d1_hbm, own_w.at[0, 2]),
            (1, pw_hbm, pw_ref), (2, tok_hbm, TB.at[0, t, 0:rows]),
            (3, g2_hbm, own_w.at[1, 0]), (3, u2_hbm, own_w.at[1, 1]), (3, d2_hbm, own_w.at[1, 2]),
            (4, pre_hbm, wide_gain.at[0:1]), (4, post_hbm, wide_gain.at[1:2]),
            (5, mixg_hbm, slim_gain.at[0:1]), (5, scale_hbm, slim_gain.at[1:2]),
        )
    ]
    for load in loads:
        load.start()

    def loaded(i, ref):
        pltpu.make_async_copy(ref, ref, ls.at[i]).wait()

    piece = rows // 2
    widths = (H0.shape[1], H1.shape[1])
    WS = (WS0, WS1, WS2, WS3)
    WB = (WB0, WB1, WB2, WB3)
    ACC = (ACC0, ACC1)
    H = (H0, H1)
    axes = (along_x, along_y)
    turn = (0, 1, 1, 0)
    places = (x, y)

    def slab(s, lo, j, c):
        a = lax.rem(places[turn[s]] + j, SIDE)
        c = lax.rem(places[1 - turn[s]] + c, SIDE)
        yy, xx = (c, a) if turn[s] == 0 else (a, c)
        start = ((lo * SIDE + yy) * SIDE + xx) * depth
        return WB[s].at[pl.ds(pl.multiple_of(start, depth), depth)]

    def side_of(s, lo, lanes):
        return WB[s][pl.ds(pl.multiple_of(lo * half, half), half), lanes]

    def pack(s):
        b, p = divmod(s, 2)
        n = widths[p]
        start = 2 * widths[0] * p
        for k in range(2):
            for i in range(3):
                WS[s][k, :, i * n:(i + 1) * n] = own_w[b, i, :, start + k * n:start + (k + 1) * n]
            if s == 1:
                flat = pw_ref[...]
                for i in range(2):
                    WS[s][k, i * 16:(i + 1) * 16, 3 * n:] = flat[:, i * 128:(i + 1) * 128]
        start = ((low * SIDE + y) * SIDE + x) * depth
        WB[s][pl.ds(pl.multiple_of(start, depth), depth)] = WS[s][lax.rem(places[turn[s]], 2)]

    def copy_of(op):
        kind = op[0]
        s = op[1]
        axis, ring = axes[turn[s]], axes[1 - turn[s]]
        sems = (ws.at[s], wr.at[ARRIVALS[arrival(op)]])
        if kind == "c":
            d = SIDE - op[2]
            src = WS[s].at[lax.rem(places[turn[s]] + d, 2)]
            return remote(src, slab(s, low, 0, 0), *sems, axis[d])
        if kind == "r":
            _, _, comp, j, side = op
            ref = slab(s, high if comp else low, j, 0)
            return remote(ref, ref, *sems, ring[(1, 3)[side]])
        if kind == "f":
            _, _, comp, j, side = op
            ref = slab(s, high if comp else low, j, (3, 1)[side])
            return remote(ref, ref, *sems, ring[(1, 3)[side]])
        _, _, j, c, up = op
        ref = slab(s, low, j, c)
        return remote(ref, ref, *sems, along_z[1 if up else 3])

    here = set()

    def need(op):
        if op not in here:
            here.add(op)
            copy_of(op).wait_recv()

    def issue(part):
        for op in PLAN[part]:
            for source in sources(op):
                need(source)
            if op[0] == "t":
                for k in range(2):
                    tok_send(0, op[1], op[2], k).start()
            else:
                copy_of(op).start()

    def base(p):
        return rows * (1 + p)

    own = slice(0, rows)
    foreign = tuple(slice(base(p), base(p) + rows) for p in range(2))

    def axis_of(b, p):
        return axes[turn[2 * b + p]]

    def part_of(k):
        return slice(k * piece, (k + 1) * piece)

    def far_part(p, k):
        return slice(base(p) + k * piece, base(p) + (k + 1) * piece)

    def strip(i, k):
        return slice(k * piece + i * piece // 2, k * piece + (i + 1) * piece // 2)

    def tok_send(b, p, i, k):
        cut = strip(i, k)
        src = TB.at[b, t, cut]
        dst = TB.at[b, t, base(p) + cut.start:base(p) + cut.stop]
        return remote(src, dst, ts.at[b], tr.at[b, p, k * b], axis_of(b, p)[(1, 3)[i]])

    def tok_here(b, p, k, cut):
        ref = TB.at[b, t, cut]
        remote(ref, ref, ts.at[b], tr.at[b, p, k], mate).wait_recv()

    def mate_send(b, n, cut):
        ref = TB.at[b, t, cut]
        return remote(ref, ref, ms.at[b], mr.at[b, n], mate)

    def half_send(b, n):
        cut = own if n == 2 else foreign[n]
        return remote(PX.at[b, cut], PR.at[b, cut], hs.at[b], hr.at[b, n], mate)

    def back_send(b, p, i, k):
        cut = strip(i, k)
        return remote(S.at[b, p, cut], R.at[b, p, cut], rs.at[b], rr.at[b, p, k], axis_of(b, p)[(3, 1)[i]])

    def back_here(b, p, k):
        cut = part_of(k)
        remote(S.at[b, p, cut], R.at[b, p, cut], rs.at[b], rr.at[b, p, k], mate).wait_recv()

    def norm_rows(b, cut):
        parts = [TB[b, c, cut].astype(F32) for c in range(2)]
        total = sum(jnp.sum(v * v, axis=-1, keepdims=True) for v in parts)
        inv = lax.rsqrt(total / (2 * half) + epsilon)
        for c in range(2):
            N[c, cut] = (parts[c] * inv * wide_gain[b:b + 1, c * half:(c + 1) * half]).astype(BF16)

    def gate_up(b, p, lo, cut):
        wide = side_of(2 * b + p, lo, slice(0, 2 * widths[p]))
        return jnp.dot(N[lo, cut], wide, preferred_element_type=F32)

    def hidden(p, cut, value):
        at = own if cut is own else slice(rows, 2 * rows)
        n = widths[p]
        H[p][at] = (jax.nn.silu(value[:, 0:n]) * value[:, n:2 * n]).astype(BF16)

    def down(b, p, cut, lo):
        at = own if cut is own else slice(rows, 2 * rows)
        n = widths[p]
        tall = side_of(2 * b + p, lo, slice(2 * n, 3 * n))
        return lax.dot_general(H[p][at], tall, NT, preferred_element_type=F32)

    def project(b, gaps):
        for p in TURNS[b]:
            cut = foreign[p]
            need_all(2 * b + p, False)
            begun = ACC[p][...] if b == 0 else gate_up(b, p, low, cut)
            hidden(p, cut, begun + gate_up(b, p, high, cut))
            PX[b, cut] = down(b, p, cut, other).astype(BF16)
            half_send(b, p).start()
        for p in range(2):
            PO[foreign[p]] = down(b, p, foreign[p], t)
        gaps[0]()
        for p in TURNS[b]:
            cut = foreign[p]
            half_send(b, p).wait_recv()
            S[b, p] = (PO[cut] + PR[b, cut].astype(F32)).astype(BF16)
            for k in range(2):
                for i in range(2):
                    back_send(b, p, i, k).start()
        for p in range(2):
            hidden(p, own, gate_up(b, p, low, own) + gate_up(b, p, high, own))
        PX[b, own] = (down(b, 0, own, other) + down(b, 1, own, other)).astype(BF16)
        half_send(b, 2).start()
        gaps[1]()
        PO[own] = down(b, 0, own, t) + down(b, 1, own, t)
        gaps[2]()
        half_send(b, 2).wait_recv()

    def collect(b, k):
        cut = part_of(k)
        total = PO[cut] + PR[b, cut].astype(F32)
        for p in range(2):
            back_here(b, p, k)
            total = total + R[b, p, cut].astype(F32)
        return total

    groups_here = 2
    width = half // groups_here

    def ready_pool():
        issue(8)
        maps = WB1[:, 3 * widths[1]:].reshape(2 * SIDE * SIDE, depth, 128).astype(F32)
        maps = maps.reshape(2 * SIDE * SIDE, 4, 8, 128)
        for g in range(groups_here):
            TM[g] = jnp.concatenate(
                [maps[:, g].reshape(width, 128), maps[:, 2 + g].reshape(width, 128)], axis=1
            ).astype(BF16)
            reached = 2 * 2 ** g * jnp.where(t == 0, 1, 2 ** groups_here)
            ages = lax.broadcasted_iota(jnp.int32, (rows, 128), 0) + 1
            RC[g] = 1.0 / jnp.minimum(ages, reached).astype(F32)

    def slabs(s, n):
        ref = WB[s].at[0:n * depth]
        return lambda key: remote(ref, ref, ws.at[s], wr.at[ARRIVALS[key]], mate)

    def need_all(s, mine):
        for op in COPIES:
            if op[1] == s and own_rows(op) == mine and op in WANTED:
                need(op)
        key = ("low" if mine else "high", s)
        n = sum(arrival(op) == key for op in COPIES)
        if n:
            slabs(s, n)(key).wait_recv()

    loaded(0, own_w.at[0])
    loaded(1, pw_ref)
    pack(0)
    pack(1)
    loaded(3, own_w.at[1])
    pack(2)
    pack(3)
    loaded(2, TB.at[0, t, own])
    loaded(4, wide_gain)
    loaded(5, slim_gain)
    pl.semaphore_wait(barrier, len(peers))

    issue(0)
    mate_send(0, 2, own).start()
    mate_send(0, 2, own).wait_recv()
    norm_rows(0, own)
    issue(1)
    issue(2)
    for p in range(2):
        tok_here(0, p, 0, foreign[p])
        mate_send(0, p, foreign[p]).start()
    issue(3)
    for p in range(2):
        mate_send(0, p, foreign[p]).wait_recv()
        norm_rows(0, foreign[p])
    issue(4)
    for p in TURNS[0]:
        need_all(p, True)
        ACC[p][...] = gate_up(0, p, low, foreign[p])
    issue(5)
    project(0, [lambda: issue(6), lambda: issue(7), ready_pool])

    def shifted(v, by):
        spot_ids = lax.broadcasted_iota(jnp.int32, v.shape, 0)
        return jnp.where(spot_ids >= by, pltpu.roll(v, by, 0), 0.0)

    def swap(k):
        cut = part_of(k)
        return remote(SQ.at[0, cut], SQ.at[1, cut], qs.at[0], qs.at[1 + k], mate)

    reach = 2 ** GROUPS
    for k in range(2):
        cut = part_of(k)
        after_first = (TB[0, t, cut].astype(F32) + 0.5 * collect(0, k)).astype(BF16).astype(F32)
        square = after_first * after_first
        SQ[0, cut] = sum(square[:, i * 128:(i + 1) * 128] for i in range(half // 128))
        swap(k).start()
        swap(k).wait_recv()
        total = jnp.sum(SQ[0, cut] + SQ[1, cut], axis=-1, keepdims=True)
        inv = lax.rsqrt(total / (2 * half) + epsilon)
        HB[cut] = (after_first * inv * slim_gain[0:1, :]).astype(BF16).astype(F32)
        lead = reach if k else 0
        for g in range(groups_here):
            at = slice(g * width, (g + 1) * width)
            hg = HB[cut.start - lead:cut.stop, at]
            run = hg + shifted(hg, 1)
            window = 2
            found = run
            number = t * groups_here + g
            for level in range(1, GROUPS):
                run = run + shifted(run, window)
                window = window * 2
                found = jnp.where(number >= level, run, found)
            share = jnp.concatenate([RC[g, cut]] * (width // 128), axis=1)
            diff = (found[lead:] * share - hg[lead:]).astype(BF16)
            mixed = lax.dot_general(diff, TM[g], NT, preferred_element_type=F32)
            TB[1, t, cut, at] = (after_first[:, at] + slim_gain[1:2, at] * mixed).astype(BF16)
        for p in range(2):
            for i in range(2):
                tok_send(1, p, i, k).start()
        mate_send(1, 2 + 3 * k, cut).start()

    issue(9)
    for k in range(2):
        for p in TURNS[1]:
            tok_here(1, p, k, far_part(p, k))
            mate_send(1, p + 3 * k, far_part(p, k)).start()
        if k == 0:
            for i in range(2):
                mate_send(1, 2 + 3 * i, part_of(i)).wait_recv()
            norm_rows(1, own)
        for p in TURNS[1]:
            mate_send(1, p + 3 * k, far_part(p, k)).wait_recv()
            norm_rows(1, far_part(p, k))
    for p in TURNS[1]:
        need_all(2 + p, True)
    project(1, [lambda: None] * 3)
    for k in range(2):
        cut = part_of(k)
        out_ref[cut] = (TB[1, t, cut].astype(F32) + 0.5 * collect(1, k)).astype(BF16)

    for s in range(4):
        n = sum(op[1] == s for op in COPIES)
        ref = WB[s].at[0:n * depth]
        remote(ref, ref, ws.at[s], wr.at[0], mate).wait_send()
    for b in range(2):
        remote(S.at[b], R.at[b], ts.at[b], tr.at[b, 0, 0], mate).wait_send()
        remote(S.at[b], R.at[b], rs.at[b], rr.at[b, 0, 0], mate).wait_send()
        remote(PX.at[b], PR.at[b], ms.at[b], mr.at[b, 0], mate).wait_send()
        remote(PX.at[b], PR.at[b], hs.at[b], hr.at[b, 0], mate).wait_send()
    remote(SQ.at[0], SQ.at[1], qs.at[0], qs.at[1], mate).wait_send()


def fused(
    tokens, pre_gain, first_gate, first_up, first_down, mix_gain, pool_weight,
    pool_scale, post_gain, second_gate, second_up, second_down,
):
    _, rows, half = tokens.shape
    depth, hid = first_gate.shape
    wide = 3 * hid // 10
    slim = hid // 2 - wide
    groups, width, out_cols = pool_weight.shape
    lanes = (3 * wide, 3 * slim + 128, 3 * wide, 3 * slim)

    vmem = pl.BlockSpec(memory_space=pltpu.VMEM)
    anyw = pl.BlockSpec(memory_space=pl.ANY)
    dma = pltpu.SemaphoreType.DMA
    out = pl.pallas_call(
        layer_kernel,
        out_shape=pltpu.VMEM((rows, half), BF16),
        in_specs=[anyw] * 12,
        out_specs=vmem,
        scratch_shapes=[
            pltpu.VMEM((2, 2 * half), F32),
            pltpu.VMEM((2, half), F32),
            pltpu.VMEM((groups * out_cols, width), BF16),
            pltpu.VMEM((2, 3, depth, hid), BF16),
        ]
        + [pltpu.VMEM((2, depth, n), BF16) for n in lanes]
        + [pltpu.VMEM((2 * half, n), BF16) for n in lanes]
        + [
            pltpu.VMEM((2, 2, 3 * rows, half), BF16),
            pltpu.VMEM((2, 3 * rows, half), BF16),
            pltpu.VMEM((rows, 2 * wide), F32),
            pltpu.VMEM((rows, 2 * slim), F32),
            pltpu.VMEM((2 * rows, wide), BF16),
            pltpu.VMEM((2 * rows, slim), BF16),
            pltpu.VMEM((2, 3 * rows, half), BF16),
            pltpu.VMEM((2, 3 * rows, half), BF16),
            pltpu.VMEM((3 * rows, half), F32),
            pltpu.VMEM((2, 2, rows, half), BF16),
            pltpu.VMEM((2, 2, rows, half), BF16),
            pltpu.VMEM((2, rows, 128), F32),
            pltpu.VMEM((groups, width, width), BF16),
            pltpu.VMEM((groups, rows, 128), F32),
            pltpu.VMEM((rows, half), F32),
            dma((6,)), dma((4,)), dma((len(ARRIVALS),)),
            dma((2,)), dma((2, 2, 2)), dma((2,)), dma((2, 6)), dma((2,)), dma((2, 3)),
            dma((2,)), dma((2, 2, 2)), dma((3,)),
        ],
        compiler_params=pltpu.CompilerParams(
            collective_id=0, has_side_effects=True, vmem_limit_bytes=60 * 1024 * 1024
        ),
    )(
        tokens.reshape(rows, half), pre_gain.reshape(1, -1), mix_gain.reshape(1, -1),
        pool_scale.reshape(1, -1), post_gain.reshape(1, -1),
        jnp.swapaxes(pool_weight, 1, 2).reshape(groups * out_cols, width),
        first_gate, first_up, first_down.T, second_gate, second_up, second_down.T,
    )
    return out.reshape(tokens.shape)


def solution(mesh):
    tok = P(("rep", "fs"), None, "tp")
    wide = P("fs", "tp")
    tall = P("tp", "fs")
    placed = (
        tok, P(), wide, wide, tall, P("tp"), P("tp", None, "fs"), P("tp"), P(), wide, wide, tall,
    )

    def layer(*args):
        return jax.shard_map(fused, mesh=mesh, in_specs=placed, out_specs=tok, check_vma=False)(*args)

    return layer
```

```python
import jax
import jax.numpy as jnp
from jax import lax
from jax.experimental import pallas as pl
from jax.experimental.pallas import tpu as pltpu
from jax.sharding import PartitionSpec as P

F32 = jnp.float32
BF16 = jnp.bfloat16
MESH = pl.DeviceIdType.MESH
GROUPS = 4
SIDE = 4
epsilon = 1e-06
NT = (((1,), (1,)), ((), ()))

PLAN = (
    (
        ("c", 0, 1), ("c", 1, 3), ("c", 1, 1), ("c", 0, 3), ("z", 0, 0, 0, 1), ("z", 1, 0, 0, 0), ("c", 1, 2),
        ("z", 3, 0, 0, 0), ("c", 0, 2), ("z", 2, 0, 0, 1), ("r", 0, 0, 0, 1), ("t", 1, 0), ("r", 1, 0, 0, 1),
        ("t", 0, 0),
    ),
    (
        ("z", 1, 3, 0, 1), ("z", 1, 1, 0, 0), ("r", 1, 0, 3, 1), ("r", 1, 0, 3, 0), ("r", 1, 0, 1, 0),
        ("r", 0, 0, 3, 1), ("z", 0, 3, 0, 0), ("z", 0, 1, 0, 1), ("r", 0, 0, 1, 0), ("r", 0, 0, 1, 1),
        ("r", 1, 0, 2, 1), ("z", 1, 2, 0, 0), ("r", 1, 0, 1, 1), ("r", 1, 1, 0, 1), ("r", 1, 0, 2, 0),
        ("r", 1, 1, 0, 0), ("z", 0, 2, 0, 1), ("r", 0, 0, 2, 0), ("r", 0, 0, 2, 1), ("r", 0, 0, 3, 0),
        ("f", 1, 0, 0, 1), ("z", 0, 3, 1, 0), ("z", 1, 3, 1, 1), ("f", 0, 0, 3, 1), ("r", 0, 1, 0, 1),
        ("t", 1, 1), ("z", 0, 1, 3, 1), ("f", 0, 0, 1, 0), ("z", 1, 2, 1, 0), ("f", 1, 0, 3, 0),
        ("z", 0, 1, 1, 1), ("f", 1, 0, 1, 1), ("z", 1, 1, 1, 0), ("t", 0, 1), ("c", 3, 1), ("r", 2, 0, 0, 1),
        ("r", 2, 1, 0, 1), ("f", 0, 0, 2, 0), ("z", 1, 1, 3, 0), ("r", 0, 0, 0, 0), ("r", 0, 1, 0, 0),
    ),
    (
        ("f", 1, 0, 2, 0), ("z", 1, 2, 3, 1), ("r", 1, 0, 0, 0), ("z", 0, 2, 1, 1), ("z", 0, 3, 3, 0),
        ("f", 1, 1, 0, 0), ("c", 3, 3), ("r", 2, 0, 0, 0), ("r", 2, 1, 0, 0), ("c", 3, 2), ("z", 0, 1, 2, 1),
        ("z", 1, 1, 2, 0), ("z", 0, 3, 2, 0), ("z", 0, 2, 3, 0), ("f", 0, 1, 0, 1), ("c", 2, 2), ("c", 2, 1),
        ("z", 1, 3, 2, 1), ("z", 1, 3, 3, 1), ("z", 0, 2, 2, 0), ("z", 1, 2, 2, 1), ("f", 0, 0, 0, 0),
        ("c", 2, 3),
    ),
    (
        ("z", 3, 1, 0, 0),
    ),
    (
        ("r", 3, 0, 3, 1), ("z", 3, 3, 0, 1), ("r", 3, 0, 1, 1), ("r", 3, 0, 3, 0), ("r", 3, 1, 0, 1),
        ("r", 3, 0, 1, 0), ("r", 3, 0, 0, 1), ("r", 3, 0, 0, 0), ("r", 3, 1, 0, 0), ("r", 2, 0, 2, 0),
        ("r", 2, 0, 2, 1), ("z", 2, 2, 0, 1), ("r", 2, 0, 1, 0), ("r", 2, 0, 1, 1),
    ),
    (
        ("z", 3, 3, 1, 1), ("z", 2, 3, 0, 0), ("r", 2, 0, 3, 1), ("r", 2, 0, 3, 0),
    ),
    (
        ("f", 3, 0, 1, 1), ("z", 3, 1, 1, 0), ("z", 3, 2, 0, 1), ("r", 3, 0, 2, 1), ("z", 3, 3, 3, 1),
        ("f", 3, 0, 3, 0), ("z", 2, 1, 0, 1), ("z", 2, 2, 3, 0),
    ),
    (
        ("z", 2, 1, 1, 1), ("z", 2, 1, 3, 1), ("z", 2, 2, 1, 1), ("f", 2, 0, 1, 0), ("f", 2, 0, 2, 0),
        ("f", 2, 0, 0, 0), ("z", 3, 1, 2, 0), ("r", 3, 1, 2, 1), ("f", 3, 0, 0, 1), ("r", 3, 0, 2, 0),
        ("r", 3, 1, 2, 0), ("f", 3, 1, 0, 0), ("f", 2, 0, 3, 1), ("z", 2, 3, 3, 0), ("f", 2, 1, 0, 1),
        ("z", 2, 3, 1, 0), ("z", 3, 1, 3, 0),
    ),
    (

    ),
    (
        ("f", 3, 1, 2, 1), ("z", 2, 1, 2, 1), ("z", 2, 3, 2, 0), ("z", 3, 3, 2, 1), ("f", 3, 0, 2, 0),
        ("z", 2, 2, 2, 0),
    ),
)

TURNS = ((1, 0), (0, 1))
WAVES = [op for part in PLAN for op in part]
RING_SIDE = {(op[1], op[3]): op[4] for op in WAVES if op[0] == "f" and op[2] == 0}
RISE = {op[1:4]: op[4] for op in WAVES if op[0] == "z"}
def sources(op):
    kind, s = op[:2]
    if kind == "c" or kind == "t":
        return []
    if kind == "r":
        _, _, comp, j, _ = op
        if comp:
            return [("z", s, j, 0, RISE[s, j, 0])]
        return [("c", s, j)] if j else []
    if kind == "f":
        return [("r",) + op[1:]]
    _, _, j, c, _ = op
    if c == 0:
        return [("c", s, j)] if j else []
    if c == 2:
        return [("f", s, 0, j, RING_SIDE[s, j])]
    return [("r", s, 0, j, 0 if c == 3 else 1)]


def own_rows(op):
    return op[0] == "c" or (op[0] in "rf" and op[2] == 0)


COPIES = [op for op in WAVES if op[0] != "t"]
WANTED = {source for op in COPIES for source in sources(op)}


def arrival(op):
    return op if op in WANTED else ("low" if own_rows(op) else "high", op[1])


ARRIVALS = {key: i for i, key in enumerate(dict.fromkeys(arrival(op) for op in COPIES))}


def layer_kernel(
    tok_hbm, pre_hbm, mixg_hbm, scale_hbm, post_hbm, pw_hbm,
    g1_hbm, u1_hbm, d1_hbm, g2_hbm, u2_hbm, d2_hbm, out_ref,
    wide_gain, slim_gain, pw_ref, own_w,
    WS0, WS1, WS2, WS3, WB0, WB1, WB2, WB3, TB, N, ACC0, ACC1, H0, H1, PX, PR, PO, S, R, SQ, TM, RC, HB,
    ls, ws, wr, ts, tr, ms, mr, hs, hr, rs, rr, qs,
):
    rep = lax.axis_index("rep")
    fs = lax.axis_index("fs")
    t = lax.axis_index("tp")
    x = lax.rem(fs, SIDE)
    y = lax.rem(fs // SIDE, SIDE)
    low = fs // (SIDE * SIDE)
    z = 2 * rep + low
    other = 1 - t
    high = 1 - low

    def dev(dx, dy, dz, tt):
        xx = lax.rem(x + dx, SIDE)
        yy = lax.rem(y + dy, SIDE)
        zz = lax.rem(z + dz, SIDE)
        return {"rep": zz // 2, "fs": lax.rem(zz, 2) * (SIDE * SIDE) + yy * SIDE + xx, "tp": tt}

    mate = dev(0, 0, 0, other)
    along_x = {d: dev(d, 0, 0, t) for d in (1, 2, 3)}
    along_y = {d: dev(0, d, 0, t) for d in (1, 2, 3)}
    along_z = {d: dev(0, 0, d, t) for d in (1, 3)}
    peers = [mate] + list(along_x.values()) + list(along_y.values()) + list(along_z.values())

    barrier = pltpu.get_barrier_semaphore()
    for peer in peers:
        pl.semaphore_signal(barrier, inc=1, device_id=peer, device_id_type=MESH)

    rows, half = out_ref.shape
    def remote(src, dst, ss, sr, to):
        return pltpu.make_async_remote_copy(
            src_ref=src, dst_ref=dst, send_sem=ss, recv_sem=sr, device_id=to, device_id_type=MESH
        )

    depth, hid = g1_hbm.shape
    loads = [
        pltpu.make_async_copy(src, dst, ls.at[i])
        for i, src, dst in (
            (0, g1_hbm, own_w.at[0, 0]), (0, u1_hbm, own_w.at[0, 1]), (0, d1_hbm, own_w.at[0, 2]),
            (1, pw_hbm, pw_ref), (2, tok_hbm, TB.at[0, t, 0:rows]),
            (3, g2_hbm, own_w.at[1, 0]), (3, u2_hbm, own_w.at[1, 1]), (3, d2_hbm, own_w.at[1, 2]),
            (4, pre_hbm, wide_gain.at[0:1]), (4, post_hbm, wide_gain.at[1:2]),
            (5, mixg_hbm, slim_gain.at[0:1]), (5, scale_hbm, slim_gain.at[1:2]),
        )
    ]
    for load in loads:
        load.start()

    def loaded(i, ref):
        pltpu.make_async_copy(ref, ref, ls.at[i]).wait()

    piece = rows // 2
    widths = (H0.shape[1], H1.shape[1])
    WS = (WS0, WS1, WS2, WS3)
    WB = (WB0, WB1, WB2, WB3)
    ACC = (ACC0, ACC1)
    H = (H0, H1)
    axes = (along_x, along_y)
    turn = (0, 1, 1, 0)
    places = (x, y)

    def slab(s, lo, j, c):
        a = lax.rem(places[turn[s]] + j, SIDE)
        c = lax.rem(places[1 - turn[s]] + c, SIDE)
        yy, xx = (c, a) if turn[s] == 0 else (a, c)
        start = ((lo * SIDE + yy) * SIDE + xx) * depth
        return WB[s].at[pl.ds(pl.multiple_of(start, depth), depth)]

    def side_of(s, lo, lanes):
        return WB[s][pl.ds(pl.multiple_of(lo * half, half), half), lanes]

    def pack(s):
        b, p = divmod(s, 2)
        n = widths[p]
        start = 2 * widths[0] * p
        for k in range(2):
            for i in range(3):
                WS[s][k, :, i * n:(i + 1) * n] = own_w[b, i, :, start + k * n:start + (k + 1) * n]
            if s == 1:
                flat = pw_ref[...]
                for i in range(2):
                    WS[s][k, i * 16:(i + 1) * 16, 3 * n:] = flat[:, i * 128:(i + 1) * 128]
        start = ((low * SIDE + y) * SIDE + x) * depth
        WB[s][pl.ds(pl.multiple_of(start, depth), depth)] = WS[s][lax.rem(places[turn[s]], 2)]

    def copy_of(op):
        kind = op[0]
        s = op[1]
        axis, ring = axes[turn[s]], axes[1 - turn[s]]
        sems = (ws.at[s], wr.at[ARRIVALS[arrival(op)]])
        if kind == "c":
            d = SIDE - op[2]
            src = WS[s].at[lax.rem(places[turn[s]] + d, 2)]
            return remote(src, slab(s, low, 0, 0), *sems, axis[d])
        if kind == "r":
            _, _, comp, j, side = op
            ref = slab(s, high if comp else low, j, 0)
            return remote(ref, ref, *sems, ring[(1, 3)[side]])
        if kind == "f":
            _, _, comp, j, side = op
            ref = slab(s, high if comp else low, j, (3, 1)[side])
            return remote(ref, ref, *sems, ring[(1, 3)[side]])
        _, _, j, c, up = op
        ref = slab(s, low, j, c)
        return remote(ref, ref, *sems, along_z[1 if up else 3])

    here = set()

    def need(op):
        if op not in here:
            here.add(op)
            copy_of(op).wait_recv()

    def issue(part):
        for op in PLAN[part]:
            for source in sources(op):
                need(source)
            if op[0] == "t":
                for k in range(2):
                    tok_send(0, op[1], op[2], k).start()
            else:
                copy_of(op).start()

    def base(p):
        return rows * (1 + p)

    own = slice(0, rows)
    foreign = tuple(slice(base(p), base(p) + rows) for p in range(2))

    def axis_of(b, p):
        return axes[turn[2 * b + p]]

    def part_of(k):
        return slice(k * piece, (k + 1) * piece)

    def far_part(p, k):
        return slice(base(p) + k * piece, base(p) + (k + 1) * piece)

    def strip(i, k):
        return slice(k * piece + i * piece // 2, k * piece + (i + 1) * piece // 2)

    def tok_send(b, p, i, k):
        cut = strip(i, k)
        src = TB.at[b, t, cut]
        dst = TB.at[b, t, base(p) + cut.start:base(p) + cut.stop]
        return remote(src, dst, ts.at[b], tr.at[b, p, k * b], axis_of(b, p)[(1, 3)[i]])

    def tok_here(b, p, k, cut):
        ref = TB.at[b, t, cut]
        remote(ref, ref, ts.at[b], tr.at[b, p, k], mate).wait_recv()

    def mate_send(b, n, cut):
        ref = TB.at[b, t, cut]
        return remote(ref, ref, ms.at[b], mr.at[b, n], mate)

    def half_send(b, n):
        cut = own if n == 2 else foreign[n]
        return remote(PX.at[b, cut], PR.at[b, cut], hs.at[b], hr.at[b, n], mate)

    def back_send(b, p, i, k):
        cut = strip(i, k)
        return remote(S.at[b, p, cut], R.at[b, p, cut], rs.at[b], rr.at[b, p, k], axis_of(b, p)[(3, 1)[i]])

    def back_here(b, p, k):
        cut = part_of(k)
        remote(S.at[b, p, cut], R.at[b, p, cut], rs.at[b], rr.at[b, p, k], mate).wait_recv()

    def norm_rows(b, cut):
        parts = [TB[b, c, cut].astype(F32) for c in range(2)]
        total = sum(jnp.sum(v * v, axis=-1, keepdims=True) for v in parts)
        inv = lax.rsqrt(total / (2 * half) + epsilon)
        for c in range(2):
            N[c, cut] = (parts[c] * inv * wide_gain[b:b + 1, c * half:(c + 1) * half]).astype(BF16)

    def gate_up(b, p, lo, cut):
        wide = side_of(2 * b + p, lo, slice(0, 2 * widths[p]))
        return jnp.dot(N[lo, cut], wide, preferred_element_type=F32)

    def hidden(p, cut, value):
        at = own if cut is own else slice(rows, 2 * rows)
        n = widths[p]
        H[p][at] = (jax.nn.silu(value[:, 0:n]) * value[:, n:2 * n]).astype(BF16)

    def down(b, p, cut, lo):
        at = own if cut is own else slice(rows, 2 * rows)
        n = widths[p]
        tall = side_of(2 * b + p, lo, slice(2 * n, 3 * n))
        return lax.dot_general(H[p][at], tall, NT, preferred_element_type=F32)

    def project(b, gaps):
        for p in TURNS[b]:
            cut = foreign[p]
            need_all(2 * b + p, False)
            begun = ACC[p][...] if b == 0 else gate_up(b, p, low, cut)
            hidden(p, cut, begun + gate_up(b, p, high, cut))
            PX[b, cut] = down(b, p, cut, other).astype(BF16)
            half_send(b, p).start()
        for p in range(2):
            PO[foreign[p]] = down(b, p, foreign[p], t)
        gaps[0]()
        for p in TURNS[b]:
            cut = foreign[p]
            half_send(b, p).wait_recv()
            S[b, p] = (PO[cut] + PR[b, cut].astype(F32)).astype(BF16)
            for k in range(2):
                for i in range(2):
                    back_send(b, p, i, k).start()
        for p in range(2):
            hidden(p, own, gate_up(b, p, low, own) + gate_up(b, p, high, own))
        PX[b, own] = (down(b, 0, own, other) + down(b, 1, own, other)).astype(BF16)
        half_send(b, 2).start()
        gaps[1]()
        PO[own] = down(b, 0, own, t) + down(b, 1, own, t)
        gaps[2]()
        half_send(b, 2).wait_recv()

    def collect(b, k):
        cut = part_of(k)
        total = PO[cut] + PR[b, cut].astype(F32)
        for p in range(2):
            back_here(b, p, k)
            total = total + R[b, p, cut].astype(F32)
        return total

    groups_here = 2
    width = half // groups_here

    def ready_pool():
        issue(8)
        maps = WB1[:, 3 * widths[1]:].reshape(2 * SIDE * SIDE, depth, 128).astype(F32)
        maps = maps.reshape(2 * SIDE * SIDE, 4, 8, 128)
        for g in range(groups_here):
            TM[g] = jnp.concatenate(
                [maps[:, g].reshape(width, 128), maps[:, 2 + g].reshape(width, 128)], axis=1
            ).astype(BF16)
            reached = 2 * 2 ** g * jnp.where(t == 0, 1, 2 ** groups_here)
            ages = lax.broadcasted_iota(jnp.int32, (rows, 128), 0) + 1
            RC[g] = 1.0 / jnp.minimum(ages, reached).astype(F32)

    def slabs(s, n):
        ref = WB[s].at[0:n * depth]
        return lambda key: remote(ref, ref, ws.at[s], wr.at[ARRIVALS[key]], mate)

    def need_all(s, mine):
        for op in COPIES:
            if op[1] == s and own_rows(op) == mine and op in WANTED:
                need(op)
        key = ("low" if mine else "high", s)
        n = sum(arrival(op) == key for op in COPIES)
        if n:
            slabs(s, n)(key).wait_recv()

    loaded(0, own_w.at[0])
    loaded(1, pw_ref)
    pack(0)
    pack(1)
    loaded(3, own_w.at[1])
    pack(2)
    pack(3)
    loaded(2, TB.at[0, t, own])
    loaded(4, wide_gain)
    loaded(5, slim_gain)
    pl.semaphore_wait(barrier, len(peers))

    issue(0)
    mate_send(0, 2, own).start()
    mate_send(0, 2, own).wait_recv()
    norm_rows(0, own)
    issue(1)
    issue(2)
    for p in range(2):
        tok_here(0, p, 0, foreign[p])
        mate_send(0, p, foreign[p]).start()
    issue(3)
    for p in range(2):
        mate_send(0, p, foreign[p]).wait_recv()
        norm_rows(0, foreign[p])
    issue(4)
    for p in TURNS[0]:
        need_all(p, True)
        ACC[p][...] = gate_up(0, p, low, foreign[p])
    issue(5)
    project(0, [lambda: issue(6), lambda: issue(7), ready_pool])

    def shifted(v, by):
        spot_ids = lax.broadcasted_iota(jnp.int32, v.shape, 0)
        return jnp.where(spot_ids >= by, pltpu.roll(v, by, 0), 0.0)

    def swap(k):
        cut = part_of(k)
        return remote(SQ.at[0, cut], SQ.at[1, cut], qs.at[0], qs.at[1 + k], mate)

    reach = 2 ** GROUPS
    for k in range(2):
        cut = part_of(k)
        after_first = (TB[0, t, cut].astype(F32) + 0.5 * collect(0, k)).astype(BF16).astype(F32)
        square = after_first * after_first
        SQ[0, cut] = sum(square[:, i * 128:(i + 1) * 128] for i in range(half // 128))
        swap(k).start()
        swap(k).wait_recv()
        total = jnp.sum(SQ[0, cut] + SQ[1, cut], axis=-1, keepdims=True)
        inv = lax.rsqrt(total / (2 * half) + epsilon)
        HB[cut] = (after_first * inv * slim_gain[0:1, :]).astype(BF16).astype(F32)
        lead = reach if k else 0
        for g in range(groups_here):
            at = slice(g * width, (g + 1) * width)
            hg = HB[cut.start - lead:cut.stop, at]
            run = hg + shifted(hg, 1)
            window = 2
            found = run
            number = t * groups_here + g
            for level in range(1, GROUPS):
                run = run + shifted(run, window)
                window = window * 2
                found = jnp.where(number >= level, run, found)
            share = jnp.concatenate([RC[g, cut]] * (width // 128), axis=1)
            diff = (found[lead:] * share - hg[lead:]).astype(BF16)
            mixed = lax.dot_general(diff, TM[g], NT, preferred_element_type=F32)
            TB[1, t, cut, at] = (after_first[:, at] + slim_gain[1:2, at] * mixed).astype(BF16)
        for p in range(2):
            for i in range(2):
                tok_send(1, p, i, k).start()
        mate_send(1, 2 + 3 * k, cut).start()

    issue(9)
    for k in range(2):
        for p in TURNS[1]:
            tok_here(1, p, k, far_part(p, k))
            mate_send(1, p + 3 * k, far_part(p, k)).start()
        if k == 0:
            for i in range(2):
                mate_send(1, 2 + 3 * i, part_of(i)).wait_recv()
            norm_rows(1, own)
        for p in TURNS[1]:
            mate_send(1, p + 3 * k, far_part(p, k)).wait_recv()
            norm_rows(1, far_part(p, k))
    for p in TURNS[1]:
        need_all(2 + p, True)
    project(1, [lambda: None] * 3)
    for k in range(2):
        cut = part_of(k)
        out_ref[cut] = (TB[1, t, cut].astype(F32) + 0.5 * collect(1, k)).astype(BF16)

    for s in range(4):
        n = sum(op[1] == s for op in COPIES)
        ref = WB[s].at[0:n * depth]
        remote(ref, ref, ws.at[s], wr.at[0], mate).wait_send()
    for b in range(2):
        remote(S.at[b], R.at[b], ts.at[b], tr.at[b, 0, 0], mate).wait_send()
        remote(S.at[b], R.at[b], rs.at[b], rr.at[b, 0, 0], mate).wait_send()
        remote(PX.at[b], PR.at[b], ms.at[b], mr.at[b, 0], mate).wait_send()
        remote(PX.at[b], PR.at[b], hs.at[b], hr.at[b, 0], mate).wait_send()
    remote(SQ.at[0], SQ.at[1], qs.at[0], qs.at[1], mate).wait_send()


def fused(
    tokens, pre_gain, first_gate, first_up, first_down, mix_gain, pool_weight,
    pool_scale, post_gain, second_gate, second_up, second_down,
):
    _, rows, half = tokens.shape
    depth, hid = first_gate.shape
    wide = 3 * hid // 10
    slim = hid // 2 - wide
    groups, width, out_cols = pool_weight.shape
    lanes = (3 * wide, 3 * slim + 128, 3 * wide, 3 * slim)

    vmem = pl.BlockSpec(memory_space=pltpu.VMEM)
    anyw = pl.BlockSpec(memory_space=pl.ANY)
    dma = pltpu.SemaphoreType.DMA
    out = pl.pallas_call(
        layer_kernel,
        out_shape=pltpu.VMEM((rows, half), BF16),
        in_specs=[anyw] * 12,
        out_specs=vmem,
        scratch_shapes=[
            pltpu.VMEM((2, 2 * half), F32),
            pltpu.VMEM((2, half), F32),
            pltpu.VMEM((groups * out_cols, width), BF16),
            pltpu.VMEM((2, 3, depth, hid), BF16),
        ]
        + [pltpu.VMEM((2, depth, n), BF16) for n in lanes]
        + [pltpu.VMEM((2 * half, n), BF16) for n in lanes]
        + [
            pltpu.VMEM((2, 2, 3 * rows, half), BF16),
            pltpu.VMEM((2, 3 * rows, half), BF16),
            pltpu.VMEM((rows, 2 * wide), F32),
            pltpu.VMEM((rows, 2 * slim), F32),
            pltpu.VMEM((2 * rows, wide), BF16),
            pltpu.VMEM((2 * rows, slim), BF16),
            pltpu.VMEM((2, 3 * rows, half), BF16),
            pltpu.VMEM((2, 3 * rows, half), BF16),
            pltpu.VMEM((3 * rows, half), F32),
            pltpu.VMEM((2, 2, rows, half), BF16),
            pltpu.VMEM((2, 2, rows, half), BF16),
            pltpu.VMEM((2, rows, 128), F32),
            pltpu.VMEM((groups, width, width), BF16),
            pltpu.VMEM((groups, rows, 128), F32),
            pltpu.VMEM((rows, half), F32),
            dma((6,)), dma((4,)), dma((len(ARRIVALS),)),
            dma((2,)), dma((2, 2, 2)), dma((2,)), dma((2, 6)), dma((2,)), dma((2, 3)),
            dma((2,)), dma((2, 2, 2)), dma((3,)),
        ],
        compiler_params=pltpu.CompilerParams(
            collective_id=0, has_side_effects=True, vmem_limit_bytes=60 * 1024 * 1024
        ),
    )(
        tokens.reshape(rows, half), pre_gain.reshape(1, -1), mix_gain.reshape(1, -1),
        pool_scale.reshape(1, -1), post_gain.reshape(1, -1),
        jnp.swapaxes(pool_weight, 1, 2).reshape(groups * out_cols, width),
        first_gate, first_up, first_down.T, second_gate, second_up, second_down.T,
    )
    return out.reshape(tokens.shape)


def solution(mesh):
    tok = P(("rep", "fs"), None, "tp")
    wide = P("fs", "tp")
    tall = P("tp", "fs")
    placed = (
        tok, P(), wide, wide, tall, P("tp"), P("tp", None, "fs"), P("tp"), P(), wide, wide, tall,
    )

    def layer(*args):
        return jax.shard_map(fused, mesh=mesh, in_specs=placed, out_specs=tok, check_vma=False)(*args)

    return layer
```

```python
import jax
import jax.numpy as jnp
from jax import lax
from jax.experimental import pallas as pl
from jax.experimental.pallas import tpu as pltpu
from jax.sharding import PartitionSpec as P

F32 = jnp.float32
BF16 = jnp.bfloat16
MESH = pl.DeviceIdType.MESH
GROUPS = 4
SIDE = 4
epsilon = 1e-06
NT = (((1,), (1,)), ((), ()))

PLAN = (
    (
        ("c", 0, 1), ("c", 1, 3), ("c", 1, 1), ("c", 0, 3), ("z", 0, 0, 0, 1), ("z", 1, 0, 0, 0), ("c", 1, 2),
        ("z", 3, 0, 0, 0), ("c", 0, 2), ("z", 2, 0, 0, 1), ("r", 0, 0, 0, 1), ("t", 1, 0), ("r", 1, 0, 0, 1),
        ("t", 0, 0),
    ),
    (
        ("z", 1, 3, 0, 1), ("z", 1, 1, 0, 0), ("r", 1, 0, 3, 1), ("r", 1, 0, 3, 0), ("r", 1, 0, 1, 0),
        ("r", 0, 0, 3, 1), ("z", 0, 3, 0, 0), ("z", 0, 1, 0, 1), ("r", 0, 0, 1, 0), ("r", 0, 0, 1, 1),
        ("r", 1, 0, 2, 1), ("z", 1, 2, 0, 0), ("r", 1, 0, 1, 1), ("r", 1, 1, 0, 1), ("r", 1, 0, 2, 0),
        ("r", 1, 1, 0, 0), ("z", 0, 2, 0, 1), ("r", 0, 0, 2, 0), ("r", 0, 0, 2, 1), ("r", 0, 0, 3, 0),
        ("f", 1, 0, 0, 1), ("z", 0, 3, 1, 0), ("z", 1, 3, 1, 1), ("f", 0, 0, 3, 1), ("r", 0, 1, 0, 1),
        ("t", 1, 1), ("z", 0, 1, 3, 1), ("f", 0, 0, 1, 0), ("z", 1, 2, 1, 0), ("f", 1, 0, 3, 0),
        ("z", 0, 1, 1, 1), ("f", 1, 0, 1, 1), ("z", 1, 1, 1, 0), ("t", 0, 1), ("c", 3, 1), ("r", 2, 0, 0, 1),
        ("r", 2, 1, 0, 1), ("f", 0, 0, 2, 0), ("z", 1, 1, 3, 0), ("r", 0, 0, 0, 0), ("r", 0, 1, 0, 0),
    ),
    (
        ("f", 1, 0, 2, 0), ("z", 1, 2, 3, 1), ("r", 1, 0, 0, 0), ("z", 0, 2, 1, 1), ("z", 0, 3, 3, 0),
        ("f", 1, 1, 0, 0), ("c", 3, 3), ("r", 2, 0, 0, 0), ("r", 2, 1, 0, 0), ("c", 3, 2), ("z", 0, 1, 2, 1),
        ("z", 1, 1, 2, 0), ("z", 0, 3, 2, 0), ("z", 0, 2, 3, 0), ("f", 0, 1, 0, 1), ("c", 2, 2), ("c", 2, 1),
        ("z", 1, 3, 2, 1), ("z", 1, 3, 3, 1), ("z", 0, 2, 2, 0), ("z", 1, 2, 2, 1), ("f", 0, 0, 0, 0),
        ("c", 2, 3),
    ),
    (
        ("z", 3, 1, 0, 0), ("r", 3, 0, 3, 1), ("z", 3, 3, 0, 1), ("r", 3, 0, 1, 1), ("r", 3, 0, 3, 0),
        ("r", 3, 1, 0, 1), ("r", 3, 0, 1, 0), ("r", 3, 0, 0, 1), ("r", 3, 0, 0, 0), ("r", 3, 1, 0, 0),
    ),
    (
        ("r", 2, 0, 2, 0), ("r", 2, 0, 2, 1), ("z", 2, 2, 0, 1), ("r", 2, 0, 1, 0), ("r", 2, 0, 1, 1),
    ),
    (
        ("z", 3, 3, 1, 1), ("z", 2, 3, 0, 0), ("r", 2, 0, 3, 1), ("r", 2, 0, 3, 0),
    ),
    (
        ("f", 3, 0, 1, 1), ("z", 3, 1, 1, 0), ("z", 3, 2, 0, 1), ("r", 3, 0, 2, 1), ("z", 3, 3, 3, 1),
        ("f", 3, 0, 3, 0), ("z", 2, 1, 0, 1), ("z", 2, 2, 3, 0),
    ),
    (
        ("z", 2, 1, 1, 1), ("z", 2, 1, 3, 1), ("z", 2, 2, 1, 1), ("f", 2, 0, 1, 0), ("f", 2, 0, 2, 0),
        ("f", 2, 0, 0, 0), ("z", 3, 1, 2, 0), ("r", 3, 1, 2, 1), ("f", 3, 0, 0, 1), ("r", 3, 0, 2, 0),
        ("r", 3, 1, 2, 0), ("f", 3, 1, 0, 0), ("f", 2, 0, 3, 1), ("z", 2, 3, 3, 0), ("f", 2, 1, 0, 1),
        ("z", 2, 3, 1, 0), ("z", 3, 1, 3, 0),
    ),
    (

    ),
    (
        ("f", 3, 1, 2, 1), ("z", 2, 1, 2, 1), ("z", 2, 3, 2, 0), ("z", 3, 3, 2, 1), ("f", 3, 0, 2, 0),
        ("z", 2, 2, 2, 0),
    ),
)

TURNS = ((1, 0), (0, 1))
WAVES = [op for part in PLAN for op in part]
RING_SIDE = {(op[1], op[3]): op[4] for op in WAVES if op[0] == "f" and op[2] == 0}
RISE = {op[1:4]: op[4] for op in WAVES if op[0] == "z"}
def sources(op):
    kind, s = op[:2]
    if kind == "c" or kind == "t":
        return []
    if kind == "r":
        _, _, comp, j, _ = op
        if comp:
            return [("z", s, j, 0, RISE[s, j, 0])]
        return [("c", s, j)] if j else []
    if kind == "f":
        return [("r",) + op[1:]]
    _, _, j, c, _ = op
    if c == 0:
        return [("c", s, j)] if j else []
    if c == 2:
        return [("f", s, 0, j, RING_SIDE[s, j])]
    return [("r", s, 0, j, 0 if c == 3 else 1)]


def own_rows(op):
    return op[0] == "c" or (op[0] in "rf" and op[2] == 0)


COPIES = [op for op in WAVES if op[0] != "t"]
WANTED = {source for op in COPIES for source in sources(op)}


def arrival(op):
    return op if op in WANTED else ("low" if own_rows(op) else "high", op[1])


ARRIVALS = {key: i for i, key in enumerate(dict.fromkeys(arrival(op) for op in COPIES))}


def layer_kernel(
    tok_hbm, pre_hbm, mixg_hbm, scale_hbm, post_hbm, pw_hbm,
    g1_hbm, u1_hbm, d1_hbm, g2_hbm, u2_hbm, d2_hbm, out_ref,
    wide_gain, slim_gain, pw_ref, own_w,
    WS0, WS1, WS2, WS3, WB0, WB1, WB2, WB3, TB, N, ACC0, ACC1, H0, H1, PX, PR, PO, S, R, SQ, TM, RC, HB,
    ls, ws, wr, ts, tr, ms, mr, hs, hr, rs, rr, qs,
):
    rep = lax.axis_index("rep")
    fs = lax.axis_index("fs")
    t = lax.axis_index("tp")
    x = lax.rem(fs, SIDE)
    y = lax.rem(fs // SIDE, SIDE)
    low = fs // (SIDE * SIDE)
    z = 2 * rep + low
    other = 1 - t
    high = 1 - low

    def dev(dx, dy, dz, tt):
        xx = lax.rem(x + dx, SIDE)
        yy = lax.rem(y + dy, SIDE)
        zz = lax.rem(z + dz, SIDE)
        return {"rep": zz // 2, "fs": lax.rem(zz, 2) * (SIDE * SIDE) + yy * SIDE + xx, "tp": tt}

    mate = dev(0, 0, 0, other)
    along_x = {d: dev(d, 0, 0, t) for d in (1, 2, 3)}
    along_y = {d: dev(0, d, 0, t) for d in (1, 2, 3)}
    along_z = {d: dev(0, 0, d, t) for d in (1, 3)}
    peers = [along_x[2], along_y[2]] + [axis[d] for axis in (along_x, along_y, along_z) for d in (1, 3)] + [mate]

    barrier = pltpu.get_barrier_semaphore()
    for peer in peers:
        pl.semaphore_signal(barrier, inc=1, device_id=peer, device_id_type=MESH)

    rows, half = out_ref.shape
    def remote(src, dst, ss, sr, to):
        return pltpu.make_async_remote_copy(
            src_ref=src, dst_ref=dst, send_sem=ss, recv_sem=sr, device_id=to, device_id_type=MESH
        )

    depth, hid = g1_hbm.shape
    loads = [
        pltpu.make_async_copy(src, dst, ls.at[i])
        for i, src, dst in (
            (0, g1_hbm, own_w.at[0, 0]), (0, u1_hbm, own_w.at[0, 1]), (0, d1_hbm, own_w.at[0, 2]),
            (1, pw_hbm, pw_ref), (2, tok_hbm, TB.at[0, t, 0:rows]),
            (3, g2_hbm, own_w.at[1, 0]), (3, u2_hbm, own_w.at[1, 1]), (3, d2_hbm, own_w.at[1, 2]),
            (4, pre_hbm, wide_gain.at[0:1]), (4, post_hbm, wide_gain.at[1:2]),
            (5, mixg_hbm, slim_gain.at[0:1]), (5, scale_hbm, slim_gain.at[1:2]),
        )
    ]
    for load in loads:
        load.start()

    def loaded(i, ref):
        pltpu.make_async_copy(ref, ref, ls.at[i]).wait()

    piece = rows // 2
    widths = (H0.shape[1], H1.shape[1])
    WS = (WS0, WS1, WS2, WS3)
    WB = (WB0, WB1, WB2, WB3)
    ACC = (ACC0, ACC1)
    H = (H0, H1)
    axes = (along_x, along_y)
    turn = (0, 1, 1, 0)
    places = (x, y)

    def slab(s, lo, j, c):
        a = lax.rem(places[turn[s]] + j, SIDE)
        c = lax.rem(places[1 - turn[s]] + c, SIDE)
        yy, xx = (c, a) if turn[s] == 0 else (a, c)
        start = ((lo * SIDE + yy) * SIDE + xx) * depth
        return WB[s].at[pl.ds(pl.multiple_of(start, depth), depth)]

    def side_of(s, lo, lanes):
        return WB[s][pl.ds(pl.multiple_of(lo * half, half), half), lanes]

    def pack(s):
        b, p = divmod(s, 2)
        n = widths[p]
        start = 2 * widths[0] * p
        for k in range(2):
            for i in range(3):
                WS[s][k, :, i * n:(i + 1) * n] = own_w[b, i, :, start + k * n:start + (k + 1) * n]
            if s == 1:
                flat = pw_ref[...]
                for i in range(2):
                    WS[s][k, i * 16:(i + 1) * 16, 3 * n:] = flat[:, i * 128:(i + 1) * 128]
        start = ((low * SIDE + y) * SIDE + x) * depth
        WB[s][pl.ds(pl.multiple_of(start, depth), depth)] = WS[s][lax.rem(places[turn[s]], 2)]

    def copy_of(op):
        kind = op[0]
        s = op[1]
        axis, ring = axes[turn[s]], axes[1 - turn[s]]
        sems = (ws.at[s], wr.at[ARRIVALS[arrival(op)]])
        if kind == "c":
            d = SIDE - op[2]
            src = WS[s].at[lax.rem(places[turn[s]] + d, 2)]
            return remote(src, slab(s, low, 0, 0), *sems, axis[d])
        if kind == "r":
            _, _, comp, j, side = op
            ref = slab(s, high if comp else low, j, 0)
            return remote(ref, ref, *sems, ring[(1, 3)[side]])
        if kind == "f":
            _, _, comp, j, side = op
            ref = slab(s, high if comp else low, j, (3, 1)[side])
            return remote(ref, ref, *sems, ring[(1, 3)[side]])
        _, _, j, c, up = op
        ref = slab(s, low, j, c)
        return remote(ref, ref, *sems, along_z[1 if up else 3])

    here = set()

    def need(op):
        if op not in here:
            here.add(op)
            copy_of(op).wait_recv()

    def issue(part):
        for op in PLAN[part]:
            for source in sources(op):
                need(source)
            if op[0] == "t":
                for k in range(2):
                    tok_send(0, op[1], op[2], k).start()
            else:
                copy_of(op).start()

    def base(p):
        return rows * (1 + p)

    own = slice(0, rows)
    foreign = tuple(slice(base(p), base(p) + rows) for p in range(2))

    def axis_of(b, p):
        return axes[turn[2 * b + p]]

    def part_of(k):
        return slice(k * piece, (k + 1) * piece)

    def far_part(p, k):
        return slice(base(p) + k * piece, base(p) + (k + 1) * piece)

    def strip(i, k):
        return slice(k * piece + i * piece // 2, k * piece + (i + 1) * piece // 2)

    def tok_send(b, p, i, k):
        cut = strip(i, k)
        src = TB.at[b, t, cut]
        dst = TB.at[b, t, base(p) + cut.start:base(p) + cut.stop]
        return remote(src, dst, ts.at[b], tr.at[b, p, k * b], axis_of(b, p)[(1, 3)[i]])

    def tok_here(b, p, k, cut):
        ref = TB.at[b, t, cut]
        remote(ref, ref, ts.at[b], tr.at[b, p, k], mate).wait_recv()

    def mate_send(b, n, cut):
        ref = TB.at[b, t, cut]
        return remote(ref, ref, ms.at[b], mr.at[b, n], mate)

    def half_send(b, n):
        cut = own if n == 2 else foreign[n]
        return remote(PX.at[b, cut], PR.at[b, cut], hs.at[b], hr.at[b, n], mate)

    def back_send(b, p, i, k):
        cut = strip(i, k)
        return remote(S.at[b, p, cut], R.at[b, p, cut], rs.at[b], rr.at[b, p, k], axis_of(b, p)[(3, 1)[i]])

    def back_here(b, p, k):
        cut = part_of(k)
        remote(S.at[b, p, cut], R.at[b, p, cut], rs.at[b], rr.at[b, p, k], mate).wait_recv()

    def norm_rows(b, cut):
        parts = [TB[b, c, cut].astype(F32) for c in range(2)]
        total = sum(jnp.sum(v * v, axis=-1, keepdims=True) for v in parts)
        inv = lax.rsqrt(total / (2 * half) + epsilon)
        for c in range(2):
            N[c, cut] = (parts[c] * inv * wide_gain[b:b + 1, c * half:(c + 1) * half]).astype(BF16)

    def gate_up(b, p, lo, cut):
        wide = side_of(2 * b + p, lo, slice(0, 2 * widths[p]))
        return jnp.dot(N[lo, cut], wide, preferred_element_type=F32)

    def hidden(p, cut, value):
        at = own if cut is own else slice(rows, 2 * rows)
        n = widths[p]
        H[p][at] = (jax.nn.silu(value[:, 0:n]) * value[:, n:2 * n]).astype(BF16)

    def down(b, p, cut, lo):
        at = own if cut is own else slice(rows, 2 * rows)
        n = widths[p]
        tall = side_of(2 * b + p, lo, slice(2 * n, 3 * n))
        return lax.dot_general(H[p][at], tall, NT, preferred_element_type=F32)

    def project(b, gaps):
        for p in TURNS[b]:
            cut = foreign[p]
            need_all(2 * b + p, False)
            begun = ACC[p][...] if b == 0 else gate_up(b, p, low, cut)
            hidden(p, cut, begun + gate_up(b, p, high, cut))
            PX[b, cut] = down(b, p, cut, other).astype(BF16)
            half_send(b, p).start()
        for p in range(2):
            PO[foreign[p]] = down(b, p, foreign[p], t)
        gaps[0]()
        for p in TURNS[b]:
            cut = foreign[p]
            half_send(b, p).wait_recv()
            S[b, p] = (PO[cut] + PR[b, cut].astype(F32)).astype(BF16)
            for k in range(2):
                for i in range(2):
                    back_send(b, p, i, k).start()
        for p in range(2):
            hidden(p, own, gate_up(b, p, low, own) + gate_up(b, p, high, own))
        PX[b, own] = (down(b, 0, own, other) + down(b, 1, own, other)).astype(BF16)
        half_send(b, 2).start()
        gaps[1]()
        PO[own] = down(b, 0, own, t) + down(b, 1, own, t)
        gaps[2]()
        half_send(b, 2).wait_recv()

    def collect(b, k):
        cut = part_of(k)
        total = PO[cut] + PR[b, cut].astype(F32)
        for p in range(2):
            back_here(b, p, k)
            total = total + R[b, p, cut].astype(F32)
        return total

    groups_here = 2
    width = half // groups_here

    def ready_pool():
        issue(8)
        maps = WB1[:, 3 * widths[1]:].reshape(2 * SIDE * SIDE, depth, 128).astype(F32)
        maps = maps.reshape(2 * SIDE * SIDE, 4, 8, 128)
        for g in range(groups_here):
            TM[g] = jnp.concatenate(
                [maps[:, g].reshape(width, 128), maps[:, 2 + g].reshape(width, 128)], axis=1
            ).astype(BF16)
            reached = 2 * 2 ** g * jnp.where(t == 0, 1, 2 ** groups_here)
            ages = lax.broadcasted_iota(jnp.int32, (rows, 128), 0) + 1
            RC[g] = 1.0 / jnp.minimum(ages, reached).astype(F32)

    def slabs(s, n):
        ref = WB[s].at[0:n * depth]
        return lambda key: remote(ref, ref, ws.at[s], wr.at[ARRIVALS[key]], mate)

    def need_all(s, mine):
        for op in COPIES:
            if op[1] == s and own_rows(op) == mine and op in WANTED:
                need(op)
        key = ("low" if mine else "high", s)
        n = sum(arrival(op) == key for op in COPIES)
        if n:
            slabs(s, n)(key).wait_recv()

    loaded(0, own_w.at[0])
    loaded(1, pw_ref)
    pack(0)
    pack(1)
    loaded(3, own_w.at[1])
    pack(2)
    pack(3)
    loaded(2, TB.at[0, t, own])
    loaded(4, wide_gain)
    loaded(5, slim_gain)
    pl.semaphore_wait(barrier, len(peers))

    issue(0)
    mate_send(0, 2, own).start()
    mate_send(0, 2, own).wait_recv()
    norm_rows(0, own)
    issue(1)
    issue(2)
    for p in range(2):
        tok_here(0, p, 0, foreign[p])
        mate_send(0, p, foreign[p]).start()
    issue(3)
    for p in range(2):
        mate_send(0, p, foreign[p]).wait_recv()
        norm_rows(0, foreign[p])
    issue(4)
    for p in TURNS[0]:
        need_all(p, True)
        ACC[p][...] = gate_up(0, p, low, foreign[p])
    issue(5)
    project(0, [lambda: issue(6), lambda: issue(7), ready_pool])

    def shifted(v, by):
        spot_ids = lax.broadcasted_iota(jnp.int32, v.shape, 0)
        return jnp.where(spot_ids >= by, pltpu.roll(v, by, 0), 0.0)

    def swap(k):
        cut = part_of(k)
        return remote(SQ.at[0, cut], SQ.at[1, cut], qs.at[0], qs.at[1 + k], mate)

    reach = 2 ** GROUPS
    for k in range(2):
        cut = part_of(k)
        after_first = (TB[0, t, cut].astype(F32) + 0.5 * collect(0, k)).astype(BF16).astype(F32)
        square = after_first * after_first
        SQ[0, cut] = sum(square[:, i * 128:(i + 1) * 128] for i in range(half // 128))
        swap(k).start()
        swap(k).wait_recv()
        total = jnp.sum(SQ[0, cut] + SQ[1, cut], axis=-1, keepdims=True)
        inv = lax.rsqrt(total / (2 * half) + epsilon)
        HB[cut] = (after_first * inv * slim_gain[0:1, :]).astype(BF16).astype(F32)
        lead = reach if k else 0
        for g in range(groups_here):
            at = slice(g * width, (g + 1) * width)
            hg = HB[cut.start - lead:cut.stop, at]
            run = hg + shifted(hg, 1)
            window = 2
            found = run
            number = t * groups_here + g
            for level in range(1, GROUPS):
                run = run + shifted(run, window)
                window = window * 2
                found = jnp.where(number >= level, run, found)
            share = jnp.concatenate([RC[g, cut]] * (width // 128), axis=1)
            diff = (found[lead:] * share - hg[lead:]).astype(BF16)
            mixed = lax.dot_general(diff, TM[g], NT, preferred_element_type=F32)
            TB[1, t, cut, at] = (after_first[:, at] + slim_gain[1:2, at] * mixed).astype(BF16)
        for p in range(2):
            for i in range(2):
                tok_send(1, p, i, k).start()
        mate_send(1, 2 + 3 * k, cut).start()

    issue(9)
    for k in range(2):
        for p in TURNS[1]:
            tok_here(1, p, k, far_part(p, k))
            mate_send(1, p + 3 * k, far_part(p, k)).start()
        if k == 0:
            for i in range(2):
                mate_send(1, 2 + 3 * i, part_of(i)).wait_recv()
            norm_rows(1, own)
        for p in TURNS[1]:
            mate_send(1, p + 3 * k, far_part(p, k)).wait_recv()
            norm_rows(1, far_part(p, k))
    for p in TURNS[1]:
        need_all(2 + p, True)
    project(1, [lambda: None] * 3)
    for k in range(2):
        cut = part_of(k)
        out_ref[cut] = (TB[1, t, cut].astype(F32) + 0.5 * collect(1, k)).astype(BF16)

    for s in range(4):
        n = sum(op[1] == s for op in COPIES)
        ref = WB[s].at[0:n * depth]
        remote(ref, ref, ws.at[s], wr.at[0], mate).wait_send()
    for b in range(2):
        remote(S.at[b], R.at[b], ts.at[b], tr.at[b, 0, 0], mate).wait_send()
        remote(S.at[b], R.at[b], rs.at[b], rr.at[b, 0, 0], mate).wait_send()
        remote(PX.at[b], PR.at[b], ms.at[b], mr.at[b, 0], mate).wait_send()
        remote(PX.at[b], PR.at[b], hs.at[b], hr.at[b, 0], mate).wait_send()
    remote(SQ.at[0], SQ.at[1], qs.at[0], qs.at[1], mate).wait_send()


def fused(
    tokens, pre_gain, first_gate, first_up, first_down, mix_gain, pool_weight,
    pool_scale, post_gain, second_gate, second_up, second_down,
):
    _, rows, half = tokens.shape
    depth, hid = first_gate.shape
    wide = 3 * hid // 10
    slim = hid // 2 - wide
    groups, width, out_cols = pool_weight.shape
    lanes = (3 * wide, 3 * slim + 128, 3 * wide, 3 * slim)

    vmem = pl.BlockSpec(memory_space=pltpu.VMEM)
    anyw = pl.BlockSpec(memory_space=pl.ANY)
    dma = pltpu.SemaphoreType.DMA
    out = pl.pallas_call(
        layer_kernel,
        out_shape=pltpu.VMEM((rows, half), BF16),
        in_specs=[anyw] * 12,
        out_specs=vmem,
        scratch_shapes=[
            pltpu.VMEM((2, 2 * half), F32),
            pltpu.VMEM((2, half), F32),
            pltpu.VMEM((groups * out_cols, width), BF16),
            pltpu.VMEM((2, 3, depth, hid), BF16),
        ]
        + [pltpu.VMEM((2, depth, n), BF16) for n in lanes]
        + [pltpu.VMEM((2 * half, n), BF16) for n in lanes]
        + [
            pltpu.VMEM((2, 2, 3 * rows, half), BF16),
            pltpu.VMEM((2, 3 * rows, half), BF16),
            pltpu.VMEM((rows, 2 * wide), F32),
            pltpu.VMEM((rows, 2 * slim), F32),
            pltpu.VMEM((2 * rows, wide), BF16),
            pltpu.VMEM((2 * rows, slim), BF16),
            pltpu.VMEM((2, 3 * rows, half), BF16),
            pltpu.VMEM((2, 3 * rows, half), BF16),
            pltpu.VMEM((3 * rows, half), F32),
            pltpu.VMEM((2, 2, rows, half), BF16),
            pltpu.VMEM((2, 2, rows, half), BF16),
            pltpu.VMEM((2, rows, 128), F32),
            pltpu.VMEM((groups, width, width), BF16),
            pltpu.VMEM((groups, rows, 128), F32),
            pltpu.VMEM((rows, half), F32),
            dma((6,)), dma((4,)), dma((len(ARRIVALS),)),
            dma((2,)), dma((2, 2, 2)), dma((2,)), dma((2, 6)), dma((2,)), dma((2, 3)),
            dma((2,)), dma((2, 2, 2)), dma((3,)),
        ],
        compiler_params=pltpu.CompilerParams(
            collective_id=0, has_side_effects=True, vmem_limit_bytes=60 * 1024 * 1024
        ),
    )(
        tokens.reshape(rows, half), pre_gain.reshape(1, -1), mix_gain.reshape(1, -1),
        pool_scale.reshape(1, -1), post_gain.reshape(1, -1),
        jnp.swapaxes(pool_weight, 1, 2).reshape(groups * out_cols, width),
        first_gate, first_up, first_down.T, second_gate, second_up, second_down.T,
    )
    return out.reshape(tokens.shape)


def solution(mesh):
    tok = P(("rep", "fs"), None, "tp")
    wide = P("fs", "tp")
    tall = P("tp", "fs")
    placed = (
        tok, P(), wide, wide, tall, P("tp"), P("tp", None, "fs"), P("tp"), P(), wide, wide, tall,
    )

    def layer(*args):
        return jax.shard_map(fused, mesh=mesh, in_specs=placed, out_specs=tok, check_vma=False)(*args)

    return layer
```
